32 devices in a mesh: sp: 8 (over z, y), tp: 4 (over x, core).
Axes of the slice: x: 2, y: 2, z: 4, core: 2. Of those that a mesh axis runs over, the one named last changes fastest.
Arguments:
- tokens: bfloat16 [4096, 2048], P('sp', 'tp'), may hold values from -400 to 400
- norm_gain: float32 [2048], replicated, may hold values from 0.1 to 1.9
- query_weight: bfloat16 [2048, 1024], P(None, 'tp'), may hold values from -0.37306796 to 0.37306796
- key_weight: bfloat16 [2048, 1024], P(None, 'tp'), may hold values from -0.2625825 to 0.2625825
- value_weight: bfloat16 [2048, 1024], P(None, 'tp'), may hold values from -0.125 to 0.125
- outer_gate_weight: bfloat16 [2048, 1024], P(None, 'tp'), may hold values from -0.125 to 0.125
- inner_gate_weight: bfloat16 [2048, 1024], P(None, 'tp'), may hold values from -0.125 to 0.125
- conv_input_weight: bfloat16 [2048, 1024], P(None, 'tp'), may hold values from -0.125 to 0.125
- conv_taps: float32 [3, 1024], P(None, 'tp'), may hold values from -3.5 to 3.5
- lambdas: float32 [8], P('tp'), may hold values from 0.3 to 0.8
- head_gain: float32 [128], replicated, may hold values from 0.1 to 1.9
- attn_out_weight: bfloat16 [1024, 2048], P(None, 'tp'), may hold values from -0.125 to 0.125
- conv_out_weight: bfloat16 [1024, 2048], P(None, 'tp'), may hold values from -0.125 to 0.125
Outputs:
- mixed_out: bfloat16 [4096, 2048], P('sp', 'tp')
- log_totals: float32 [8, 2, 4096], P('tp', None, 'sp')
The draws below stay inside these ranges and needn't reach their ends.
All inputs are finite; a program needn't handle non-finite values.
Results may differ from the reference program's by a relative error of at most 0.014.
The reference program's roundings to bfloat16 on the way count: a program that leaves them out, or rounds other values in their place, can miss the bound.
Values may be sent and summed in bfloat16 or wider, within the bound.
A program may use at most 128 MiB of HBM per device.

```python
import jax
import jax.numpy as jnp
from jax import lax

WIDTH = 2048
HEADS = 8
HEAD_DIM = 64
TAPS = 3
TOK_DEV = 512
CHANNELS = 1024
TOKENS = 4096


def drawn_weight(key, salt, fan_in):
    base = jax.random.normal(jax.random.fold_in(key, salt), (WIDTH, CHANNELS), jnp.float32)
    base = jnp.clip(base, -6.0, 6.0) * fan_in ** (-0.5)
    return base.astype(jnp.bfloat16)


def draw_query_weight(key, part):
    return drawn_weight(key, 11, WIDTH / 3.0)


def draw_key_weight(key, part):
    return drawn_weight(key, 12, WIDTH * 1.0)


def draw_tokens(key, part):
    values = jnp.clip(jax.random.normal(jax.random.fold_in(key, 2), (TOKENS, WIDTH), jnp.float32), -6.0, 6.0)
    return values.astype(jnp.bfloat16)


def level_of(stream_key, shape, split, low, largest):
    def one(position, parts):
        heights = jax.random.uniform(jax.random.fold_in(jax.random.fold_in(stream_key, 6), position), (parts,), jnp.float32, low / len(split), largest / len(split))
        return jnp.repeat(jnp.exp(heights), shape[position] // parts).reshape((-1,) + (1,) * (len(shape) - position - 1))

    level = one(*split[0])
    for cut in split[1:]:
        level = level * one(*cut)
    return level


def centred(key, dims, spread, most, split=(), held_as=jnp.bfloat16):
    array = jax.random.normal(key, dims, jnp.float32) * spread
    if len(split) > 0:
        array = level_of(key, dims, split, -0.22, 0.18) * array
    return jnp.clip(array, min=-most, max=most).astype(held_as)


def setup_inputs(seed: int = 0) -> dict:
    streams_of = jax.random.split(jax.random.key(seed), 14)
    return {
        "tokens": draw_tokens(jax.random.fold_in(streams_of[13], 71), 0),
        "norm_gain": jnp.clip(1.0 + 0.18 * jax.random.normal(streams_of[1], (WIDTH,), jnp.float32), 0.1, 1.9),
        "query_weight": draw_query_weight(jax.random.fold_in(streams_of[13], 71), 0),
        "key_weight": draw_key_weight(jax.random.fold_in(streams_of[13], 71), 0),
        "value_weight": centred(streams_of[4], (WIDTH, CHANNELS), WIDTH ** -0.5, 0.125, ((1, 4),)),
        "outer_gate_weight": centred(streams_of[5], (WIDTH, CHANNELS), WIDTH ** -0.5, 0.125, ((1, 4),)),
        "inner_gate_weight": centred(streams_of[6], (WIDTH, CHANNELS), WIDTH ** -0.5, 0.125, ((1, 4),)),
        "conv_input_weight": centred(streams_of[7], (WIDTH, CHANNELS), WIDTH ** -0.5, 0.125, ((1, 4),)),
        "conv_taps": centred(streams_of[8], (TAPS, CHANNELS), TAPS ** -0.5, 3.5, ((1, 4),), jnp.float32),
        "lambdas": jnp.clip(0.3 + 0.5 * jax.random.uniform(streams_of[9], (HEADS,), jnp.float32) ** level_of(streams_of[9], (HEADS,), ((0, 4),), -0.2, 0.2), 0.3, 0.8),
        "head_gain": jnp.clip(1.0 + 0.18 * jax.random.normal(streams_of[10], (2 * HEAD_DIM,), jnp.float32), 0.1, 1.9),
        "attn_out_weight": centred(streams_of[11], (CHANNELS, WIDTH), (2 * CHANNELS) ** -0.5, 0.125, ((1, 4),)),
        "conv_out_weight": centred(streams_of[12], (CHANNELS, WIDTH), (2 * CHANNELS) ** -0.5, 0.125, ((1, 4),)),
    }


NORM_EPS = 1e-06
HEAD_EPS = 1e-05
ROPE_BASE = 500000.0
MASKED = -1e+30
HEAD_SCALE = 0.8

def rotate(field_in, positions):
    half_dim = field_in.shape[-1] // 2
    frequency = ROPE_BASE ** (-jnp.arange(half_dim, dtype=jnp.float32) * 2.0 / field_in.shape[-1])
    angles = positions[:, None] * frequency[None, :]
    cosine = jnp.cos(angles)[:, None, None, :]
    sine_part = jnp.sin(angles)[:, None, None, :]
    first_half = field_in[..., :half_dim]
    second_half = field_in[..., half_dim:]
    return jnp.concatenate([first_half * cosine - second_half * sine_part, second_half * cosine + first_half * sine_part], axis=-1)

def reference(tokens, norm_gain, query_weight, key_weight, value_weight, outer_gate_weight, inner_gate_weight, conv_input_weight, conv_taps, lambdas, head_gain, attn_out_weight, conv_out_weight):
    floats = tokens.astype(jnp.float32)
    inverse_rms = lax.rsqrt(lax.optimization_barrier(jnp.mean(floats * floats, axis=1, keepdims=True)) + NORM_EPS)
    scaled = (floats * norm_gain[None, :]).astype(jnp.bfloat16)

    def project(weight):
        return inverse_rms * jnp.dot(scaled, weight, preferred_element_type=jnp.float32)
    positions = jnp.arange(TOKENS, dtype=jnp.float32)
    queries = rotate(project(query_weight).reshape(TOKENS, HEADS, 2, HEAD_DIM), positions).astype(jnp.bfloat16)
    key_rows = rotate(project(key_weight).reshape(TOKENS, HEADS, 2, HEAD_DIM), positions).astype(jnp.bfloat16)
    values = project(value_weight).astype(jnp.bfloat16).reshape(TOKENS, HEADS, 2 * HEAD_DIM)
    outer_gate = project(outer_gate_weight).astype(jnp.bfloat16)
    inner_gate = project(inner_gate_weight).astype(jnp.bfloat16)
    signal = project(conv_input_weight).astype(jnp.bfloat16)
    conv_in = (inner_gate.astype(jnp.float32) * signal.astype(jnp.float32)).astype(jnp.bfloat16)
    padded = jnp.concatenate([jnp.zeros((TAPS - 1, CHANNELS), jnp.bfloat16), conv_in], axis=0)
    summed = jnp.zeros((TOKENS, CHANNELS), jnp.float32)
    for tap_index in range(TAPS):
        summed = summed + conv_taps[tap_index][None, :] * padded[tap_index:tap_index + TOKENS].astype(jnp.float32)
    conv_out = (outer_gate.astype(jnp.float32) * summed).astype(jnp.bfloat16)
    blocks = TOKENS // TOK_DEV

    def one_block(flat_index):
        head_index = flat_index // blocks
        row_start = (flat_index % blocks * TOK_DEV).astype(jnp.int32)
        query_rows = lax.dynamic_slice_in_dim(queries, row_start, TOK_DEV, 0)
        query_rows = lax.dynamic_index_in_dim(query_rows, head_index, 1, keepdims=False)
        head_keys = lax.dynamic_index_in_dim(key_rows, head_index, 1, keepdims=False)
        head_values = lax.dynamic_index_in_dim(values, head_index, 1, keepdims=False)
        scores = jnp.einsum('qcd,kcd->cqk', query_rows.astype(jnp.float32), head_keys.astype(jnp.float32)) * HEAD_DIM ** (-0.5)
        visible = (row_start + jnp.arange(TOK_DEV, dtype=jnp.int32))[:, None] >= jnp.arange(TOKENS, dtype=jnp.int32)[None, :]
        scores = jnp.where(visible[None], scores, MASKED)
        row_max = lax.optimization_barrier(jnp.max(scores, axis=-1, keepdims=True))
        exponent = jnp.where(visible[None], jnp.exp(scores - row_max), 0.0)
        row_sum = lax.optimization_barrier(jnp.sum(exponent, axis=-1, keepdims=True))
        normalized = exponent / row_sum
        lambda_value = lambdas[head_index]
        weights = (normalized[0] - lambda_value * normalized[1]).astype(jnp.bfloat16)
        head_mix = jnp.dot(weights, head_values, preferred_element_type=jnp.float32)
        normed = head_mix * lax.rsqrt(lax.optimization_barrier(jnp.mean(head_mix * head_mix, axis=-1, keepdims=True)) + HEAD_EPS) * head_gain[None, :] * HEAD_SCALE
        return (normed.astype(jnp.bfloat16), (row_max + jnp.log(row_sum))[..., 0])
    head_rows, log_rows = lax.map(one_block, jnp.arange(HEADS * blocks, dtype=jnp.int32))
    attn_out = jnp.transpose(head_rows.reshape(HEADS, blocks, TOK_DEV, 2 * HEAD_DIM), (1, 2, 0, 3)).reshape(TOKENS, CHANNELS)
    log_totals = jnp.transpose(log_rows.reshape(HEADS, blocks, 2, TOK_DEV), (0, 2, 1, 3)).reshape(HEADS, 2, TOKENS)
    mixed_out = jnp.dot(attn_out, attn_out_weight, preferred_element_type=jnp.float32) + jnp.dot(conv_out, conv_out_weight, preferred_element_type=jnp.float32)
    return (mixed_out.astype(jnp.bfloat16), log_totals)
```

```python
import functools

import jax
import jax.numpy as jnp
import numpy as np
from jax import lax
from jax.experimental import pallas as pl
from jax.experimental.pallas import tpu as pltpu
from jax.sharding import PartitionSpec as P

NORM_EPS = 1e-06
HEAD_EPS = 1e-05
ROPE_BASE = 500000.0
MASKED = -1e30
HEAD_SCALE = 0.8
F32 = jnp.float32
BF16 = jnp.bfloat16


def dot(a, b):
    return jnp.dot(a, b, preferred_element_type=F32)


def dot_t(a, b):
    return lax.dot_general(a, b, (((1,), (1,)), ((), ())), preferred_element_type=F32)


def ring_kernel(
    dims,
    tokens,
    gain,
    freq,
    wq_h,
    wk_h,
    wv_h,
    wo_h,
    wi_h,
    ws_h,
    taps,
    lambdas,
    head_gain,
    wa_h,
    wc_h,
    out,
    lse,
    tok,
    scaled,
    inv,
    cos_t,
    sin_t,
    wq,
    wk,
    wv,
    wo,
    wi,
    ws,
    wa,
    wc,
    kv,
    qz,
    row_max,
    row_sum,
    acc,
    gate,
    padded,
    tail,
    rim,
    conv_all,
    attn_all,
    total,
    w_sem,
    own_sem,
    tok_recv,
    tok_send,
    tok_relay,
    kv_recv,
    kv_send_z,
    kv_send_y,
    kv_extra,
    rim_sem,
    mix_recv,
    mix_send,
    mix_relay,
):
    S, T, Z, Y, H = dims["S"], dims["T"], dims["Z"], dims["Y"], dims["H"]
    L, Dt = tokens.shape
    Wd = T * Dt
    C = wq_h.shape[1]
    V = C // H
    hd = V // 2
    NR = tok_recv.shape[1]
    R = L // NR
    NM = mix_recv.shape[2]
    M = L // NM
    X = T // 2
    taps_n = taps.shape[0]
    PAD = tail.shape[0]

    sp = lax.axis_index("sp")
    tp = lax.axis_index("tp")
    z = sp // Y
    y = sp % Y
    core = tp % 2
    xi = tp // 2
    sib = xi * 2 + (1 - core)

    def peer(k):
        return ((xi + k) % X) * 2 + core

    def source(k):
        return ((xi - k + X) % X) * 2 + core

    pairs = [(wk_h, wk), (wv_h, wv), (wq_h, wq), (wi_h, wi), (ws_h, ws), (wo_h, wo), (wc_h, wc), (wa_h, wa)]
    own = pltpu.make_async_copy(tokens, tok.at[tp], own_sem)
    own.start()
    loads = [pltpu.make_async_copy(s, d, w_sem.at[i]) for i, (s, d) in enumerate(pairs)]
    for load in loads:
        load.start()

    barrier = pltpu.get_barrier_semaphore()

    def greet(target):
        pl.semaphore_signal(barrier, inc=1, device_id=target)

    for k in range(1, T):
        greet({"tp": (tp + k) % T})
    for k in range(1, Y):
        greet({"sp": z * Y + (y + k) % Y})
    has_up = z + 1 < Z
    has_down = z > 0
    far_up = jnp.logical_and(has_up, y == Y - 1) if Y > 1 else None
    far_down = jnp.logical_and(has_down, y == 0) if Y > 1 else None
    expect = (T - 1) + (Y - 1) + has_up.astype(jnp.int32) + has_down.astype(jnp.int32)

    @pl.when(has_up)
    def _():
        greet({"sp": sp + Y})

    @pl.when(has_down)
    def _():
        greet({"sp": sp - Y})

    if Y > 1:
        expect = expect + far_up.astype(jnp.int32) + far_down.astype(jnp.int32)

        @pl.when(far_up)
        def _():
            greet({"sp": sp + 1})

        @pl.when(far_down)
        def _():
            greet({"sp": sp - 1})

    pl.semaphore_wait(barrier, expect)

    def tok_rows(r):
        return pl.ds(pl.multiple_of(r * R, R), R)

    def tok_copy(src, piece, r, send, target):
        return pltpu.make_async_remote_copy(
            src_ref=src,
            dst_ref=tok.at[piece, tok_rows(r), :],
            send_sem=send,
            recv_sem=tok_recv.at[piece, r],
            device_id={"tp": target},
        )

    def tok_own(k, r):
        target = peer(k) if k else sib
        return tok_copy(tokens.at[tok_rows(r), :], tp, r, tok_send.at[k, r], target)

    def tok_forward(k, r):
        piece = source(k)
        return tok_copy(tok.at[piece, tok_rows(r), :], piece, r, tok_relay.at[k, r], sib)

    def tok_wait(piece, r):
        tok_copy(tok.at[piece, tok_rows(r), :], piece, r, tok_send.at[0, r], sib).wait_recv()

    for r in range(NR):
        for k in list(range(1, X)) + [0]:
            tok_own(k, r).start()

    lane = lax.broadcasted_iota(jnp.int32, (R, V), 1)
    first = (lane % hd) < (hd // 2)

    def table(r, carry):
        base = sp * L + r * R
        pos = (base + lax.broadcasted_iota(jnp.int32, (R, V), 0)).astype(F32)
        angle = pos * freq[...]
        sine = jnp.sin(angle)
        cos_t[tok_rows(r), :] = jnp.cos(angle)
        sin_t[tok_rows(r), :] = jnp.where(first, -sine, sine)
        return carry

    lax.fori_loop(0, NR, table, 0)

    def rotate(block, rows):
        low = (lax.broadcasted_iota(jnp.int32, block.shape, 1) % hd) < (hd // 2)
        other = jnp.where(
            low, pltpu.roll(block, V - hd // 2, 1), pltpu.roll(block, hd // 2, 1)
        )
        return block * cos_t[rows, :] + other * sin_t[rows, :]

    def kv_copy(j, r, send, target):
        block = kv.at[j, tok_rows(r), :]
        return pltpu.make_async_remote_copy(
            src_ref=block,
            dst_ref=block,
            send_sem=send,
            recv_sem=kv_recv.at[j, r],
            device_id={"sp": target},
        )

    def kv_up(dz, r):
        return kv_copy(sp - dz * Y, r, kv_send_z.at[dz, r], sp + Y)

    def kv_side(dz, r, k):
        return kv_copy(sp - dz * Y, r, kv_send_y.at[dz, r, k - 1], z * Y + (y + k) % Y)

    def kv_wait(j, r):
        kv_copy(j, r, kv_send_z.at[0, r], sp).wait_recv()

    EX = NR // 2 if Y == 2 else 0

    def extra(r):
        return kv_copy(0, r, kv_extra.at[r], sp + Y)

    def kv_send(dz, r, act):
        @pl.when(has_up)
        def _():
            act(kv_up(dz, r))

        for k in range(1, Y):
            wanted = jnp.logical_or(dz > 0, y + k < Y)
            if EX:
                other_way = jnp.logical_and(dz == z, jnp.logical_and(dz > 0, r < EX))
                wanted = jnp.logical_and(wanted, jnp.logical_not(jnp.logical_and(y == 0, other_way)))

            @pl.when(wanted)
            def _():
                act(kv_side(dz, r, k))

    def relay(dz, r):
        @pl.when(dz <= z)
        def _():
            kv_wait(sp - dz * Y, r)
            kv_send(dz, r, lambda copy: copy.start())

    def first_relay(r):
        relay(1, r)
        if EX:

            @pl.when(jnp.logical_and(jnp.logical_and(z == 0, y == 1), r < EX))
            def _():
                kv_wait(0, r)

                @pl.when(has_up)
                def _():
                    extra(r).start()

    own.wait()
    loads[0].wait()
    loads[1].wait()

    def key_chunk(r, carry):
        rows = tok_rows(r)
        for k in range(1, X):
            tok_wait(source(k), r)
            tok_forward(k, r).start()
        tok_wait(sib, r)
        for k in range(1, X):
            tok_wait(((xi + k) % X) * 2 + (1 - core), r)
        squares = jnp.zeros((R, 1), F32)
        for t in range(T):
            block = tok[t, rows, :].astype(F32)
            squares = squares + jnp.sum(block * block, axis=1, keepdims=True)
            scaled[rows, t * Dt : (t + 1) * Dt] = (block * gain[:, t * Dt : (t + 1) * Dt]).astype(BF16)
        inverse = lax.rsqrt(squares / Wd + NORM_EPS)
        inv[rows, :] = inverse
        left = scaled[rows, :]
        keys = inverse * dot(left, wk[...])
        for h in range(H):
            kv[sp, rows, h * V : (h + 1) * V] = rotate(keys[:, h * V : (h + 1) * V], rows).astype(BF16)
        kv[sp, rows, C : 2 * C] = (inverse * dot(left, wv[...])).astype(BF16)
        kv_send(0, r, lambda copy: copy.start())

        @pl.when(r > 0)
        def _():
            first_relay(r - 1)

        return carry

    lax.fori_loop(0, NR, key_chunk, 0)

    for load in loads[2:6]:
        load.wait()
    half = lax.broadcasted_iota(jnp.int32, (M, V), 1) < hd
    scale = hd ** (-0.5)

    def mix_rows(r):
        return pl.ds(pl.multiple_of(r * M, M), M)

    def query_chunk(r, carry):
        rows = mix_rows(r)
        inverse = inv[rows, :]
        left = scaled[rows, :]
        queries = inverse * dot(left, wq[...])
        for h in range(H):
            turned = rotate(queries[:, h * V : (h + 1) * V], rows).astype(BF16).astype(F32) * scale
            qz[h, 0, rows, :] = jnp.where(half, turned, 0.0).astype(BF16)
            qz[h, 1, rows, :] = jnp.where(half, 0.0, turned).astype(BF16)
        inner = (inverse * dot(left, wi[...])).astype(BF16)
        signal = (inverse * dot(left, ws[...])).astype(BF16)
        conv_in = (inner.astype(F32) * signal.astype(F32)).astype(BF16)
        padded[pl.ds(pl.multiple_of(PAD + r * M, PAD), M), :] = conv_in.astype(F32)
        gate[rows, :] = (inverse * dot(left, wo[...])).astype(BF16)

        @pl.when(r == 0)
        def _():
            first_relay(NR - 1)

        return carry

    lax.fori_loop(0, NM, query_chunk, 0)
    tail[...] = padded[L : L + PAD, :].astype(BF16)
    rim_copy = pltpu.make_async_remote_copy(
        src_ref=tail,
        dst_ref=rim,
        send_sem=rim_sem.at[0],
        recv_sem=rim_sem.at[1],
        device_id={"sp": (sp + 1) % S},
    )

    @pl.when(sp + 1 < S)
    def _():
        rim_copy.start()

    def attend(j, diagonal):
        def one(i, carry):
            rows = mix_rows(i)
            for h in range(H):
                query = qz[h, :, rows, :].reshape(2 * M, V)
                scores = dot_t(query, kv[j, :, h * V : (h + 1) * V])
                if diagonal:
                    row = lax.broadcasted_iota(jnp.int32, scores.shape, 0)
                    row = jnp.where(row >= M, row - M, row) + i * M
                    col = lax.broadcasted_iota(jnp.int32, scores.shape, 1)
                    scores = jnp.where(row >= col, scores, MASKED)
                    new_max = jnp.max(scores, axis=1, keepdims=True)
                else:
                    old_max = row_max[h, :, rows, :].reshape(2 * M, 1)
                    new_max = jnp.maximum(old_max, jnp.max(scores, axis=1, keepdims=True))
                weights = jnp.exp(scores - new_max)
                sums = jnp.sum(weights, axis=1, keepdims=True)
                mixed = dot(weights.astype(BF16), kv[j, :, C + h * V : C + (h + 1) * V])
                if not diagonal:
                    fade = jnp.exp(old_max - new_max)
                    sums = sums + fade * row_sum[h, :, rows, :].reshape(2 * M, 1)
                    mixed = mixed + fade * acc[h, :, rows, :].reshape(2 * M, V)
                row_max[h, :, rows, :] = new_max.reshape(2, M, 1)
                row_sum[h, :, rows, :] = sums.reshape(2, M, 1)
                acc[h, :, rows, :] = mixed.reshape(2, M, V)
            return carry

        lax.fori_loop(0, NM, one, 0)

    attend(sp, True)

    @pl.when(sp > 0)
    def _():
        rim_copy.wait_recv()
        padded[0:PAD, :] = rim[...].astype(F32)

    @pl.when(sp == 0)
    def _():
        padded[0:PAD, :] = jnp.zeros((PAD, C), F32)

    summed = jnp.zeros((L, C), F32)
    for j in range(taps_n):
        begin = PAD - (taps_n - 1) + j
        summed = summed + taps[j : j + 1, :] * padded[begin : begin + L, :]
    conv_all[tp, :, :] = (gate[...].astype(F32) * summed).astype(BF16)

    def mix_copy(which, buf, piece, r, send, target):
        block = buf.at[piece, mix_rows(r), :]
        return pltpu.make_async_remote_copy(
            src_ref=block,
            dst_ref=block,
            send_sem=send,
            recv_sem=mix_recv.at[which, piece, r],
            device_id={"tp": target},
        )

    def mix_own(which, buf, k, r):
        target = peer(k) if k else sib
        return mix_copy(which, buf, tp, r, mix_send.at[which, k, r], target)

    def mix_forward(which, buf, k, r):
        return mix_copy(which, buf, source(k), r, mix_relay.at[which, k, r], sib)

    def mix_wait(which, buf, piece, r):
        mix_copy(which, buf, piece, r, mix_send.at[which, 0, r], sib).wait_recv()

    for r in range(NM):
        for k in list(range(1, X)) + [0]:
            mix_own(0, conv_all, k, r).start()

    def step(dz, carry):
        def row_block(k, inner):
            def forward(r, c):
                relay(dz + 1, r)
                return c

            lax.fori_loop(k * NR // Y, (k + 1) * NR // Y, forward, 0)
            side = (y + k) % Y
            level = jnp.where(k == 0, z - dz, z - dz + 1)
            j = level * Y + side
            valid = jnp.where(k == 0, dz <= z, jnp.logical_or(level < z, side < y))

            @pl.when(valid)
            def _():
                @pl.when(k > 0)
                def _():
                    for r in range(NR):
                        if r < EX:
                            climbs = jnp.logical_and(level == 0, y == 1)

                            @pl.when(jnp.logical_not(jnp.logical_and(climbs, z == 0)))
                            def _():
                                kv_wait(j, r)

                            @pl.when(jnp.logical_and(climbs, jnp.logical_and(z > 0, has_up)))
                            def _():
                                extra(r).start()

                        else:
                            kv_wait(j, r)

                attend(j, False)

            return inner

        lax.fori_loop(0, Y, row_block, 0)
        return carry

    lax.fori_loop(1, z + 2, step, 0)

    def finish(i, carry):
        rows = mix_rows(i)
        for h in range(H):
            first_map = acc[h, 0, rows, :] / row_sum[h, 0, rows, :]
            second_map = acc[h, 1, rows, :] / row_sum[h, 1, rows, :]
            head_mix = first_map - lambdas[h] * second_map
            mean = jnp.mean(head_mix * head_mix, axis=1, keepdims=True)
            normed = head_mix * lax.rsqrt(mean + HEAD_EPS) * head_gain[...] * HEAD_SCALE
            attn_all[tp, rows, h * V : (h + 1) * V] = normed.astype(BF16)
        for k in list(range(1, X)) + [0]:
            mix_own(1, attn_all, k, i).start()
        return carry

    lax.fori_loop(0, NM, finish, 0)

    loads[6].wait()
    loads[7].wait()

    def gather(which, buf, r):
        for k in range(1, X):
            mix_wait(which, buf, source(k), r)
            mix_forward(which, buf, k, r).start()

    def gather_rest(which, buf, r):
        mix_wait(which, buf, sib, r)
        for k in range(1, X):
            mix_wait(which, buf, ((xi + k) % X) * 2 + (1 - core), r)

    def conv_part(r, carry):
        rows = mix_rows(r)
        gather(0, conv_all, r)
        gather_rest(0, conv_all, r)
        part = dot(conv_all[0, rows, :], wc[0:C, :])
        for t in range(1, T):
            part = part + dot(conv_all[t, rows, :], wc[t * C : (t + 1) * C, :])
        total[rows, :] = part
        return carry

    lax.fori_loop(0, NM, conv_part, 0)

    lanes = lax.broadcasted_iota(jnp.int32, (L, 128), 1)
    columns = jnp.zeros((L, 128), F32)
    for h in range(H):
        for c in range(2):
            value = row_max[h, c, :, :] + jnp.log(row_sum[h, c, :, :])
            columns = jnp.where(lanes == 2 * h + c, value, columns)
    turned_columns = jnp.transpose(columns)
    for h in range(H):
        lse[h] = turned_columns[2 * h : 2 * h + 2, :]

    def attn_part(r, carry):
        rows = mix_rows(r)
        gather(1, attn_all, r)
        gather_rest(1, attn_all, r)
        part = total[rows, :]
        for t in range(T):
            part = part + dot(attn_all[t, rows, :], wa[t * C : (t + 1) * C, :])
        out[rows, :] = part.astype(BF16)
        return carry

    lax.fori_loop(0, NM, attn_part, 0)

    for r in range(NR):
        for k in range(X):
            tok_own(k, r).wait_send()
        for k in range(1, X):
            tok_forward(k, r).wait_send()

    def drain(dz, carry):
        def inner(r, c):
            kv_send(dz, r, lambda copy: copy.wait_send())
            return c

        return lax.fori_loop(0, NR, inner, carry)

    lax.fori_loop(0, z + 1, drain, 0)
    if EX:

        @pl.when(jnp.logical_and(y == 1, has_up))
        def _():
            for r in range(EX):
                extra(r).wait_send()

    for which, buf in ((0, conv_all), (1, attn_all)):
        for r in range(NM):
            for k in range(X):
                mix_own(which, buf, k, r).wait_send()
            for k in range(1, X):
                mix_forward(which, buf, k, r).wait_send()

    @pl.when(sp + 1 < S)
    def _():
        rim_copy.wait_send()


def ring_device(
    dims,
    tokens,
    norm_gain,
    query_weight,
    key_weight,
    value_weight,
    outer_gate_weight,
    inner_gate_weight,
    conv_input_weight,
    conv_taps,
    lambdas,
    head_gain,
    attn_out_weight,
    conv_out_weight,
):
    S, T, Z, Y = dims["S"], dims["T"], dims["Z"], dims["Y"]
    L, Dt = tokens.shape
    H = lambdas.shape[0]
    C = query_weight.shape[1]
    V = C // H
    hd = V // 2
    O = attn_out_weight.shape[1]
    Wd = norm_gain.shape[0]
    NR, NM, PAD = 4, 2, 16
    X = T // 2
    frequency = ROPE_BASE ** (-np.arange(hd // 2) * 2.0 / hd)
    freq = jnp.asarray(np.tile(frequency, 4)[None, :], F32)
    any_spec = pl.BlockSpec(memory_space=pl.ANY)
    vmem = pl.BlockSpec(memory_space=pltpu.VMEM)
    smem = pl.BlockSpec(memory_space=pltpu.SMEM)
    dma = pltpu.SemaphoreType.DMA
    mixed, lse = pl.pallas_call(
        functools.partial(ring_kernel, dict(dims, H=H)),
        out_shape=(
            jax.ShapeDtypeStruct((L, O), BF16),
            jax.ShapeDtypeStruct((H, 2, L), F32),
        ),
        in_specs=[any_spec, vmem, vmem] + [any_spec] * 6 + [vmem, smem, vmem] + [any_spec] * 2,
        out_specs=(vmem, vmem),
        scratch_shapes=[
            pltpu.VMEM((T, L, Dt), BF16),
            pltpu.VMEM((L, Wd), BF16),
            pltpu.VMEM((L, 1), F32),
            pltpu.VMEM((L, V), F32),
            pltpu.VMEM((L, V), F32),
        ]
        + [pltpu.VMEM((Wd, C), BF16)] * 6
        + [pltpu.VMEM((T * C, O), BF16)] * 2
        + [
            pltpu.VMEM((S, L, 2 * C), BF16),
            pltpu.VMEM((H, 2, L, V), BF16),
            pltpu.VMEM((H, 2, L, 1), F32),
            pltpu.VMEM((H, 2, L, 1), F32),
            pltpu.VMEM((H, 2, L, V), F32),
            pltpu.VMEM((L, C), BF16),
            pltpu.VMEM((PAD + L, C), F32),
            pltpu.VMEM((PAD, C), BF16),
            pltpu.VMEM((PAD, C), BF16),
            pltpu.VMEM((T, L, C), BF16),
            pltpu.VMEM((T, L, C), BF16),
            pltpu.VMEM((L, O), F32),
            dma((8,)),
            dma,
            dma((T, NR)),
            dma((X, NR)),
            dma((X, NR)),
            dma((S, NR)),
            dma((Z, NR)),
            dma((Z, NR, max(Y - 1, 1))),
            dma((NR,)),
            dma((2,)),
            dma((2, T, NM)),
            dma((2, X, NM)),
            dma((2, X, NM)),
        ],
        compiler_params=pltpu.CompilerParams(
            collective_id=0, has_side_effects=True, vmem_limit_bytes=60 * 1024 * 1024
        ),
        name="mixer",
    )(
        tokens,
        norm_gain[None, :],
        freq,
        query_weight,
        key_weight,
        value_weight,
        outer_gate_weight,
        inner_gate_weight,
        conv_input_weight,
        conv_taps,
        lambdas,
        head_gain[None, :],
        attn_out_weight,
        conv_out_weight,
    )
    return mixed, lse


def pair_kernel(
    dims,
    tokens,
    gain,
    freq,
    wq_h,
    wk_h,
    wv_h,
    wo_h,
    wi_h,
    ws_h,
    taps,
    lambdas,
    head_gain,
    wa_h,
    wc_h,
    out,
    lse,
    tok,
    scaled,
    inv,
    cos_t,
    sin_t,
    wq,
    wk,
    wv,
    wo,
    wi,
    ws,
    wa,
    wc,
    kvq,
    row_max,
    row_sum,
    acc,
    gate,
    padded,
    tail,
    rim,
    conv_all,
    attn_all,
    away,
    lse_away,
    lse_in,
    total,
    w_sem,
    own_sem,
    tok_recv,
    tok_send,
    tok_relay,
    kv_recv,
    swap_send,
    cross_send,
    side_send,
    up_send,
    rim_sem,
    lse_sem,
    mix_recv,
    mix_send,
    mix_relay,
    at_recv,
    at_send,
    at_away,
    at_relay,
    at_relay_away,
):
    S, T, Z, Y, H = dims["S"], dims["T"], dims["Z"], dims["Y"], dims["H"]
    L, Dt = tokens.shape
    Wd = T * Dt
    C = wq_h.shape[1]
    V = C // H
    hd = V // 2
    NR = tok_recv.shape[1]
    R = L // NR
    NM = mix_recv.shape[1]
    M = L // NM
    G = M // R
    X = T // 2
    taps_n = taps.shape[0]
    PAD = tail.shape[0]

    sp = lax.axis_index("sp")
    tp = lax.axis_index("tp")
    z = sp // Y
    y = sp % Y
    pair = z // 2
    a = z % 2
    mate = sp + (1 - 2 * a) * Y
    core = tp % 2
    xi = tp // 2
    sib = xi * 2 + (1 - core)
    has_up = z + 2 - a < Z
    has_down = pair > 0

    def peer(k):
        return ((xi + k) % X) * 2 + core

    def source(k):
        return ((xi - k + X) % X) * 2 + core

    def source_sib(k):
        return ((xi - k + X) % X) * 2 + (1 - core)

    pairs = [(wk_h, wk), (wv_h, wv), (wq_h, wq), (wi_h, wi), (ws_h, ws), (wo_h, wo), (wc_h, wc), (wa_h, wa)]
    own = pltpu.make_async_copy(tokens, tok.at[tp], own_sem)
    own.start()
    loads = [pltpu.make_async_copy(s, d, w_sem.at[i]) for i, (s, d) in enumerate(pairs)]
    for load in loads:
        load.start()

    barrier = pltpu.get_barrier_semaphore()

    def greet(target):
        pl.semaphore_signal(barrier, inc=1, device_id=target)

    for k in range(1, T):
        greet({"tp": (tp + k) % T})
    for k in range(X):
        greet({"sp": mate, "tp": peer(k)})
    for k in range(1, Y):
        greet({"sp": z * Y + (y + k) % Y})
    expect = (T - 1) + X + (Y - 1)
    bridge_up = jnp.logical_and(a == 1, has_up)
    bridge_down = jnp.logical_and(a == 0, has_down)
    for near, step in (
        (has_up, 2 * Y),
        (has_down, -2 * Y),
        (bridge_up, Y),
        (bridge_down, -Y),
        (sp + 1 < S, 1),
        (sp > 0, -1),
    ):
        expect = expect + near.astype(jnp.int32)

        @pl.when(near)
        def _():
            greet({"sp": sp + step})

    pl.semaphore_wait(barrier, expect)

    def tok_rows(r):
        return pl.ds(pl.multiple_of(r * R, R), R)

    def tok_copy(src, piece, r, send, target):
        return pltpu.make_async_remote_copy(
            src_ref=src,
            dst_ref=tok.at[piece, tok_rows(r), :],
            send_sem=send,
            recv_sem=tok_recv.at[piece, r],
            device_id={"tp": target},
        )

    def tok_own(k, r):
        target = peer(k) if k else sib
        return tok_copy(tokens.at[tok_rows(r), :], tp, r, tok_send.at[k, r], target)

    def tok_forward(k, r):
        piece = source(k)
        return tok_copy(tok.at[piece, tok_rows(r), :], piece, r, tok_relay.at[k, r], sib)

    def tok_wait(piece, r):
        tok_copy(tok.at[piece, tok_rows(r), :], piece, r, tok_send.at[0, r], sib).wait_recv()

    for r in range(NR):
        for k in list(range(1, X)) + [0]:
            tok_own(k, r).start()

    lane = lax.broadcasted_iota(jnp.int32, (R, V), 1)
    first = (lane % hd) < (hd // 2)

    def table(r, carry):
        base = sp * L + r * R
        pos = (base + lax.broadcasted_iota(jnp.int32, (R, V), 0)).astype(F32)
        angle = pos * freq[...]
        sine = jnp.sin(angle)
        cos_t[tok_rows(r), :] = jnp.cos(angle)
        sin_t[tok_rows(r), :] = jnp.where(first, -sine, sine)
        return carry

    lax.fori_loop(0, NR, table, 0)

    row_max[...] = jnp.full(row_max.shape, MASKED, F32)
    row_sum[...] = jnp.zeros(row_sum.shape, F32)
    acc[...] = jnp.zeros(acc.shape, F32)

    def rotate(block, rows):
        other = jnp.where(first, pltpu.roll(block, V - hd // 2, 1), pltpu.roll(block, hd // 2, 1))
        return block * cos_t[rows, :] + other * sin_t[rows, :]

    def kv_copy(src, j, r, send, target):
        return pltpu.make_async_remote_copy(
            src_ref=src,
            dst_ref=kvq.at[j, r, pl.ds(0, 2)],
            send_sem=send,
            recv_sem=kv_recv.at[j, r],
            device_id={"sp": target},
        )

    def swap(j, r):
        return pltpu.make_async_remote_copy(
            src_ref=kvq.at[S, r],
            dst_ref=kvq.at[j, r],
            send_sem=swap_send.at[r],
            recv_sem=kv_recv.at[j, r],
            device_id={"sp": mate},
        )

    def cross(r):
        return kv_copy(kvq.at[S, r, pl.ds(0, 2)], sp, r, cross_send.at[r], sp + Y)

    def level_block(level):
        return level * Y + y

    def up(level, r):
        j = level_block(level)
        return kv_copy(kvq.at[j, r, pl.ds(0, 2)], j, r, up_send.at[level, r], sp + 2 * Y)

    def side(level, r, k):
        j = level_block(level)
        return kv_copy(
            kvq.at[j, r, pl.ds(0, 2)], j, r, side_send.at[level, r, k - 1], z * Y + (y + k) % Y
        )

    def kv_wait(j, r):
        kv_copy(kvq.at[j, r, pl.ds(0, 2)], j, r, cross_send.at[r], sp).wait_recv()

    top = 2 * pair + 1

    def spread(level, r, rises, act):
        @pl.when(rises)
        def _():
            act(up(level, r))

        for k in range(1, Y):

            @pl.when(jnp.logical_or(level < top, y < (y + k) % Y))
            def _():
                act(side(level, r, k))

    def start(copy):
        copy.start()

    def drain(copy):
        copy.wait_send()

    def send_own(r, act):
        act(swap(sp, r))

        @pl.when(bridge_up)
        def _():
            act(cross(r))

        spread(z, r, has_up, act)

    mate_level = z + 1 - 2 * a

    def send_mate(r, act):
        spread(mate_level, r, bridge_up, act)

    def send_below(level, r, act):
        spread(level, r, has_up, act)

    def relay_mate(r):
        swap(mate, r).wait_recv()
        send_mate(r, start)

    def relay_below(level, r):
        kv_wait(level_block(level), r)
        send_below(level, r, start)

    own.wait()
    for load in loads[:3]:
        load.wait()
    scale = hd ** (-0.5)

    def chunk(r, carry):
        rows = tok_rows(r)
        for k in range(1, X):
            tok_wait(source(k), r)
            tok_forward(k, r).start()
        tok_wait(sib, r)
        for k in range(1, X):
            tok_wait(source_sib(k), r)
        squares = jnp.zeros((R, 1), F32)
        for t in range(T):
            block = tok[t, rows, :].astype(F32)
            squares = squares + jnp.sum(block * block, axis=1, keepdims=True)
            scaled[rows, t * Dt : (t + 1) * Dt] = (block * gain[:, t * Dt : (t + 1) * Dt]).astype(BF16)
        inverse = lax.rsqrt(squares / Wd + NORM_EPS)
        inv[rows, :] = inverse
        left = scaled[rows, :]
        keys = inverse * dot(left, wk[...])
        values = inverse * dot(left, wv[...])
        queries = inverse * dot(left, wq[...])
        for h in range(H):
            mine = a if h else 1 - a
            slot = sp * mine + S * (1 - mine)
            cols = slice(h * V, (h + 1) * V)
            kvq[slot, r, 0] = rotate(keys[:, cols], rows).astype(BF16)
            kvq[slot, r, 1] = jnp.transpose(values[:, cols]).astype(BF16)
            turned = rotate(queries[:, cols], rows).astype(BF16).astype(F32) * scale
            kvq[slot, r, 2] = jnp.transpose(turned).astype(BF16)
        send_own(r, start)

        @pl.when(r > 0)
        def _():
            relay_mate(r - 1)

        return carry

    lax.fori_loop(0, NR, chunk, 0)
    relay_mate(NR - 1)

    def relay_some(dp, begin, end):
        @pl.when(dp <= pair)
        def _():
            for r in range(begin, end):
                for b in range(2):
                    relay_below(2 * (pair - dp) + b, r)

    relay_some(1, 0, G // 2)

    for load in loads[3:6]:
        load.wait()

    def mix_rows(r):
        return pl.ds(pl.multiple_of(r * M, M), M)

    def gate_chunk(r, carry):
        rows = mix_rows(r)
        inverse = inv[rows, :]
        left = scaled[rows, :]
        inner = (inverse * dot(left, wi[...])).astype(BF16)
        signal = (inverse * dot(left, ws[...])).astype(BF16)
        conv_in = (inner.astype(F32) * signal.astype(F32)).astype(BF16)
        padded[pl.ds(pl.multiple_of(PAD + r * M, PAD), M), :] = conv_in.astype(F32)
        gate[rows, :] = (inverse * dot(left, wo[...])).astype(BF16)
        return carry

    lax.fori_loop(0, NM, gate_chunk, 0)
    tail[...] = padded[L : L + PAD, :].astype(BF16)
    rim_copy = pltpu.make_async_remote_copy(
        src_ref=tail,
        dst_ref=rim,
        send_sem=rim_sem.at[0],
        recv_sem=rim_sem.at[1],
        device_id={"sp": (sp + 1) % S},
    )

    @pl.when(sp + 1 < S)
    def _():
        rim_copy.start()

    relay_some(1, G // 2, G)

    key_row = lax.broadcasted_iota(jnp.int32, (M, M), 0)
    query_lane = lax.broadcasted_iota(jnp.int32, (M, M), 1)
    blank = jnp.zeros((hd, M), BF16)

    def attend(j, half, tiles, diagonal=None):
        keys = jnp.concatenate([kvq[j, G * half + g, 0] for g in range(G)], axis=0)
        values = jnp.concatenate([kvq[j, G * half + g, 1] for g in range(G)], axis=1)
        for b, part in tiles:
            turned = jnp.concatenate(
                [kvq[level_block(2 * pair + b), G * part + g, 2] for g in range(G)], axis=1
            )
            for c in range(2):
                if c:
                    right = jnp.concatenate([blank, turned[hd:]], axis=0)
                else:
                    right = jnp.concatenate([turned[:hd], blank], axis=0)
                scores = dot(keys, right)
                if (b, part) == diagonal:
                    scores = jnp.where(key_row <= query_lane, scores, MASKED)
                old_max = row_max[b, part, c]
                new_max = jnp.maximum(old_max, jnp.max(scores, axis=0, keepdims=True))
                weights = jnp.exp(scores - new_max)
                fade = jnp.exp(old_max - new_max)
                row_max[b, part, c] = new_max
                row_sum[b, part, c] = fade * row_sum[b, part, c] + jnp.sum(weights, axis=0, keepdims=True)
                acc[b, part, c] = fade * acc[b, part, c] + dot(values, weights.astype(BF16))

    every = [(b, part) for b in range(2) for part in range(NM)]
    for b in range(2):
        for half in range(NM):
            tiles = [(i, part) for i, part in every if (i, part) >= (b, half)]
            attend(level_block(2 * pair + b), half, tiles, (b, half))

    @pl.when(sp > 0)
    def _():
        rim_copy.wait_recv()
        padded[0:PAD, :] = rim[...].astype(F32)

    @pl.when(sp == 0)
    def _():
        padded[0:PAD, :] = jnp.zeros((PAD, C), F32)

    summed = jnp.zeros((L, C), F32)
    for j in range(taps_n):
        begin = PAD - (taps_n - 1) + j
        summed = summed + taps[j : j + 1, :] * padded[begin : begin + L, :]
    conv_all[tp, :, :] = (gate[...].astype(F32) * summed).astype(BF16)

    def mix_copy(piece, r, send, target):
        block = conv_all.at[piece, mix_rows(r), :]
        return pltpu.make_async_remote_copy(
            src_ref=block,
            dst_ref=block,
            send_sem=send,
            recv_sem=mix_recv.at[piece, r],
            device_id={"tp": target},
        )

    def mix_own(k, r):
        return mix_copy(tp, r, mix_send.at[k, r], peer(k) if k else sib)

    def mix_forward(k, r):
        return mix_copy(source(k), r, mix_relay.at[k, r], sib)

    def mix_wait(piece, r):
        mix_copy(piece, r, mix_send.at[0, r], sib).wait_recv()

    for r in range(NM):
        for k in list(range(1, X)) + [0]:
            mix_own(k, r).start()

    for k in range(1, Y):
        other = (y + k) % Y
        ahead = other < y
        low = 2 * pair * Y + other
        for r in range(NR):
            kv_wait(low, r)

        @pl.when(ahead)
        def _():
            for r in range(NR):
                kv_wait(low + Y, r)

        def beside(i, carry):
            item = i // NM
            half = i % NM
            high = (item == 2).astype(jnp.int32)
            late = 1 - (item == 1).astype(jnp.int32)
            attend(low + high * Y, half, [(late, part) for part in range(NM)])
            return carry

        lax.fori_loop(0, NM * jnp.where(ahead, 3, 1), beside, 0)

    def below(dp, carry):
        def half_step(half, inner):
            last = half == NM - 1
            next_dp = dp + last.astype(jnp.int32)
            next_r = G * ((half + 1) % NM)

            def relay_next(g):
                @pl.when(next_dp <= pair)
                def _():
                    for b in range(2):
                        relay_below(2 * (pair - next_dp) + b, next_r + g)

            def item(i, c):
                k = i // 2
                j = (2 * (pair - dp) + i % 2) * Y + (y + k) % Y

                @pl.when(i == 2)
                def _():
                    for g in range(G // 2):
                        relay_next(g)

                @pl.when(k > 0)
                def _():
                    for g in range(G):
                        kv_wait(j, G * half + g)

                attend(j, half, every)
                return c

            lax.fori_loop(0, 2 * Y, item, 0)
            for g in range(G // 2, G):
                relay_next(g)
            return inner

        return lax.fori_loop(0, NM, half_step, carry)

    lax.fori_loop(1, pair + 1, below, 0)

    def at_copy(src, piece, h, r, send, target):
        return pltpu.make_async_remote_copy(
            src_ref=src,
            dst_ref=attn_all.at[piece, h, mix_rows(r), :],
            send_sem=send,
            recv_sem=at_recv.at[piece, h, r],
            device_id=target,
        )

    def at_own(k, r):
        target = {"tp": peer(k) if k else sib}
        return at_copy(attn_all.at[tp, a, mix_rows(r), :], tp, a, r, at_send.at[k, r], target)

    def at_off(k, r):
        target = {"sp": mate, "tp": peer(k)}
        return at_copy(away.at[mix_rows(r), :], tp, a, r, at_away.at[k, r], target)

    def at_forward(k, h, r, send):
        piece = source(k)
        return at_copy(attn_all.at[piece, h, mix_rows(r), :], piece, h, r, send, {"tp": sib})

    def at_wait(piece, h, r):
        at_copy(attn_all.at[piece, h, mix_rows(r), :], piece, h, r, at_send.at[0, r], {"tp": sib}).wait_recv()

    def near_forward(k, r):
        return at_forward(k, a, r, at_relay.at[k, r])

    def far_forward(k, r):
        return at_forward(k, 1 - a, r, at_relay_away.at[k, r])

    def finished(b, part):
        first_map = acc[b, part, 0] / row_sum[b, part, 0]
        second_map = acc[b, part, 1] / row_sum[b, part, 1]
        head_mix = first_map - lambdas[a] * second_map
        mean = jnp.mean(head_mix * head_mix, axis=0, keepdims=True)
        normed = head_mix * lax.rsqrt(mean + HEAD_EPS) * head_gain[...] * HEAD_SCALE
        return jnp.transpose(normed).astype(BF16)

    def log_total(b, part, c):
        return row_max[b, part, c] + jnp.log(row_sum[b, part, c])

    for part in range(NM):
        away[part * M : (part + 1) * M, :] = finished(1 - a, part)
        for k in list(range(1, X)) + [0]:
            at_off(k, part).start()
    for part in range(NM):
        attn_all[tp, a, part * M : (part + 1) * M, :] = finished(a, part)
        for k in list(range(1, X)) + [0]:
            at_own(k, part).start()
    for part in range(NM):
        for c in range(2):
            lse_away[c : c + 1, part * M : (part + 1) * M] = log_total(1 - a, part, c)
            lse[a, c : c + 1, part * M : (part + 1) * M] = log_total(a, part, c)
    lse_copy = pltpu.make_async_remote_copy(
        src_ref=lse_away,
        dst_ref=lse_in,
        send_sem=lse_sem.at[0],
        recv_sem=lse_sem.at[1],
        device_id={"sp": mate},
    )
    lse_copy.start()

    loads[6].wait()
    loads[7].wait()

    def conv_part(r, carry):
        rows = mix_rows(r)
        for k in range(1, X):
            mix_wait(source(k), r)
            mix_forward(k, r).start()
        mix_wait(sib, r)
        for k in range(1, X):
            mix_wait(source_sib(k), r)
        part = dot(conv_all[0, rows, :], wc[0:C, :])
        for t in range(1, T):
            part = part + dot(conv_all[t, rows, :], wc[t * C : (t + 1) * C, :])
        total[rows, :] = part
        return carry

    lax.fori_loop(0, NM, conv_part, 0)

    for r in range(NM):
        for k in range(1, X):
            at_wait(source(k), a, r)
            near_forward(k, r).start()

    def attn_part(r, carry):
        rows = mix_rows(r)
        for k in range(X):
            at_wait(source(k), 1 - a, r)
            far_forward(k, r).start()
        for k in range(X):
            at_wait(source_sib(k), a, r)
        for k in range(X):
            at_wait(source_sib(k), 1 - a, r)
        part = total[rows, :]
        for t in range(T):
            both = jnp.concatenate([attn_all[t, h, rows, :] for h in range(H)], axis=1)
            part = part + dot(both, wa[t * C : (t + 1) * C, :])
        out[rows, :] = part.astype(BF16)
        return carry

    lax.fori_loop(0, NM, attn_part, 0)
    lse_copy.wait_recv()
    lse[1 - a] = lse_in[...]
    lse_copy.wait_send()

    for r in range(NR):
        for k in range(X):
            tok_own(k, r).wait_send()
        for k in range(1, X):
            tok_forward(k, r).wait_send()
        send_own(r, drain)
        send_mate(r, drain)

    def drain_level(level, carry):
        for r in range(NR):
            send_below(level, r, drain)
        return carry

    lax.fori_loop(0, 2 * pair, drain_level, 0)

    for r in range(NM):
        for k in range(X):
            mix_own(k, r).wait_send()
            at_own(k, r).wait_send()
            at_off(k, r).wait_send()
            far_forward(k, r).wait_send()
        for k in range(1, X):
            mix_forward(k, r).wait_send()
            near_forward(k, r).wait_send()

    @pl.when(sp + 1 < S)
    def _():
        rim_copy.wait_send()


def pair_device(
    dims,
    tokens,
    norm_gain,
    query_weight,
    key_weight,
    value_weight,
    outer_gate_weight,
    inner_gate_weight,
    conv_input_weight,
    conv_taps,
    lambdas,
    head_gain,
    attn_out_weight,
    conv_out_weight,
):
    S, T, Z, Y = dims["S"], dims["T"], dims["Z"], dims["Y"]
    L, Dt = tokens.shape
    H = lambdas.shape[0]
    C = query_weight.shape[1]
    V = C // H
    hd = V // 2
    O = attn_out_weight.shape[1]
    Wd = norm_gain.shape[0]
    R = V
    M = 2 * R
    NR, NM, PAD = L // R, L // M, 16
    X = T // 2
    frequency = ROPE_BASE ** (-np.arange(hd // 2) * 2.0 / hd)
    freq = jnp.asarray(np.tile(frequency, 4)[None, :], F32)
    any_spec = pl.BlockSpec(memory_space=pl.ANY)
    vmem = pl.BlockSpec(memory_space=pltpu.VMEM)
    smem = pl.BlockSpec(memory_space=pltpu.SMEM)
    dma = pltpu.SemaphoreType.DMA
    mixed, lse = pl.pallas_call(
        functools.partial(pair_kernel, dict(dims, H=H)),
        out_shape=(
            jax.ShapeDtypeStruct((L, O), BF16),
            jax.ShapeDtypeStruct((H, 2, L), F32),
        ),
        in_specs=[any_spec, vmem, vmem] + [any_spec] * 6 + [vmem, smem, vmem] + [any_spec] * 2,
        out_specs=(vmem, vmem),
        scratch_shapes=[
            pltpu.VMEM((T, L, Dt), BF16),
            pltpu.VMEM((L, Wd), BF16),
            pltpu.VMEM((L, 1), F32),
            pltpu.VMEM((L, V), F32),
            pltpu.VMEM((L, V), F32),
        ]
        + [pltpu.VMEM((Wd, C), BF16)] * 6
        + [pltpu.VMEM((T * C, O), BF16)] * 2
        + [
            pltpu.VMEM((S + 1, NR, 3, R, V), BF16),
            pltpu.VMEM((2, NM, 2, 1, M), F32),
            pltpu.VMEM((2, NM, 2, 1, M), F32),
            pltpu.VMEM((2, NM, 2, V, M), F32),
            pltpu.VMEM((L, C), BF16),
            pltpu.VMEM((PAD + L, C), F32),
            pltpu.VMEM((PAD, C), BF16),
            pltpu.VMEM((PAD, C), BF16),
            pltpu.VMEM((T, L, C), BF16),
            pltpu.VMEM((T, H, L, V), BF16),
            pltpu.VMEM((L, V), BF16),
            pltpu.VMEM((2, L), F32),
            pltpu.VMEM((2, L), F32),
            pltpu.VMEM((L, O), F32),
            dma((8,)),
            dma,
            dma((T, NR)),
            dma((X, NR)),
            dma((X, NR)),
            dma((S, NR)),
            dma((NR,)),
            dma((NR,)),
            dma((Z, NR, max(Y - 1, 1))),
            dma((Z, NR)),
            dma((2,)),
            dma((2,)),
            dma((T, NM)),
            dma((X, NM)),
            dma((X, NM)),
            dma((T, H, NM)),
            dma((X, NM)),
            dma((X, NM)),
            dma((X, NM)),
            dma((X, NM)),
        ],
        compiler_params=pltpu.CompilerParams(
            collective_id=0, has_side_effects=True, vmem_limit_bytes=60 * 1024 * 1024
        ),
        name="mixer",
    )(
        tokens,
        norm_gain[None, :],
        freq,
        query_weight,
        key_weight,
        value_weight,
        outer_gate_weight,
        inner_gate_weight,
        conv_input_weight,
        conv_taps,
        lambdas,
        head_gain[:, None],
        attn_out_weight,
        conv_out_weight,
    )
    return mixed, lse


def per_device(dims, *arrays):
    tokens, query_weight, lambdas = arrays[0], arrays[2], arrays[9]
    width = query_weight.shape[1] // lambdas.shape[0]
    paired = lambdas.shape[0] == 2 and dims["Z"] % 2 == 0 and dims["T"] % 2 == 0
    paired = paired and width == 128 and tokens.shape[0] % (2 * width) == 0
    return (pair_device if paired else ring_device)(dims, *arrays)


def solution(mesh):
    S, T = mesh.shape["sp"], mesh.shape["tp"]
    Y = max(d for d in range(1, S + 1) if S % d == 0 and d * d <= S)
    dims = {"S": S, "T": T, "Z": S // Y, "Y": Y}
    in_specs = (
        P("sp", "tp"),
        P(),
        P(None, "tp"),
        P(None, "tp"),
        P(None, "tp"),
        P(None, "tp"),
        P(None, "tp"),
        P(None, "tp"),
        P(None, "tp"),
        P("tp"),
        P(),
        P(None, "tp"),
        P(None, "tp"),
    )
    out_specs = (P("sp", "tp"), P("tp", None, "sp"))
    return jax.shard_map(
        functools.partial(per_device, dims),
        mesh=mesh,
        in_specs=in_specs,
        out_specs=out_specs,
        check_vma=False,
    )
```

```python
import functools

import jax
import jax.numpy as jnp
import numpy as np
from jax import lax
from jax.experimental import pallas as pl
from jax.experimental.pallas import tpu as pltpu
from jax.sharding import PartitionSpec as P

NORM_EPS = 1e-06
HEAD_EPS = 1e-05
ROPE_BASE = 500000.0
MASKED = -1e30
HEAD_SCALE = 0.8
F32 = jnp.float32
BF16 = jnp.bfloat16


def dot(a, b):
    return jnp.dot(a, b, preferred_element_type=F32)


def dot_t(a, b):
    return lax.dot_general(a, b, (((1,), (1,)), ((), ())), preferred_element_type=F32)


def ring_kernel(
    dims,
    tokens,
    gain,
    freq,
    wq_h,
    wk_h,
    wv_h,
    wo_h,
    wi_h,
    ws_h,
    taps,
    lambdas,
    head_gain,
    wa_h,
    wc_h,
    out,
    lse,
    tok,
    scaled,
    inv,
    cos_t,
    sin_t,
    wq,
    wk,
    wv,
    wo,
    wi,
    ws,
    wa,
    wc,
    kv,
    qz,
    row_max,
    row_sum,
    acc,
    gate,
    padded,
    tail,
    rim,
    conv_all,
    attn_all,
    total,
    w_sem,
    own_sem,
    tok_recv,
    tok_send,
    tok_relay,
    kv_recv,
    kv_send_z,
    kv_send_y,
    kv_extra,
    rim_sem,
    mix_recv,
    mix_send,
    mix_relay,
):
    S, T, Z, Y, H = dims["S"], dims["T"], dims["Z"], dims["Y"], dims["H"]
    L, Dt = tokens.shape
    Wd = T * Dt
    C = wq_h.shape[1]
    V = C // H
    hd = V // 2
    NR = tok_recv.shape[1]
    R = L // NR
    NM = mix_recv.shape[2]
    M = L // NM
    X = T // 2
    taps_n = taps.shape[0]
    PAD = tail.shape[0]

    sp = lax.axis_index("sp")
    tp = lax.axis_index("tp")
    z = sp // Y
    y = sp % Y
    core = tp % 2
    xi = tp // 2
    sib = xi * 2 + (1 - core)

    def peer(k):
        return ((xi + k) % X) * 2 + core

    def source(k):
        return ((xi - k + X) % X) * 2 + core

    pairs = [(wk_h, wk), (wv_h, wv), (wq_h, wq), (wi_h, wi), (ws_h, ws), (wo_h, wo), (wc_h, wc), (wa_h, wa)]
    own = pltpu.make_async_copy(tokens, tok.at[tp], own_sem)
    own.start()
    loads = [pltpu.make_async_copy(s, d, w_sem.at[i]) for i, (s, d) in enumerate(pairs)]
    for load in loads:
        load.start()

    barrier = pltpu.get_barrier_semaphore()

    def greet(target):
        pl.semaphore_signal(barrier, inc=1, device_id=target)

    for k in range(1, T):
        greet({"tp": (tp + k) % T})
    for k in range(1, Y):
        greet({"sp": z * Y + (y + k) % Y})
    has_up = z + 1 < Z
    has_down = z > 0
    far_up = jnp.logical_and(has_up, y == Y - 1) if Y > 1 else None
    far_down = jnp.logical_and(has_down, y == 0) if Y > 1 else None
    expect = (T - 1) + (Y - 1) + has_up.astype(jnp.int32) + has_down.astype(jnp.int32)

    @pl.when(has_up)
    def _():
        greet({"sp": sp + Y})

    @pl.when(has_down)
    def _():
        greet({"sp": sp - Y})

    if Y > 1:
        expect = expect + far_up.astype(jnp.int32) + far_down.astype(jnp.int32)

        @pl.when(far_up)
        def _():
            greet({"sp": sp + 1})

        @pl.when(far_down)
        def _():
            greet({"sp": sp - 1})

    pl.semaphore_wait(barrier, expect)

    def tok_rows(r):
        return pl.ds(pl.multiple_of(r * R, R), R)

    def tok_copy(src, piece, r, send, target):
        return pltpu.make_async_remote_copy(
            src_ref=src,
            dst_ref=tok.at[piece, tok_rows(r), :],
            send_sem=send,
            recv_sem=tok_recv.at[piece, r],
            device_id={"tp": target},
        )

    def tok_own(k, r):
        target = peer(k) if k else sib
        return tok_copy(tokens.at[tok_rows(r), :], tp, r, tok_send.at[k, r], target)

    def tok_forward(k, r):
        piece = source(k)
        return tok_copy(tok.at[piece, tok_rows(r), :], piece, r, tok_relay.at[k, r], sib)

    def tok_wait(piece, r):
        tok_copy(tok.at[piece, tok_rows(r), :], piece, r, tok_send.at[0, r], sib).wait_recv()

    for r in range(NR):
        for k in list(range(1, X)) + [0]:
            tok_own(k, r).start()

    lane = lax.broadcasted_iota(jnp.int32, (R, V), 1)
    first = (lane % hd) < (hd // 2)

    def table(r, carry):
        base = sp * L + r * R
        pos = (base + lax.broadcasted_iota(jnp.int32, (R, V), 0)).astype(F32)
        angle = pos * freq[...]
        sine = jnp.sin(angle)
        cos_t[tok_rows(r), :] = jnp.cos(angle)
        sin_t[tok_rows(r), :] = jnp.where(first, -sine, sine)
        return carry

    lax.fori_loop(0, NR, table, 0)

    def rotate(block, rows):
        low = (lax.broadcasted_iota(jnp.int32, block.shape, 1) % hd) < (hd // 2)
        other = jnp.where(
            low, pltpu.roll(block, V - hd // 2, 1), pltpu.roll(block, hd // 2, 1)
        )
        return block * cos_t[rows, :] + other * sin_t[rows, :]

    def kv_copy(j, r, send, target):
        block = kv.at[j, tok_rows(r), :]
        return pltpu.make_async_remote_copy(
            src_ref=block,
            dst_ref=block,
            send_sem=send,
            recv_sem=kv_recv.at[j, r],
            device_id={"sp": target},
        )

    def kv_up(dz, r):
        return kv_copy(sp - dz * Y, r, kv_send_z.at[dz, r], sp + Y)

    def kv_side(dz, r, k):
        return kv_copy(sp - dz * Y, r, kv_send_y.at[dz, r, k - 1], z * Y + (y + k) % Y)

    def kv_wait(j, r):
        kv_copy(j, r, kv_send_z.at[0, r], sp).wait_recv()

    EX = NR // 2 if Y == 2 else 0

    def extra(r):
        return kv_copy(0, r, kv_extra.at[r], sp + Y)

    def kv_send(dz, r, act):
        @pl.when(has_up)
        def _():
            act(kv_up(dz, r))

        for k in range(1, Y):
            wanted = jnp.logical_or(dz > 0, y + k < Y)
            if EX:
                other_way = jnp.logical_and(dz == z, jnp.logical_and(dz > 0, r < EX))
                wanted = jnp.logical_and(wanted, jnp.logical_not(jnp.logical_and(y == 0, other_way)))

            @pl.when(wanted)
            def _():
                act(kv_side(dz, r, k))

    def relay(dz, r):
        @pl.when(dz <= z)
        def _():
            kv_wait(sp - dz * Y, r)
            kv_send(dz, r, lambda copy: copy.start())

    def first_relay(r):
        relay(1, r)
        if EX:

            @pl.when(jnp.logical_and(jnp.logical_and(z == 0, y == 1), r < EX))
            def _():
                kv_wait(0, r)

                @pl.when(has_up)
                def _():
                    extra(r).start()

    own.wait()
    loads[0].wait()
    loads[1].wait()

    def key_chunk(r, carry):
        rows = tok_rows(r)
        for k in range(1, X):
            tok_wait(source(k), r)
            tok_forward(k, r).start()
        tok_wait(sib, r)
        for k in range(1, X):
            tok_wait(((xi + k) % X) * 2 + (1 - core), r)
        squares = jnp.zeros((R, 1), F32)
        for t in range(T):
            block = tok[t, rows, :].astype(F32)
            squares = squares + jnp.sum(block * block, axis=1, keepdims=True)
            scaled[rows, t * Dt : (t + 1) * Dt] = (block * gain[:, t * Dt : (t + 1) * Dt]).astype(BF16)
        inverse = lax.rsqrt(squares / Wd + NORM_EPS)
        inv[rows, :] = inverse
        left = scaled[rows, :]
        keys = inverse * dot(left, wk[...])
        for h in range(H):
            kv[sp, rows, h * V : (h + 1) * V] = rotate(keys[:, h * V : (h + 1) * V], rows).astype(BF16)
        kv[sp, rows, C : 2 * C] = (inverse * dot(left, wv[...])).astype(BF16)
        kv_send(0, r, lambda copy: copy.start())

        @pl.when(r > 0)
        def _():
            first_relay(r - 1)

        return carry

    lax.fori_loop(0, NR, key_chunk, 0)

    for load in loads[2:6]:
        load.wait()
    half = lax.broadcasted_iota(jnp.int32, (M, V), 1) < hd
    scale = hd ** (-0.5)

    def mix_rows(r):
        return pl.ds(pl.multiple_of(r * M, M), M)

    def query_chunk(r, carry):
        rows = mix_rows(r)
        inverse = inv[rows, :]
        left = scaled[rows, :]
        queries = inverse * dot(left, wq[...])
        for h in range(H):
            turned = rotate(queries[:, h * V : (h + 1) * V], rows).astype(BF16).astype(F32) * scale
            qz[h, 0, rows, :] = jnp.where(half, turned, 0.0).astype(BF16)
            qz[h, 1, rows, :] = jnp.where(half, 0.0, turned).astype(BF16)
        inner = (inverse * dot(left, wi[...])).astype(BF16)
        signal = (inverse * dot(left, ws[...])).astype(BF16)
        conv_in = (inner.astype(F32) * signal.astype(F32)).astype(BF16)
        padded[pl.ds(pl.multiple_of(PAD + r * M, PAD), M), :] = conv_in.astype(F32)
        gate[rows, :] = (inverse * dot(left, wo[...])).astype(BF16)

        @pl.when(r == 0)
        def _():
            first_relay(NR - 1)

        return carry

    lax.fori_loop(0, NM, query_chunk, 0)
    tail[...] = padded[L : L + PAD, :].astype(BF16)
    rim_copy = pltpu.make_async_remote_copy(
        src_ref=tail,
        dst_ref=rim,
        send_sem=rim_sem.at[0],
        recv_sem=rim_sem.at[1],
        device_id={"sp": (sp + 1) % S},
    )

    @pl.when(sp + 1 < S)
    def _():
        rim_copy.start()

    def attend(j, diagonal):
        def one(i, carry):
            rows = mix_rows(i)
            for h in range(H):
                query = qz[h, :, rows, :].reshape(2 * M, V)
                scores = dot_t(query, kv[j, :, h * V : (h + 1) * V])
                if diagonal:
                    row = lax.broadcasted_iota(jnp.int32, scores.shape, 0)
                    row = jnp.where(row >= M, row - M, row) + i * M
                    col = lax.broadcasted_iota(jnp.int32, scores.shape, 1)
                    scores = jnp.where(row >= col, scores, MASKED)
                    new_max = jnp.max(scores, axis=1, keepdims=True)
                else:
                    old_max = row_max[h, :, rows, :].reshape(2 * M, 1)
                    new_max = jnp.maximum(old_max, jnp.max(scores, axis=1, keepdims=True))
                weights = jnp.exp(scores - new_max)
                sums = jnp.sum(weights, axis=1, keepdims=True)
                mixed = dot(weights.astype(BF16), kv[j, :, C + h * V : C + (h + 1) * V])
                if not diagonal:
                    fade = jnp.exp(old_max - new_max)
                    sums = sums + fade * row_sum[h, :, rows, :].reshape(2 * M, 1)
                    mixed = mixed + fade * acc[h, :, rows, :].reshape(2 * M, V)
                row_max[h, :, rows, :] = new_max.reshape(2, M, 1)
                row_sum[h, :, rows, :] = sums.reshape(2, M, 1)
                acc[h, :, rows, :] = mixed.reshape(2, M, V)
            return carry

        lax.fori_loop(0, NM, one, 0)

    attend(sp, True)

    @pl.when(sp > 0)
    def _():
        rim_copy.wait_recv()
        padded[0:PAD, :] = rim[...].astype(F32)

    @pl.when(sp == 0)
    def _():
        padded[0:PAD, :] = jnp.zeros((PAD, C), F32)

    summed = jnp.zeros((L, C), F32)
    for j in range(taps_n):
        begin = PAD - (taps_n - 1) + j
        summed = summed + taps[j : j + 1, :] * padded[begin : begin + L, :]
    conv_all[tp, :, :] = (gate[...].astype(F32) * summed).astype(BF16)

    def mix_copy(which, buf, piece, r, send, target):
        block = buf.at[piece, mix_rows(r), :]
        return pltpu.make_async_remote_copy(
            src_ref=block,
            dst_ref=block,
            send_sem=send,
            recv_sem=mix_recv.at[which, piece, r],
            device_id={"tp": target},
        )

    def mix_own(which, buf, k, r):
        target = peer(k) if k else sib
        return mix_copy(which, buf, tp, r, mix_send.at[which, k, r], target)

    def mix_forward(which, buf, k, r):
        return mix_copy(which, buf, source(k), r, mix_relay.at[which, k, r], sib)

    def mix_wait(which, buf, piece, r):
        mix_copy(which, buf, piece, r, mix_send.at[which, 0, r], sib).wait_recv()

    for r in range(NM):
        for k in list(range(1, X)) + [0]:
            mix_own(0, conv_all, k, r).start()

    def step(dz, carry):
        def row_block(k, inner):
            def forward(r, c):
                relay(dz + 1, r)
                return c

            lax.fori_loop(k * NR // Y, (k + 1) * NR // Y, forward, 0)
            side = (y + k) % Y
            level = jnp.where(k == 0, z - dz, z - dz + 1)
            j = level * Y + side
            valid = jnp.where(k == 0, dz <= z, jnp.logical_or(level < z, side < y))

            @pl.when(valid)
            def _():
                @pl.when(k > 0)
                def _():
                    for r in range(NR):
                        if r < EX:
                            climbs = jnp.logical_and(level == 0, y == 1)

                            @pl.when(jnp.logical_not(jnp.logical_and(climbs, z == 0)))
                            def _():
                                kv_wait(j, r)

                            @pl.when(jnp.logical_and(climbs, jnp.logical_and(z > 0, has_up)))
                            def _():
                                extra(r).start()

                        else:
                            kv_wait(j, r)

                attend(j, False)

            return inner

        lax.fori_loop(0, Y, row_block, 0)
        return carry

    lax.fori_loop(1, z + 2, step, 0)

    def finish(i, carry):
        rows = mix_rows(i)
        for h in range(H):
            first_map = acc[h, 0, rows, :] / row_sum[h, 0, rows, :]
            second_map = acc[h, 1, rows, :] / row_sum[h, 1, rows, :]
            head_mix = first_map - lambdas[h] * second_map
            mean = jnp.mean(head_mix * head_mix, axis=1, keepdims=True)
            normed = head_mix * lax.rsqrt(mean + HEAD_EPS) * head_gain[...] * HEAD_SCALE
            attn_all[tp, rows, h * V : (h + 1) * V] = normed.astype(BF16)
        for k in list(range(1, X)) + [0]:
            mix_own(1, attn_all, k, i).start()
        return carry

    lax.fori_loop(0, NM, finish, 0)

    loads[6].wait()
    loads[7].wait()

    def gather(which, buf, r):
        for k in range(1, X):
            mix_wait(which, buf, source(k), r)
            mix_forward(which, buf, k, r).start()

    def gather_rest(which, buf, r):
        mix_wait(which, buf, sib, r)
        for k in range(1, X):
            mix_wait(which, buf, ((xi + k) % X) * 2 + (1 - core), r)

    def conv_part(r, carry):
        rows = mix_rows(r)
        gather(0, conv_all, r)
        gather_rest(0, conv_all, r)
        part = dot(conv_all[0, rows, :], wc[0:C, :])
        for t in range(1, T):
            part = part + dot(conv_all[t, rows, :], wc[t * C : (t + 1) * C, :])
        total[rows, :] = part
        return carry

    lax.fori_loop(0, NM, conv_part, 0)

    lanes = lax.broadcasted_iota(jnp.int32, (L, 128), 1)
    columns = jnp.zeros((L, 128), F32)
    for h in range(H):
        for c in range(2):
            value = row_max[h, c, :, :] + jnp.log(row_sum[h, c, :, :])
            columns = jnp.where(lanes == 2 * h + c, value, columns)
    turned_columns = jnp.transpose(columns)
    for h in range(H):
        lse[h] = turned_columns[2 * h : 2 * h + 2, :]

    def attn_part(r, carry):
        rows = mix_rows(r)
        gather(1, attn_all, r)
        gather_rest(1, attn_all, r)
        part = total[rows, :]
        for t in range(T):
            part = part + dot(attn_all[t, rows, :], wa[t * C : (t + 1) * C, :])
        out[rows, :] = part.astype(BF16)
        return carry

    lax.fori_loop(0, NM, attn_part, 0)

    for r in range(NR):
        for k in range(X):
            tok_own(k, r).wait_send()
        for k in range(1, X):
            tok_forward(k, r).wait_send()

    def drain(dz, carry):
        def inner(r, c):
            kv_send(dz, r, lambda copy: copy.wait_send())
            return c

        return lax.fori_loop(0, NR, inner, carry)

    lax.fori_loop(0, z + 1, drain, 0)
    if EX:

        @pl.when(jnp.logical_and(y == 1, has_up))
        def _():
            for r in range(EX):
                extra(r).wait_send()

    for which, buf in ((0, conv_all), (1, attn_all)):
        for r in range(NM):
            for k in range(X):
                mix_own(which, buf, k, r).wait_send()
            for k in range(1, X):
                mix_forward(which, buf, k, r).wait_send()

    @pl.when(sp + 1 < S)
    def _():
        rim_copy.wait_send()


def ring_device(
    dims,
    tokens,
    norm_gain,
    query_weight,
    key_weight,
    value_weight,
    outer_gate_weight,
    inner_gate_weight,
    conv_input_weight,
    conv_taps,
    lambdas,
    head_gain,
    attn_out_weight,
    conv_out_weight,
):
    S, T, Z, Y = dims["S"], dims["T"], dims["Z"], dims["Y"]
    L, Dt = tokens.shape
    H = lambdas.shape[0]
    C = query_weight.shape[1]
    V = C // H
    hd = V // 2
    O = attn_out_weight.shape[1]
    Wd = norm_gain.shape[0]
    NR, NM, PAD = 4, 2, 16
    X = T // 2
    frequency = ROPE_BASE ** (-np.arange(hd // 2) * 2.0 / hd)
    freq = jnp.asarray(np.tile(frequency, 4)[None, :], F32)
    any_spec = pl.BlockSpec(memory_space=pl.ANY)
    vmem = pl.BlockSpec(memory_space=pltpu.VMEM)
    smem = pl.BlockSpec(memory_space=pltpu.SMEM)
    dma = pltpu.SemaphoreType.DMA
    mixed, lse = pl.pallas_call(
        functools.partial(ring_kernel, dict(dims, H=H)),
        out_shape=(
            jax.ShapeDtypeStruct((L, O), BF16),
            jax.ShapeDtypeStruct((H, 2, L), F32),
        ),
        in_specs=[any_spec, vmem, vmem] + [any_spec] * 6 + [vmem, smem, vmem] + [any_spec] * 2,
        out_specs=(vmem, vmem),
        scratch_shapes=[
            pltpu.VMEM((T, L, Dt), BF16),
            pltpu.VMEM((L, Wd), BF16),
            pltpu.VMEM((L, 1), F32),
            pltpu.VMEM((L, V), F32),
            pltpu.VMEM((L, V), F32),
        ]
        + [pltpu.VMEM((Wd, C), BF16)] * 6
        + [pltpu.VMEM((T * C, O), BF16)] * 2
        + [
            pltpu.VMEM((S, L, 2 * C), BF16),
            pltpu.VMEM((H, 2, L, V), BF16),
            pltpu.VMEM((H, 2, L, 1), F32),
            pltpu.VMEM((H, 2, L, 1), F32),
            pltpu.VMEM((H, 2, L, V), F32),
            pltpu.VMEM((L, C), BF16),
            pltpu.VMEM((PAD + L, C), F32),
            pltpu.VMEM((PAD, C), BF16),
            pltpu.VMEM((PAD, C), BF16),
            pltpu.VMEM((T, L, C), BF16),
            pltpu.VMEM((T, L, C), BF16),
            pltpu.VMEM((L, O), F32),
            dma((8,)),
            dma,
            dma((T, NR)),
            dma((X, NR)),
            dma((X, NR)),
            dma((S, NR)),
            dma((Z, NR)),
            dma((Z, NR, max(Y - 1, 1))),
            dma((NR,)),
            dma((2,)),
            dma((2, T, NM)),
            dma((2, X, NM)),
            dma((2, X, NM)),
        ],
        compiler_params=pltpu.CompilerParams(
            collective_id=0, has_side_effects=True, vmem_limit_bytes=60 * 1024 * 1024
        ),
        name="mixer",
    )(
        tokens,
        norm_gain[None, :],
        freq,
        query_weight,
        key_weight,
        value_weight,
        outer_gate_weight,
        inner_gate_weight,
        conv_input_weight,
        conv_taps,
        lambdas,
        head_gain[None, :],
        attn_out_weight,
        conv_out_weight,
    )
    return mixed, lse


def pair_kernel(
    dims,
    tokens,
    gain,
    freq,
    wq_h,
    wk_h,
    wv_h,
    wo_h,
    wi_h,
    ws_h,
    taps,
    lambdas,
    head_gain,
    wa_h,
    wc_h,
    out,
    lse,
    tok,
    scaled,
    inv,
    cos_t,
    sin_t,
    wq,
    wk,
    wv,
    wo,
    wi,
    ws,
    wa,
    wc,
    kvq,
    row_max,
    row_sum,
    acc,
    gate,
    padded,
    tail,
    rim,
    conv_all,
    attn_all,
    away,
    lse_away,
    lse_in,
    total,
    w_sem,
    own_sem,
    tok_recv,
    tok_send,
    tok_relay,
    kv_recv,
    swap_send,
    cross_send,
    side_send,
    up_send,
    rim_sem,
    lse_sem,
    mix_recv,
    mix_send,
    mix_relay,
    at_recv,
    at_send,
    at_away,
    at_relay,
    at_relay_away,
):
    S, T, Z, Y, H = dims["S"], dims["T"], dims["Z"], dims["Y"], dims["H"]
    L, Dt = tokens.shape
    Wd = T * Dt
    C = wq_h.shape[1]
    V = C // H
    hd = V // 2
    NR = tok_recv.shape[1]
    R = L // NR
    NM = mix_recv.shape[1]
    M = L // NM
    G = M // R
    X = T // 2
    taps_n = taps.shape[0]
    PAD = tail.shape[0]

    sp = lax.axis_index("sp")
    tp = lax.axis_index("tp")
    z = sp // Y
    y = sp % Y
    pair = z // 2
    a = z % 2
    mate = sp + (1 - 2 * a) * Y
    core = tp % 2
    xi = tp // 2
    sib = xi * 2 + (1 - core)
    has_up = z + 2 - a < Z
    has_down = pair > 0

    def peer(k):
        return ((xi + k) % X) * 2 + core

    def source(k):
        return ((xi - k + X) % X) * 2 + core

    def source_sib(k):
        return ((xi - k + X) % X) * 2 + (1 - core)

    pairs = [(wk_h, wk), (wv_h, wv), (wq_h, wq), (wi_h, wi), (ws_h, ws), (wo_h, wo), (wc_h, wc), (wa_h, wa)]
    own = pltpu.make_async_copy(tokens, tok.at[tp], own_sem)
    own.start()
    loads = [pltpu.make_async_copy(s, d, w_sem.at[i]) for i, (s, d) in enumerate(pairs)]
    for load in loads:
        load.start()

    barrier = pltpu.get_barrier_semaphore()

    def greet(target):
        pl.semaphore_signal(barrier, inc=1, device_id=target)

    for k in range(1, T):
        greet({"tp": (tp + k) % T})
    for k in range(X):
        greet({"sp": mate, "tp": peer(k)})
    for k in range(1, Y):
        greet({"sp": z * Y + (y + k) % Y})
    expect = (T - 1) + X + (Y - 1)
    bridge_up = jnp.logical_and(a == 1, has_up)
    bridge_down = jnp.logical_and(a == 0, has_down)
    for near, step in (
        (has_up, 2 * Y),
        (has_down, -2 * Y),
        (bridge_up, Y),
        (bridge_down, -Y),
        (sp + 1 < S, 1),
        (sp > 0, -1),
    ):
        expect = expect + near.astype(jnp.int32)

        @pl.when(near)
        def _():
            greet({"sp": sp + step})

    pl.semaphore_wait(barrier, expect)

    def tok_rows(r):
        return pl.ds(pl.multiple_of(r * R, R), R)

    def tok_copy(src, piece, r, send, target):
        return pltpu.make_async_remote_copy(
            src_ref=src,
            dst_ref=tok.at[piece, tok_rows(r), :],
            send_sem=send,
            recv_sem=tok_recv.at[piece, r],
            device_id={"tp": target},
        )

    def tok_own(k, r):
        target = peer(k) if k else sib
        return tok_copy(tokens.at[tok_rows(r), :], tp, r, tok_send.at[k, r], target)

    def tok_forward(k, r):
        piece = source(k)
        return tok_copy(tok.at[piece, tok_rows(r), :], piece, r, tok_relay.at[k, r], sib)

    def tok_wait(piece, r):
        tok_copy(tok.at[piece, tok_rows(r), :], piece, r, tok_send.at[0, r], sib).wait_recv()

    for r in range(NR):
        for k in list(range(1, X)) + [0]:
            tok_own(k, r).start()

    lane = lax.broadcasted_iota(jnp.int32, (R, V), 1)
    first = (lane % hd) < (hd // 2)

    def table(r, carry):
        base = sp * L + r * R
        pos = (base + lax.broadcasted_iota(jnp.int32, (R, V), 0)).astype(F32)
        angle = pos * freq[...]
        sine = jnp.sin(angle)
        cos_t[tok_rows(r), :] = jnp.cos(angle)
        sin_t[tok_rows(r), :] = jnp.where(first, -sine, sine)
        return carry

    lax.fori_loop(0, NR, table, 0)

    row_max[...] = jnp.full(row_max.shape, MASKED, F32)
    row_sum[...] = jnp.zeros(row_sum.shape, F32)
    acc[...] = jnp.zeros(acc.shape, F32)

    def rotate(block, rows):
        other = jnp.where(first, pltpu.roll(block, V - hd // 2, 1), pltpu.roll(block, hd // 2, 1))
        return block * cos_t[rows, :] + other * sin_t[rows, :]

    def kv_copy(src, j, r, send, target):
        return pltpu.make_async_remote_copy(
            src_ref=src,
            dst_ref=kvq.at[j, r, pl.ds(0, 2)],
            send_sem=send,
            recv_sem=kv_recv.at[j, r],
            device_id={"sp": target},
        )

    def swap(j, r):
        return pltpu.make_async_remote_copy(
            src_ref=kvq.at[S, r],
            dst_ref=kvq.at[j, r],
            send_sem=swap_send.at[r],
            recv_sem=kv_recv.at[j, r],
            device_id={"sp": mate},
        )

    def cross(r):
        return kv_copy(kvq.at[S, r, pl.ds(0, 2)], sp, r, cross_send.at[r], sp + Y)

    def level_block(level):
        return level * Y + y

    def up(level, r):
        j = level_block(level)
        return kv_copy(kvq.at[j, r, pl.ds(0, 2)], j, r, up_send.at[level, r], sp + 2 * Y)

    def side(level, r, k):
        j = level_block(level)
        return kv_copy(
            kvq.at[j, r, pl.ds(0, 2)], j, r, side_send.at[level, r, k - 1], z * Y + (y + k) % Y
        )

    def kv_wait(j, r):
        kv_copy(kvq.at[j, r, pl.ds(0, 2)], j, r, cross_send.at[r], sp).wait_recv()

    top = 2 * pair + 1

    def spread(level, r, rises, act):
        @pl.when(rises)
        def _():
            act(up(level, r))

        for k in range(1, Y):

            @pl.when(jnp.logical_or(level < top, y < (y + k) % Y))
            def _():
                act(side(level, r, k))

    def start(copy):
        copy.start()

    def drain(copy):
        copy.wait_send()

    def send_own(r, act):
        act(swap(sp, r))

        @pl.when(bridge_up)
        def _():
            act(cross(r))

        spread(z, r, has_up, act)

    mate_level = z + 1 - 2 * a

    def send_mate(r, act):
        spread(mate_level, r, bridge_up, act)

    def send_below(level, r, act):
        spread(level, r, has_up, act)

    def relay_mate(r):
        swap(mate, r).wait_recv()
        send_mate(r, start)

    def relay_below(level, r):
        kv_wait(level_block(level), r)
        send_below(level, r, start)

    own.wait()
    for load in loads[:3]:
        load.wait()
    scale = hd ** (-0.5)

    def chunk(r, carry):
        rows = tok_rows(r)
        for k in range(1, X):
            tok_wait(source(k), r)
            tok_forward(k, r).start()
        tok_wait(sib, r)
        for k in range(1, X):
            tok_wait(source_sib(k), r)
        squares = jnp.zeros((R, 1), F32)
        for t in range(T):
            block = tok[t, rows, :].astype(F32)
            squares = squares + jnp.sum(block * block, axis=1, keepdims=True)
            scaled[rows, t * Dt : (t + 1) * Dt] = (block * gain[:, t * Dt : (t + 1) * Dt]).astype(BF16)
        inverse = lax.rsqrt(squares / Wd + NORM_EPS)
        inv[rows, :] = inverse
        left = scaled[rows, :]
        keys = inverse * dot(left, wk[...])
        values = inverse * dot(left, wv[...])
        queries = inverse * dot(left, wq[...])
        for h in range(H):
            mine = a if h else 1 - a
            slot = sp * mine + S * (1 - mine)
            cols = slice(h * V, (h + 1) * V)
            kvq[slot, r, 0] = rotate(keys[:, cols], rows).astype(BF16)
            kvq[slot, r, 1] = jnp.transpose(values[:, cols]).astype(BF16)
            turned = rotate(queries[:, cols], rows).astype(BF16).astype(F32) * scale
            kvq[slot, r, 2] = jnp.transpose(turned).astype(BF16)
        send_own(r, start)

        @pl.when(r > 0)
        def _():
            relay_mate(r - 1)

        return carry

    lax.fori_loop(0, NR, chunk, 0)
    relay_mate(NR - 1)

    def relay_some(dp, begin, end):
        @pl.when(dp <= pair)
        def _():
            for r in range(begin, end):
                for b in range(2):
                    relay_below(2 * (pair - dp) + b, r)

    relay_some(1, 0, G // 2)

    for load in loads[3:6]:
        load.wait()

    def mix_rows(r):
        return pl.ds(pl.multiple_of(r * M, M), M)

    def gate_chunk(r, carry):
        rows = mix_rows(r)
        inverse = inv[rows, :]
        left = scaled[rows, :]
        inner = (inverse * dot(left, wi[...])).astype(BF16)
        signal = (inverse * dot(left, ws[...])).astype(BF16)
        conv_in = (inner.astype(F32) * signal.astype(F32)).astype(BF16)
        padded[pl.ds(pl.multiple_of(PAD + r * M, PAD), M), :] = conv_in.astype(F32)
        gate[rows, :] = (inverse * dot(left, wo[...])).astype(BF16)
        return carry

    lax.fori_loop(0, NM, gate_chunk, 0)
    tail[...] = padded[L : L + PAD, :].astype(BF16)
    rim_copy = pltpu.make_async_remote_copy(
        src_ref=tail,
        dst_ref=rim,
        send_sem=rim_sem.at[0],
        recv_sem=rim_sem.at[1],
        device_id={"sp": (sp + 1) % S},
    )

    @pl.when(sp + 1 < S)
    def _():
        rim_copy.start()

    relay_some(1, G // 2, G)

    blank = jnp.zeros((hd, M), BF16)

    def attend(items):
        work = [(item, c) for item in items for c in range(2)]

        def score(item, c):
            chunks, b, part, shift = item
            keys = jnp.concatenate([kvq[j, r, 0] for j, r in chunks], axis=0)
            turned = jnp.concatenate(
                [kvq[level_block(2 * pair + b), G * part + g, 2] for g in range(G)], axis=1
            )
            if c:
                right = jnp.concatenate([blank, turned[hd:]], axis=0)
            else:
                right = jnp.concatenate([turned[:hd], blank], axis=0)
            scores = dot(keys, right)
            if shift is not None:
                key_row = lax.broadcasted_iota(jnp.int32, scores.shape, 0)
                query_lane = lax.broadcasted_iota(jnp.int32, scores.shape, 1)
                scores = jnp.where(key_row <= query_lane + shift, scores, MASKED)
            return scores

        def mix(item, c, fade, weights):
            chunks, b, part, _ = item
            values = jnp.concatenate([kvq[j, r, 1] for j, r in chunks], axis=1)
            acc[b, part, c] = fade * acc[b, part, c] + dot(values, weights)

        ready = [score(*work[0])]
        waiting = []
        for i, (item, c) in enumerate(work):
            for n in range(i + len(ready), min(i + 3, len(work))):
                ready.append(score(*work[n]))
            scores = ready.pop(0)
            _, b, part, _ = item
            old_max = row_max[b, part, c]
            new_max = jnp.maximum(old_max, jnp.max(scores, axis=0, keepdims=True))
            weights = jnp.exp(scores - new_max)
            fade = jnp.exp(old_max - new_max)
            row_max[b, part, c] = new_max
            row_sum[b, part, c] = fade * row_sum[b, part, c] + jnp.sum(weights, axis=0, keepdims=True)
            if waiting:
                mix(*waiting.pop())
            waiting.append((item, c, fade, weights.astype(BF16)))
        mix(*waiting.pop())

    def chunks_of(j, begin=0, end=NR):
        return [(j, r) for r in range(begin, end)]

    low_own = level_block(2 * pair)
    own_items = [(chunks_of(low_own), 1, part, None) for part in range(NM)]
    for b in range(2):
        for part in reversed(range(NM)):
            own_items.append((chunks_of(low_own + b * Y, 0, G * (part + 1)), b, part, M * part))
    attend(own_items)

    @pl.when(sp > 0)
    def _():
        rim_copy.wait_recv()
        padded[0:PAD, :] = rim[...].astype(F32)

    @pl.when(sp == 0)
    def _():
        padded[0:PAD, :] = jnp.zeros((PAD, C), F32)

    summed = jnp.zeros((L, C), F32)
    for j in range(taps_n):
        begin = PAD - (taps_n - 1) + j
        summed = summed + taps[j : j + 1, :] * padded[begin : begin + L, :]
    conv_all[tp, :, :] = (gate[...].astype(F32) * summed).astype(BF16)

    def mix_copy(piece, r, send, target):
        block = conv_all.at[piece, mix_rows(r), :]
        return pltpu.make_async_remote_copy(
            src_ref=block,
            dst_ref=block,
            send_sem=send,
            recv_sem=mix_recv.at[piece, r],
            device_id={"tp": target},
        )

    def mix_own(k, r):
        return mix_copy(tp, r, mix_send.at[k, r], peer(k) if k else sib)

    def mix_forward(k, r):
        return mix_copy(source(k), r, mix_relay.at[k, r], sib)

    def mix_wait(piece, r):
        mix_copy(piece, r, mix_send.at[0, r], sib).wait_recv()

    for r in range(NM):
        for k in list(range(1, X)) + [0]:
            mix_own(k, r).start()

    for k in range(1, Y):
        other = (y + k) % Y
        ahead = other < y
        low = 2 * pair * Y + other
        for r in range(NR):
            kv_wait(low, r)

        late_items = [(chunks_of(low), 1, part, None) for part in range(NM)]

        @pl.when(ahead)
        def _():
            for r in range(NR):
                kv_wait(low + Y, r)
            attend(
                late_items
                + [(chunks_of(low), 0, part, None) for part in range(NM)]
                + [(chunks_of(low + Y), 1, part, None) for part in range(NM)]
            )

        @pl.when(jnp.logical_not(ahead))
        def _():
            attend(late_items)

    def below(dp, carry):
        def half_step(half, inner):
            last = half == NM - 1
            next_dp = dp + last.astype(jnp.int32)
            next_r = G * ((half + 1) % NM)

            def relay_next(g):
                @pl.when(next_dp <= pair)
                def _():
                    for b in range(2):
                        relay_below(2 * (pair - next_dp) + b, next_r + g)

            def item(k, c):
                blocks = [(2 * (pair - dp) + b) * Y + (y + k) % Y for b in range(2)]

                @pl.when(k == 1)
                def _():
                    for g in range(G // 2):
                        relay_next(g)

                @pl.when(k > 0)
                def _():
                    for j in blocks:
                        for g in range(G):
                            kv_wait(j, G * half + g)

                chunks = [(j, G * half + g) for j in blocks for g in range(G)]
                attend([(chunks, b, part, None) for b in range(2) for part in range(NM)])
                return c

            lax.fori_loop(0, Y, item, 0)
            for g in range(G // 2, G):
                relay_next(g)
            return inner

        return lax.fori_loop(0, NM, half_step, carry)

    lax.fori_loop(1, pair + 1, below, 0)

    def at_copy(src, piece, h, r, send, target):
        return pltpu.make_async_remote_copy(
            src_ref=src,
            dst_ref=attn_all.at[piece, h, mix_rows(r), :],
            send_sem=send,
            recv_sem=at_recv.at[piece, h, r],
            device_id=target,
        )

    def at_own(k, r):
        target = {"tp": peer(k) if k else sib}
        return at_copy(attn_all.at[tp, a, mix_rows(r), :], tp, a, r, at_send.at[k, r], target)

    def at_off(k, r):
        target = {"sp": mate, "tp": peer(k)}
        return at_copy(away.at[mix_rows(r), :], tp, a, r, at_away.at[k, r], target)

    def at_forward(k, h, r, send):
        piece = source(k)
        return at_copy(attn_all.at[piece, h, mix_rows(r), :], piece, h, r, send, {"tp": sib})

    def at_wait(piece, h, r):
        at_copy(attn_all.at[piece, h, mix_rows(r), :], piece, h, r, at_send.at[0, r], {"tp": sib}).wait_recv()

    def near_forward(k, r):
        return at_forward(k, a, r, at_relay.at[k, r])

    def far_forward(k, r):
        return at_forward(k, 1 - a, r, at_relay_away.at[k, r])

    def finished(b, part):
        first_map = acc[b, part, 0] / row_sum[b, part, 0]
        second_map = acc[b, part, 1] / row_sum[b, part, 1]
        head_mix = first_map - lambdas[a] * second_map
        mean = jnp.mean(head_mix * head_mix, axis=0, keepdims=True)
        normed = head_mix * lax.rsqrt(mean + HEAD_EPS) * head_gain[...] * HEAD_SCALE
        return jnp.transpose(normed).astype(BF16)

    def log_total(b, part, c):
        return row_max[b, part, c] + jnp.log(row_sum[b, part, c])

    for part in range(NM):
        away[part * M : (part + 1) * M, :] = finished(1 - a, part)
        for k in list(range(1, X)) + [0]:
            at_off(k, part).start()
    for part in range(NM):
        attn_all[tp, a, part * M : (part + 1) * M, :] = finished(a, part)
        for k in list(range(1, X)) + [0]:
            at_own(k, part).start()
    for part in range(NM):
        for c in range(2):
            lse_away[c : c + 1, part * M : (part + 1) * M] = log_total(1 - a, part, c)
            lse[a, c : c + 1, part * M : (part + 1) * M] = log_total(a, part, c)
    lse_copy = pltpu.make_async_remote_copy(
        src_ref=lse_away,
        dst_ref=lse_in,
        send_sem=lse_sem.at[0],
        recv_sem=lse_sem.at[1],
        device_id={"sp": mate},
    )
    lse_copy.start()

    loads[6].wait()
    loads[7].wait()

    def conv_part(r, carry):
        rows = mix_rows(r)
        for k in range(1, X):
            mix_wait(source(k), r)
            mix_forward(k, r).start()
        mix_wait(sib, r)
        for k in range(1, X):
            mix_wait(source_sib(k), r)
        part = dot(conv_all[0, rows, :], wc[0:C, :])
        for t in range(1, T):
            part = part + dot(conv_all[t, rows, :], wc[t * C : (t + 1) * C, :])
        total[rows, :] = part
        return carry

    lax.fori_loop(0, NM, conv_part, 0)

    for r in range(NM):
        for k in range(1, X):
            at_wait(source(k), a, r)
            near_forward(k, r).start()

    def attn_part(r, carry):
        rows = mix_rows(r)
        for k in range(X):
            at_wait(source(k), 1 - a, r)
            far_forward(k, r).start()
        for k in range(X):
            at_wait(source_sib(k), a, r)
        for k in range(X):
            at_wait(source_sib(k), 1 - a, r)
        part = total[rows, :]
        for t in range(T):
            both = jnp.concatenate([attn_all[t, h, rows, :] for h in range(H)], axis=1)
            part = part + dot(both, wa[t * C : (t + 1) * C, :])
        out[rows, :] = part.astype(BF16)
        return carry

    lax.fori_loop(0, NM, attn_part, 0)
    lse_copy.wait_recv()
    lse[1 - a] = lse_in[...]
    lse_copy.wait_send()

    for r in range(NR):
        for k in range(X):
            tok_own(k, r).wait_send()
        for k in range(1, X):
            tok_forward(k, r).wait_send()
        send_own(r, drain)
        send_mate(r, drain)

    def drain_level(level, carry):
        for r in range(NR):
            send_below(level, r, drain)
        return carry

    lax.fori_loop(0, 2 * pair, drain_level, 0)

    for r in range(NM):
        for k in range(X):
            mix_own(k, r).wait_send()
            at_own(k, r).wait_send()
            at_off(k, r).wait_send()
            far_forward(k, r).wait_send()
        for k in range(1, X):
            mix_forward(k, r).wait_send()
            near_forward(k, r).wait_send()

    @pl.when(sp + 1 < S)
    def _():
        rim_copy.wait_send()


def pair_device(
    dims,
    tokens,
    norm_gain,
    query_weight,
    key_weight,
    value_weight,
    outer_gate_weight,
    inner_gate_weight,
    conv_input_weight,
    conv_taps,
    lambdas,
    head_gain,
    attn_out_weight,
    conv_out_weight,
):
    S, T, Z, Y = dims["S"], dims["T"], dims["Z"], dims["Y"]
    L, Dt = tokens.shape
    H = lambdas.shape[0]
    C = query_weight.shape[1]
    V = C // H
    hd = V // 2
    O = attn_out_weight.shape[1]
    Wd = norm_gain.shape[0]
    R = V
    M = 2 * R
    NR, NM, PAD = L // R, L // M, 16
    X = T // 2
    frequency = ROPE_BASE ** (-np.arange(hd // 2) * 2.0 / hd)
    freq = jnp.asarray(np.tile(frequency, 4)[None, :], F32)
    any_spec = pl.BlockSpec(memory_space=pl.ANY)
    vmem = pl.BlockSpec(memory_space=pltpu.VMEM)
    smem = pl.BlockSpec(memory_space=pltpu.SMEM)
    dma = pltpu.SemaphoreType.DMA
    mixed, lse = pl.pallas_call(
        functools.partial(pair_kernel, dict(dims, H=H)),
        out_shape=(
            jax.ShapeDtypeStruct((L, O), BF16),
            jax.ShapeDtypeStruct((H, 2, L), F32),
        ),
        in_specs=[any_spec, vmem, vmem] + [any_spec] * 6 + [vmem, smem, vmem] + [any_spec] * 2,
        out_specs=(vmem, vmem),
        scratch_shapes=[
            pltpu.VMEM((T, L, Dt), BF16),
            pltpu.VMEM((L, Wd), BF16),
            pltpu.VMEM((L, 1), F32),
            pltpu.VMEM((L, V), F32),
            pltpu.VMEM((L, V), F32),
        ]
        + [pltpu.VMEM((Wd, C), BF16)] * 6
        + [pltpu.VMEM((T * C, O), BF16)] * 2
        + [
            pltpu.VMEM((S + 1, NR, 3, R, V), BF16),
            pltpu.VMEM((2, NM, 2, 1, M), F32),
            pltpu.VMEM((2, NM, 2, 1, M), F32),
            pltpu.VMEM((2, NM, 2, V, M), F32),
            pltpu.VMEM((L, C), BF16),
            pltpu.VMEM((PAD + L, C), F32),
            pltpu.VMEM((PAD, C), BF16),
            pltpu.VMEM((PAD, C), BF16),
            pltpu.VMEM((T, L, C), BF16),
            pltpu.VMEM((T, H, L, V), BF16),
            pltpu.VMEM((L, V), BF16),
            pltpu.VMEM((2, L), F32),
            pltpu.VMEM((2, L), F32),
            pltpu.VMEM((L, O), F32),
            dma((8,)),
            dma,
            dma((T, NR)),
            dma((X, NR)),
            dma((X, NR)),
            dma((S, NR)),
            dma((NR,)),
            dma((NR,)),
            dma((Z, NR, max(Y - 1, 1))),
            dma((Z, NR)),
            dma((2,)),
            dma((2,)),
            dma((T, NM)),
            dma((X, NM)),
            dma((X, NM)),
            dma((T, H, NM)),
            dma((X, NM)),
            dma((X, NM)),
            dma((X, NM)),
            dma((X, NM)),
        ],
        compiler_params=pltpu.CompilerParams(
            collective_id=0,
            has_side_effects=True,
            vmem_limit_bytes=60 * 1024 * 1024,
        ),
        name="mixer",
    )(
        tokens,
        norm_gain[None, :],
        freq,
        query_weight,
        key_weight,
        value_weight,
        outer_gate_weight,
        inner_gate_weight,
        conv_input_weight,
        conv_taps,
        lambdas,
        head_gain[:, None],
        attn_out_weight,
        conv_out_weight,
    )
    return mixed, lse


def per_device(dims, *arrays):
    tokens, query_weight, lambdas = arrays[0], arrays[2], arrays[9]
    width = query_weight.shape[1] // lambdas.shape[0]
    paired = lambdas.shape[0] == 2 and dims["Z"] % 2 == 0 and dims["T"] % 2 == 0
    paired = paired and width == 128 and tokens.shape[0] % (2 * width) == 0
    return (pair_device if paired else ring_device)(dims, *arrays)


def solution(mesh):
    S, T = mesh.shape["sp"], mesh.shape["tp"]
    Y = max(d for d in range(1, S + 1) if S % d == 0 and d * d <= S)
    dims = {"S": S, "T": T, "Z": S // Y, "Y": Y}
    in_specs = (
        P("sp", "tp"),
        P(),
        P(None, "tp"),
        P(None, "tp"),
        P(None, "tp"),
        P(None, "tp"),
        P(None, "tp"),
        P(None, "tp"),
        P(None, "tp"),
        P("tp"),
        P(),
        P(None, "tp"),
        P(None, "tp"),
    )
    out_specs = (P("sp", "tp"), P("tp", None, "sp"))
    return jax.shard_map(
        functools.partial(per_device, dims),
        mesh=mesh,
        in_specs=in_specs,
        out_specs=out_specs,
        check_vma=False,
    )
```

```python
import functools

import jax
import jax.numpy as jnp
import numpy as np
from jax import lax
from jax.experimental import pallas as pl
from jax.experimental.pallas import tpu as pltpu
from jax.sharding import PartitionSpec as P

NORM_EPS = 1e-06
HEAD_EPS = 1e-05
ROPE_BASE = 500000.0
MASKED = -1e30
HEAD_SCALE = 0.8
F32 = jnp.float32
BF16 = jnp.bfloat16


def dot(a, b):
    return jnp.dot(a, b, preferred_element_type=F32)


def dot_t(a, b):
    return lax.dot_general(a, b, (((1,), (1,)), ((), ())), preferred_element_type=F32)


def ring_kernel(
    dims,
    tokens,
    gain,
    freq,
    wq_h,
    wk_h,
    wv_h,
    wo_h,
    wi_h,
    ws_h,
    taps,
    lambdas,
    head_gain,
    wa_h,
    wc_h,
    out,
    lse,
    tok,
    scaled,
    inv,
    cos_t,
    sin_t,
    wq,
    wk,
    wv,
    wo,
    wi,
    ws,
    wa,
    wc,
    kv,
    qz,
    row_max,
    row_sum,
    acc,
    gate,
    padded,
    tail,
    rim,
    conv_all,
    attn_all,
    total,
    w_sem,
    own_sem,
    tok_recv,
    tok_send,
    tok_relay,
    kv_recv,
    kv_send_z,
    kv_send_y,
    kv_extra,
    rim_sem,
    mix_recv,
    mix_send,
    mix_relay,
):
    S, T, Z, Y, H = dims["S"], dims["T"], dims["Z"], dims["Y"], dims["H"]
    L, Dt = tokens.shape
    Wd = T * Dt
    C = wq_h.shape[1]
    V = C // H
    hd = V // 2
    NR = tok_recv.shape[1]
    R = L // NR
    NM = mix_recv.shape[2]
    M = L // NM
    X = T // 2
    taps_n = taps.shape[0]
    PAD = tail.shape[0]

    sp = lax.axis_index("sp")
    tp = lax.axis_index("tp")
    z = sp // Y
    y = sp % Y
    core = tp % 2
    xi = tp // 2
    sib = xi * 2 + (1 - core)

    def peer(k):
        return ((xi + k) % X) * 2 + core

    def source(k):
        return ((xi - k + X) % X) * 2 + core

    pairs = [(wk_h, wk), (wv_h, wv), (wq_h, wq), (wi_h, wi), (ws_h, ws), (wo_h, wo), (wc_h, wc), (wa_h, wa)]
    own = pltpu.make_async_copy(tokens, tok.at[tp], own_sem)
    own.start()
    loads = [pltpu.make_async_copy(s, d, w_sem.at[i]) for i, (s, d) in enumerate(pairs)]
    for load in loads:
        load.start()

    barrier = pltpu.get_barrier_semaphore()

    def greet(target):
        pl.semaphore_signal(barrier, inc=1, device_id=target)

    for k in range(1, T):
        greet({"tp": (tp + k) % T})
    for k in range(1, Y):
        greet({"sp": z * Y + (y + k) % Y})
    has_up = z + 1 < Z
    has_down = z > 0
    far_up = jnp.logical_and(has_up, y == Y - 1) if Y > 1 else None
    far_down = jnp.logical_and(has_down, y == 0) if Y > 1 else None
    expect = (T - 1) + (Y - 1) + has_up.astype(jnp.int32) + has_down.astype(jnp.int32)

    @pl.when(has_up)
    def _():
        greet({"sp": sp + Y})

    @pl.when(has_down)
    def _():
        greet({"sp": sp - Y})

    if Y > 1:
        expect = expect + far_up.astype(jnp.int32) + far_down.astype(jnp.int32)

        @pl.when(far_up)
        def _():
            greet({"sp": sp + 1})

        @pl.when(far_down)
        def _():
            greet({"sp": sp - 1})

    pl.semaphore_wait(barrier, expect)

    def tok_rows(r):
        return pl.ds(pl.multiple_of(r * R, R), R)

    def tok_copy(src, piece, r, send, target):
        return pltpu.make_async_remote_copy(
            src_ref=src,
            dst_ref=tok.at[piece, tok_rows(r), :],
            send_sem=send,
            recv_sem=tok_recv.at[piece, r],
            device_id={"tp": target},
        )

    def tok_own(k, r):
        target = peer(k) if k else sib
        return tok_copy(tokens.at[tok_rows(r), :], tp, r, tok_send.at[k, r], target)

    def tok_forward(k, r):
        piece = source(k)
        return tok_copy(tok.at[piece, tok_rows(r), :], piece, r, tok_relay.at[k, r], sib)

    def tok_wait(piece, r):
        tok_copy(tok.at[piece, tok_rows(r), :], piece, r, tok_send.at[0, r], sib).wait_recv()

    for r in range(NR):
        for k in list(range(1, X)) + [0]:
            tok_own(k, r).start()

    lane = lax.broadcasted_iota(jnp.int32, (R, V), 1)
    first = (lane % hd) < (hd // 2)

    def table(r, carry):
        base = sp * L + r * R
        pos = (base + lax.broadcasted_iota(jnp.int32, (R, V), 0)).astype(F32)
        angle = pos * freq[...]
        sine = jnp.sin(angle)
        cos_t[tok_rows(r), :] = jnp.cos(angle)
        sin_t[tok_rows(r), :] = jnp.where(first, -sine, sine)
        return carry

    lax.fori_loop(0, NR, table, 0)

    def rotate(block, rows):
        low = (lax.broadcasted_iota(jnp.int32, block.shape, 1) % hd) < (hd // 2)
        other = jnp.where(
            low, pltpu.roll(block, V - hd // 2, 1), pltpu.roll(block, hd // 2, 1)
        )
        return block * cos_t[rows, :] + other * sin_t[rows, :]

    def kv_copy(j, r, send, target):
        block = kv.at[j, tok_rows(r), :]
        return pltpu.make_async_remote_copy(
            src_ref=block,
            dst_ref=block,
            send_sem=send,
            recv_sem=kv_recv.at[j, r],
            device_id={"sp": target},
        )

    def kv_up(dz, r):
        return kv_copy(sp - dz * Y, r, kv_send_z.at[dz, r], sp + Y)

    def kv_side(dz, r, k):
        return kv_copy(sp - dz * Y, r, kv_send_y.at[dz, r, k - 1], z * Y + (y + k) % Y)

    def kv_wait(j, r):
        kv_copy(j, r, kv_send_z.at[0, r], sp).wait_recv()

    EX = NR // 2 if Y == 2 else 0

    def extra(r):
        return kv_copy(0, r, kv_extra.at[r], sp + Y)

    def kv_send(dz, r, act):
        @pl.when(has_up)
        def _():
            act(kv_up(dz, r))

        for k in range(1, Y):
            wanted = jnp.logical_or(dz > 0, y + k < Y)
            if EX:
                other_way = jnp.logical_and(dz == z, jnp.logical_and(dz > 0, r < EX))
                wanted = jnp.logical_and(wanted, jnp.logical_not(jnp.logical_and(y == 0, other_way)))

            @pl.when(wanted)
            def _():
                act(kv_side(dz, r, k))

    def relay(dz, r):
        @pl.when(dz <= z)
        def _():
            kv_wait(sp - dz * Y, r)
            kv_send(dz, r, lambda copy: copy.start())

    def first_relay(r):
        relay(1, r)
        if EX:

            @pl.when(jnp.logical_and(jnp.logical_and(z == 0, y == 1), r < EX))
            def _():
                kv_wait(0, r)

                @pl.when(has_up)
                def _():
                    extra(r).start()

    own.wait()
    loads[0].wait()
    loads[1].wait()

    def key_chunk(r, carry):
        rows = tok_rows(r)
        for k in range(1, X):
            tok_wait(source(k), r)
            tok_forward(k, r).start()
        tok_wait(sib, r)
        for k in range(1, X):
            tok_wait(((xi + k) % X) * 2 + (1 - core), r)
        squares = jnp.zeros((R, 1), F32)
        for t in range(T):
            block = tok[t, rows, :].astype(F32)
            squares = squares + jnp.sum(block * block, axis=1, keepdims=True)
            scaled[rows, t * Dt : (t + 1) * Dt] = (block * gain[:, t * Dt : (t + 1) * Dt]).astype(BF16)
        inverse = lax.rsqrt(squares / Wd + NORM_EPS)
        inv[rows, :] = inverse
        left = scaled[rows, :]
        keys = inverse * dot(left, wk[...])
        for h in range(H):
            kv[sp, rows, h * V : (h + 1) * V] = rotate(keys[:, h * V : (h + 1) * V], rows).astype(BF16)
        kv[sp, rows, C : 2 * C] = (inverse * dot(left, wv[...])).astype(BF16)
        kv_send(0, r, lambda copy: copy.start())

        @pl.when(r > 0)
        def _():
            first_relay(r - 1)

        return carry

    lax.fori_loop(0, NR, key_chunk, 0)

    for load in loads[2:6]:
        load.wait()
    half = lax.broadcasted_iota(jnp.int32, (M, V), 1) < hd
    scale = hd ** (-0.5)

    def mix_rows(r):
        return pl.ds(pl.multiple_of(r * M, M), M)

    def query_chunk(r, carry):
        rows = mix_rows(r)
        inverse = inv[rows, :]
        left = scaled[rows, :]
        queries = inverse * dot(left, wq[...])
        for h in range(H):
            turned = rotate(queries[:, h * V : (h + 1) * V], rows).astype(BF16).astype(F32) * scale
            qz[h, 0, rows, :] = jnp.where(half, turned, 0.0).astype(BF16)
            qz[h, 1, rows, :] = jnp.where(half, 0.0, turned).astype(BF16)
        inner = (inverse * dot(left, wi[...])).astype(BF16)
        signal = (inverse * dot(left, ws[...])).astype(BF16)
        conv_in = (inner.astype(F32) * signal.astype(F32)).astype(BF16)
        padded[pl.ds(pl.multiple_of(PAD + r * M, PAD), M), :] = conv_in.astype(F32)
        gate[rows, :] = (inverse * dot(left, wo[...])).astype(BF16)

        @pl.when(r == 0)
        def _():
            first_relay(NR - 1)

        return carry

    lax.fori_loop(0, NM, query_chunk, 0)
    tail[...] = padded[L : L + PAD, :].astype(BF16)
    rim_copy = pltpu.make_async_remote_copy(
        src_ref=tail,
        dst_ref=rim,
        send_sem=rim_sem.at[0],
        recv_sem=rim_sem.at[1],
        device_id={"sp": (sp + 1) % S},
    )

    @pl.when(sp + 1 < S)
    def _():
        rim_copy.start()

    def attend(j, diagonal):
        def one(i, carry):
            rows = mix_rows(i)
            for h in range(H):
                query = qz[h, :, rows, :].reshape(2 * M, V)
                scores = dot_t(query, kv[j, :, h * V : (h + 1) * V])
                if diagonal:
                    row = lax.broadcasted_iota(jnp.int32, scores.shape, 0)
                    row = jnp.where(row >= M, row - M, row) + i * M
                    col = lax.broadcasted_iota(jnp.int32, scores.shape, 1)
                    scores = jnp.where(row >= col, scores, MASKED)
                    new_max = jnp.max(scores, axis=1, keepdims=True)
                else:
                    old_max = row_max[h, :, rows, :].reshape(2 * M, 1)
                    new_max = jnp.maximum(old_max, jnp.max(scores, axis=1, keepdims=True))
                weights = jnp.exp(scores - new_max)
                sums = jnp.sum(weights, axis=1, keepdims=True)
                mixed = dot(weights.astype(BF16), kv[j, :, C + h * V : C + (h + 1) * V])
                if not diagonal:
                    fade = jnp.exp(old_max - new_max)
                    sums = sums + fade * row_sum[h, :, rows, :].reshape(2 * M, 1)
                    mixed = mixed + fade * acc[h, :, rows, :].reshape(2 * M, V)
                row_max[h, :, rows, :] = new_max.reshape(2, M, 1)
                row_sum[h, :, rows, :] = sums.reshape(2, M, 1)
                acc[h, :, rows, :] = mixed.reshape(2, M, V)
            return carry

        lax.fori_loop(0, NM, one, 0)

    attend(sp, True)

    @pl.when(sp > 0)
    def _():
        rim_copy.wait_recv()
        padded[0:PAD, :] = rim[...].astype(F32)

    @pl.when(sp == 0)
    def _():
        padded[0:PAD, :] = jnp.zeros((PAD, C), F32)

    summed = jnp.zeros((L, C), F32)
    for j in range(taps_n):
        begin = PAD - (taps_n - 1) + j
        summed = summed + taps[j : j + 1, :] * padded[begin : begin + L, :]
    conv_all[tp, :, :] = (gate[...].astype(F32) * summed).astype(BF16)

    def mix_copy(which, buf, piece, r, send, target):
        block = buf.at[piece, mix_rows(r), :]
        return pltpu.make_async_remote_copy(
            src_ref=block,
            dst_ref=block,
            send_sem=send,
            recv_sem=mix_recv.at[which, piece, r],
            device_id={"tp": target},
        )

    def mix_own(which, buf, k, r):
        target = peer(k) if k else sib
        return mix_copy(which, buf, tp, r, mix_send.at[which, k, r], target)

    def mix_forward(which, buf, k, r):
        return mix_copy(which, buf, source(k), r, mix_relay.at[which, k, r], sib)

    def mix_wait(which, buf, piece, r):
        mix_copy(which, buf, piece, r, mix_send.at[which, 0, r], sib).wait_recv()

    for r in range(NM):
        for k in list(range(1, X)) + [0]:
            mix_own(0, conv_all, k, r).start()

    def step(dz, carry):
        def row_block(k, inner):
            def forward(r, c):
                relay(dz + 1, r)
                return c

            lax.fori_loop(k * NR // Y, (k + 1) * NR // Y, forward, 0)
            side = (y + k) % Y
            level = jnp.where(k == 0, z - dz, z - dz + 1)
            j = level * Y + side
            valid = jnp.where(k == 0, dz <= z, jnp.logical_or(level < z, side < y))

            @pl.when(valid)
            def _():
                @pl.when(k > 0)
                def _():
                    for r in range(NR):
                        if r < EX:
                            climbs = jnp.logical_and(level == 0, y == 1)

                            @pl.when(jnp.logical_not(jnp.logical_and(climbs, z == 0)))
                            def _():
                                kv_wait(j, r)

                            @pl.when(jnp.logical_and(climbs, jnp.logical_and(z > 0, has_up)))
                            def _():
                                extra(r).start()

                        else:
                            kv_wait(j, r)

                attend(j, False)

            return inner

        lax.fori_loop(0, Y, row_block, 0)
        return carry

    lax.fori_loop(1, z + 2, step, 0)

    def finish(i, carry):
        rows = mix_rows(i)
        for h in range(H):
            first_map = acc[h, 0, rows, :] / row_sum[h, 0, rows, :]
            second_map = acc[h, 1, rows, :] / row_sum[h, 1, rows, :]
            head_mix = first_map - lambdas[h] * second_map
            mean = jnp.mean(head_mix * head_mix, axis=1, keepdims=True)
            normed = head_mix * lax.rsqrt(mean + HEAD_EPS) * head_gain[...] * HEAD_SCALE
            attn_all[tp, rows, h * V : (h + 1) * V] = normed.astype(BF16)
        for k in list(range(1, X)) + [0]:
            mix_own(1, attn_all, k, i).start()
        return carry

    lax.fori_loop(0, NM, finish, 0)

    loads[6].wait()
    loads[7].wait()

    def gather(which, buf, r):
        for k in range(1, X):
            mix_wait(which, buf, source(k), r)
            mix_forward(which, buf, k, r).start()

    def gather_rest(which, buf, r):
        mix_wait(which, buf, sib, r)
        for k in range(1, X):
            mix_wait(which, buf, ((xi + k) % X) * 2 + (1 - core), r)

    def conv_part(r, carry):
        rows = mix_rows(r)
        gather(0, conv_all, r)
        gather_rest(0, conv_all, r)
        part = dot(conv_all[0, rows, :], wc[0:C, :])
        for t in range(1, T):
            part = part + dot(conv_all[t, rows, :], wc[t * C : (t + 1) * C, :])
        total[rows, :] = part
        return carry

    lax.fori_loop(0, NM, conv_part, 0)

    lanes = lax.broadcasted_iota(jnp.int32, (L, 128), 1)
    columns = jnp.zeros((L, 128), F32)
    for h in range(H):
        for c in range(2):
            value = row_max[h, c, :, :] + jnp.log(row_sum[h, c, :, :])
            columns = jnp.where(lanes == 2 * h + c, value, columns)
    turned_columns = jnp.transpose(columns)
    for h in range(H):
        lse[h] = turned_columns[2 * h : 2 * h + 2, :]

    def attn_part(r, carry):
        rows = mix_rows(r)
        gather(1, attn_all, r)
        gather_rest(1, attn_all, r)
        part = total[rows, :]
        for t in range(T):
            part = part + dot(attn_all[t, rows, :], wa[t * C : (t + 1) * C, :])
        out[rows, :] = part.astype(BF16)
        return carry

    lax.fori_loop(0, NM, attn_part, 0)

    for r in range(NR):
        for k in range(X):
            tok_own(k, r).wait_send()
        for k in range(1, X):
            tok_forward(k, r).wait_send()

    def drain(dz, carry):
        def inner(r, c):
            kv_send(dz, r, lambda copy: copy.wait_send())
            return c

        return lax.fori_loop(0, NR, inner, carry)

    lax.fori_loop(0, z + 1, drain, 0)
    if EX:

        @pl.when(jnp.logical_and(y == 1, has_up))
        def _():
            for r in range(EX):
                extra(r).wait_send()

    for which, buf in ((0, conv_all), (1, attn_all)):
        for r in range(NM):
            for k in range(X):
                mix_own(which, buf, k, r).wait_send()
            for k in range(1, X):
                mix_forward(which, buf, k, r).wait_send()

    @pl.when(sp + 1 < S)
    def _():
        rim_copy.wait_send()


def ring_device(
    dims,
    tokens,
    norm_gain,
    query_weight,
    key_weight,
    value_weight,
    outer_gate_weight,
    inner_gate_weight,
    conv_input_weight,
    conv_taps,
    lambdas,
    head_gain,
    attn_out_weight,
    conv_out_weight,
):
    S, T, Z, Y = dims["S"], dims["T"], dims["Z"], dims["Y"]
    L, Dt = tokens.shape
    H = lambdas.shape[0]
    C = query_weight.shape[1]
    V = C // H
    hd = V // 2
    O = attn_out_weight.shape[1]
    Wd = norm_gain.shape[0]
    NR, NM, PAD = 4, 2, 16
    X = T // 2
    frequency = ROPE_BASE ** (-np.arange(hd // 2) * 2.0 / hd)
    freq = jnp.asarray(np.tile(frequency, 4)[None, :], F32)
    any_spec = pl.BlockSpec(memory_space=pl.ANY)
    vmem = pl.BlockSpec(memory_space=pltpu.VMEM)
    smem = pl.BlockSpec(memory_space=pltpu.SMEM)
    dma = pltpu.SemaphoreType.DMA
    mixed, lse = pl.pallas_call(
        functools.partial(ring_kernel, dict(dims, H=H)),
        out_shape=(
            jax.ShapeDtypeStruct((L, O), BF16),
            jax.ShapeDtypeStruct((H, 2, L), F32),
        ),
        in_specs=[any_spec, vmem, vmem] + [any_spec] * 6 + [vmem, smem, vmem] + [any_spec] * 2,
        out_specs=(vmem, vmem),
        scratch_shapes=[
            pltpu.VMEM((T, L, Dt), BF16),
            pltpu.VMEM((L, Wd), BF16),
            pltpu.VMEM((L, 1), F32),
            pltpu.VMEM((L, V), F32),
            pltpu.VMEM((L, V), F32),
        ]
        + [pltpu.VMEM((Wd, C), BF16)] * 6
        + [pltpu.VMEM((T * C, O), BF16)] * 2
        + [
            pltpu.VMEM((S, L, 2 * C), BF16),
            pltpu.VMEM((H, 2, L, V), BF16),
            pltpu.VMEM((H, 2, L, 1), F32),
            pltpu.VMEM((H, 2, L, 1), F32),
            pltpu.VMEM((H, 2, L, V), F32),
            pltpu.VMEM((L, C), BF16),
            pltpu.VMEM((PAD + L, C), F32),
            pltpu.VMEM((PAD, C), BF16),
            pltpu.VMEM((PAD, C), BF16),
            pltpu.VMEM((T, L, C), BF16),
            pltpu.VMEM((T, L, C), BF16),
            pltpu.VMEM((L, O), F32),
            dma((8,)),
            dma,
            dma((T, NR)),
            dma((X, NR)),
            dma((X, NR)),
            dma((S, NR)),
            dma((Z, NR)),
            dma((Z, NR, max(Y - 1, 1))),
            dma((NR,)),
            dma((2,)),
            dma((2, T, NM)),
            dma((2, X, NM)),
            dma((2, X, NM)),
        ],
        compiler_params=pltpu.CompilerParams(
            collective_id=0, has_side_effects=True, vmem_limit_bytes=60 * 1024 * 1024
        ),
        name="mixer",
    )(
        tokens,
        norm_gain[None, :],
        freq,
        query_weight,
        key_weight,
        value_weight,
        outer_gate_weight,
        inner_gate_weight,
        conv_input_weight,
        conv_taps,
        lambdas,
        head_gain[None, :],
        attn_out_weight,
        conv_out_weight,
    )
    return mixed, lse


def pair_kernel(
    dims,
    tokens,
    gain_h,
    freq_h,
    wq_h,
    wk_h,
    wv_h,
    wo_h,
    wi_h,
    ws_h,
    taps_h,
    lambdas,
    head_gain_h,
    wa_h,
    wc_h,
    out,
    lse_out,
    tok,
    scaled,
    inv,
    cos_t,
    sin_t,
    gain_t,
    wq,
    wk,
    wv,
    wo,
    wi,
    ws,
    wa,
    wc,
    kvq,
    row_max,
    row_sum,
    acc,
    gate,
    padded,
    tail,
    rim,
    conv_all,
    attn_all,
    away,
    lse_away,
    lse_in,
    total,
    result,
    lse,
    freq,
    gain,
    taps,
    head_gain,
    w_sem,
    own_sem,
    tok_recv,
    tok_send,
    tok_relay,
    kv_recv,
    swap_send,
    ask_send,
    ask_recv,
    cross_send,
    side_send,
    up_send,
    rim_sem,
    lse_sem,
    mix_recv,
    mix_send,
    mix_relay,
    at_recv,
    at_send,
    at_away,
    at_relay,
    at_relay_away,
    out_sem,
    lse_out_sem,
):
    S, T, Z, Y, H = dims["S"], dims["T"], dims["Z"], dims["Y"], dims["H"]
    L, Dt = tokens.shape
    Wd = T * Dt
    C = wq_h.shape[1]
    V = C // H
    hd = V // 2
    NR = tok_recv.shape[1]
    R = L // NR
    NM = mix_recv.shape[1]
    M = L // NM
    G = M // R
    X = T // 2
    taps_n = taps.shape[0]
    PAD = tail.shape[0]

    sp = lax.axis_index("sp")
    tp = lax.axis_index("tp")
    z = sp // Y
    y = sp % Y
    pair = z // 2
    a = z % 2
    mate = sp + (1 - 2 * a) * Y
    core = tp % 2
    xi = tp // 2
    sib = xi * 2 + (1 - core)
    has_up = z + 2 - a < Z
    has_down = pair > 0

    def peer(k):
        return ((xi + k) % X) * 2 + core

    def source(k):
        return ((xi - k + X) % X) * 2 + core

    def source_sib(k):
        return ((xi - k + X) % X) * 2 + (1 - core)

    pairs = [(wk_h, wk), (wv_h, wv), (wq_h, wq), (wi_h, wi), (ws_h, ws), (wo_h, wo), (wc_h, wc), (wa_h, wa)]
    pairs = pairs + [(freq_h, freq), (gain_h, gain), (taps_h, taps), (head_gain_h, head_gain)]
    own = pltpu.make_async_copy(tokens, tok.at[tp], own_sem)
    own.start()
    loads = [pltpu.make_async_copy(s, d, w_sem.at[i]) for i, (s, d) in enumerate(pairs)]
    for load in loads[8:] + loads[:8]:
        load.start()

    barrier = pltpu.get_barrier_semaphore()

    def greet(target):
        pl.semaphore_signal(barrier, inc=1, device_id=target)

    for k in range(1, T):
        greet({"tp": (tp + k) % T})
    for k in range(X):
        greet({"sp": mate, "tp": peer(k)})
    for k in range(1, Y):
        greet({"sp": z * Y + (y + k) % Y})
    expect = (T - 1) + X + (Y - 1)
    bridge_up = jnp.logical_and(a == 1, has_up)
    bridge_down = jnp.logical_and(a == 0, has_down)
    for near, step in (
        (has_up, 2 * Y),
        (has_down, -2 * Y),
        (bridge_up, Y),
        (bridge_down, -Y),
        (sp + 1 < S, 1),
        (sp > 0, -1),
    ):
        expect = expect + near.astype(jnp.int32)

        @pl.when(near)
        def _():
            greet({"sp": sp + step})

    pl.semaphore_wait(barrier, expect)

    def tok_rows(r):
        return pl.ds(pl.multiple_of(r * R, R), R)

    def tok_copy(src, piece, r, send, target):
        return pltpu.make_async_remote_copy(
            src_ref=src,
            dst_ref=tok.at[piece, tok_rows(r), :],
            send_sem=send,
            recv_sem=tok_recv.at[piece, r],
            device_id={"tp": target},
        )

    def tok_own(k, r):
        target = peer(k) if k else sib
        return tok_copy(tokens.at[tok_rows(r), :], tp, r, tok_send.at[k, r], target)

    def tok_forward(k, r):
        piece = source(k)
        return tok_copy(tok.at[piece, tok_rows(r), :], piece, r, tok_relay.at[k, r], sib)

    def tok_wait(piece, r):
        tok_copy(tok.at[piece, tok_rows(r), :], piece, r, tok_send.at[0, r], sib).wait_recv()

    for r in reversed(range(NR)):
        for k in list(range(1, X)) + [0]:
            tok_own(k, r).start()

    lane = lax.broadcasted_iota(jnp.int32, (R, V), 1)
    first = (lane % hd) < (hd // 2)

    loads[8].wait()
    loads[11].wait()

    def table(r, carry):
        base = sp * L + r * R
        pos = (base + lax.broadcasted_iota(jnp.int32, (R, V), 0)).astype(F32)
        angle = pos * freq[...]
        sine = jnp.sin(angle)
        cos_t[tok_rows(r), :] = jnp.cos(angle)
        sin_t[tok_rows(r), :] = jnp.where(first, -sine, sine)
        return carry

    lax.fori_loop(0, NR, table, 0)
    gain_t[...] = jnp.transpose(jnp.broadcast_to(head_gain[...], (M, V)))

    row_max[...] = jnp.full(row_max.shape, MASKED, F32)
    row_sum[...] = jnp.zeros(row_sum.shape, F32)
    acc[...] = jnp.zeros(acc.shape, F32)

    def rotate(block, rows):
        other = jnp.where(first, pltpu.roll(block, V - hd // 2, 1), pltpu.roll(block, hd // 2, 1))
        return block * cos_t[rows, :] + other * sin_t[rows, :]

    def kv_copy(src, j, r, send, target):
        return pltpu.make_async_remote_copy(
            src_ref=src,
            dst_ref=kvq.at[j, r, pl.ds(0, 2)],
            send_sem=send,
            recv_sem=kv_recv.at[j, r],
            device_id={"sp": target},
        )

    def swap(j, r):
        return pltpu.make_async_remote_copy(
            src_ref=kvq.at[S, r, pl.ds(0, 2)],
            dst_ref=kvq.at[j, r, pl.ds(0, 2)],
            send_sem=swap_send.at[r],
            recv_sem=kv_recv.at[j, r],
            device_id={"sp": mate},
        )

    def ask(j, r):
        return pltpu.make_async_remote_copy(
            src_ref=kvq.at[S, r, 2],
            dst_ref=kvq.at[j, r, 2],
            send_sem=ask_send.at[r],
            recv_sem=ask_recv.at[r],
            device_id={"sp": mate},
        )

    def cross(r):
        return kv_copy(kvq.at[S, r, pl.ds(0, 2)], sp, r, cross_send.at[r], sp + Y)

    def level_block(level):
        return level * Y + y

    def up(level, r):
        j = level_block(level)
        return kv_copy(kvq.at[j, r, pl.ds(0, 2)], j, r, up_send.at[level, r], sp + 2 * Y)

    def side(level, r, k):
        j = level_block(level)
        return kv_copy(
            kvq.at[j, r, pl.ds(0, 2)], j, r, side_send.at[level, r, k - 1], z * Y + (y + k) % Y
        )

    def kv_wait(j, r):
        kv_copy(kvq.at[j, r, pl.ds(0, 2)], j, r, cross_send.at[r], sp).wait_recv()

    top = 2 * pair + 1

    def spread(level, r, rises, act):
        @pl.when(rises)
        def _():
            act(up(level, r))

        for k in range(1, Y):

            @pl.when(jnp.logical_or(level < top, y < (y + k) % Y))
            def _():
                act(side(level, r, k))

    def start(copy):
        copy.start()

    def drain(copy):
        copy.wait_send()

    def send_own(r, act):
        act(swap(sp, r))

        @pl.when(bridge_up)
        def _():
            act(cross(r))

        spread(z, r, has_up, act)

    mate_level = z + 1 - 2 * a

    def send_mate(r, act):
        spread(mate_level, r, bridge_up, act)

    def send_below(level, r, act):
        spread(level, r, has_up, act)

    def relay_mate(r):
        swap(mate, r).wait_recv()
        send_mate(r, start)

    def relay_below(level, r):
        kv_wait(level_block(level), r)
        send_below(level, r, start)

    own.wait()
    for load in loads[:5] + loads[9:11]:
        load.wait()
    rim_copy = pltpu.make_async_remote_copy(
        src_ref=tail,
        dst_ref=rim,
        send_sem=rim_sem.at[0],
        recv_sem=rim_sem.at[1],
        device_id={"sp": (sp + 1) % S},
    )
    scale = hd ** (-0.5)

    def chunk(i, carry):
        r = NR - 1 - i
        rows = tok_rows(r)
        for k in range(1, X):
            tok_wait(source(k), r)
            tok_forward(k, r).start()
        tok_wait(sib, r)
        for k in range(1, X):
            tok_wait(source_sib(k), r)
        squares = jnp.zeros((R, 1), F32)
        for t in range(T):
            block = tok[t, rows, :].astype(F32)
            squares = squares + jnp.sum(block * block, axis=1, keepdims=True)
            scaled[rows, t * Dt : (t + 1) * Dt] = (block * gain[:, t * Dt : (t + 1) * Dt]).astype(BF16)
        inverse = lax.rsqrt(squares / Wd + NORM_EPS)
        inv[rows, :] = inverse
        left = scaled[rows, :]
        keys = inverse * dot(left, wk[...])
        values = inverse * dot(left, wv[...])
        queries = inverse * dot(left, wq[...])
        for h in range(H):
            mine = a if h else 1 - a
            slot = sp * mine + S * (1 - mine)
            cols = slice(h * V, (h + 1) * V)
            kvq[slot, r, 0] = rotate(keys[:, cols], rows).astype(BF16)
            kvq[slot, r, 1] = jnp.transpose(values[:, cols]).astype(BF16)
            turned = rotate(queries[:, cols], rows).astype(BF16).astype(F32) * scale
            kvq[slot, r, 2] = jnp.transpose(turned).astype(BF16)
        send_own(r, start)

        @pl.when(i == 0)
        def _():
            edge = pl.ds(L - PAD, PAD)
            inner = (inv[edge, :] * dot(scaled[edge, :], wi[...])).astype(BF16)
            signal = (inv[edge, :] * dot(scaled[edge, :], ws[...])).astype(BF16)
            tail[...] = (inner.astype(F32) * signal.astype(F32)).astype(BF16)

            @pl.when(sp + 1 < S)
            def _():
                rim_copy.start()

        @pl.when(i > 1)
        def _():
            relay_mate(r + 2)

        return carry

    lax.fori_loop(0, NR, chunk, 0)
    for r in reversed(range(NR)):
        ask(sp, r).start()

    def level_at(n):
        odd = n % 2
        return 2 * (pair - 1 - n // 2) + a * (1 - odd) + (1 - a) * odd

    def relay_level(n, rows, when=None):
        wanted = n < 2 * pair
        if when is not None:
            wanted = jnp.logical_and(wanted, when)

        @pl.when(wanted)
        def _():
            for r in rows:
                relay_below(level_at(n), r)

    order = list(reversed(range(NR)))

    loads[5].wait()

    def mix_rows(r):
        return pl.ds(pl.multiple_of(r * M, M), M)

    def gate_chunk(r, carry):
        rows = mix_rows(r)
        inverse = inv[rows, :]
        left = scaled[rows, :]
        inner = (inverse * dot(left, wi[...])).astype(BF16)
        signal = (inverse * dot(left, ws[...])).astype(BF16)
        conv_in = (inner.astype(F32) * signal.astype(F32)).astype(BF16)
        padded[pl.ds(pl.multiple_of(PAD + r * M, PAD), M), :] = conv_in.astype(F32)
        gate[rows, :] = (inverse * dot(left, wo[...])).astype(BF16)
        return carry

    lax.fori_loop(0, NM, gate_chunk, 0)

    @pl.when(sp > 0)
    def _():
        rim_copy.wait_recv()
        padded[0:PAD, :] = rim[...].astype(F32)

    @pl.when(sp == 0)
    def _():
        padded[0:PAD, :] = jnp.zeros((PAD, C), F32)

    summed = jnp.zeros((L, C), F32)
    for j in range(taps_n):
        begin = PAD - (taps_n - 1) + j
        summed = summed + taps[j : j + 1, :] * padded[begin : begin + L, :]
    conv_all[tp, :, :] = (gate[...].astype(F32) * summed).astype(BF16)

    def mix_copy(piece, r, send, target):
        block = conv_all.at[piece, mix_rows(r), :]
        return pltpu.make_async_remote_copy(
            src_ref=block,
            dst_ref=block,
            send_sem=send,
            recv_sem=mix_recv.at[piece, r],
            device_id={"tp": target},
        )

    def mix_own(k, r):
        return mix_copy(tp, r, mix_send.at[k, r], peer(k) if k else sib)

    def mix_forward(k, r):
        return mix_copy(source(k), r, mix_relay.at[k, r], sib)

    def mix_wait(piece, r):
        mix_copy(piece, r, mix_send.at[0, r], sib).wait_recv()

    for r in range(NM):
        for k in list(range(1, X)) + [0]:
            mix_own(k, r).start()

    blank = jnp.zeros((hd, M), BF16)

    def attend(items):
        work = [(item, c) for item in items for c in range(2)]

        def score(item, c):
            chunks, b, part, shift = item
            keys = jnp.concatenate([kvq[j, r, 0] for j, r in chunks], axis=0)
            turned = jnp.concatenate(
                [kvq[level_block(2 * pair + b), G * part + g, 2] for g in range(G)], axis=1
            )
            if c:
                right = jnp.concatenate([blank, turned[hd:]], axis=0)
            else:
                right = jnp.concatenate([turned[:hd], blank], axis=0)
            scores = dot(keys, right)
            if shift is not None:
                key_row = lax.broadcasted_iota(jnp.int32, scores.shape, 0)
                query_lane = lax.broadcasted_iota(jnp.int32, scores.shape, 1)
                scores = jnp.where(key_row <= query_lane + shift, scores, MASKED)
            return scores

        def mix(item, c, fade, weights):
            chunks, b, part, _ = item
            values = jnp.concatenate([kvq[j, r, 1] for j, r in chunks], axis=1)
            acc[b, part, c] = fade * acc[b, part, c] + dot(values, weights)

        ready = [score(*work[0])]
        waiting = []
        for i, (item, c) in enumerate(work):
            for n in range(i + len(ready), min(i + 3, len(work))):
                ready.append(score(*work[n]))
            scores = ready.pop(0)
            _, b, part, _ = item
            old_max = row_max[b, part, c]
            new_max = jnp.maximum(old_max, jnp.max(scores, axis=0, keepdims=True))
            weights = jnp.exp(scores - new_max)
            fade = jnp.exp(old_max - new_max)
            row_max[b, part, c] = new_max
            row_sum[b, part, c] = fade * row_sum[b, part, c] + jnp.sum(weights, axis=0, keepdims=True)
            if waiting:
                mix(*waiting.pop())
            waiting.append((item, c, fade, weights.astype(BF16)))
        mix(*waiting.pop())

    def chunks_of(j, begin=0, end=NR):
        return [(j, r) for r in range(begin, end)]

    low_own = level_block(2 * pair)

    def triangle(j, b):
        return [(chunks_of(j, 0, G * (part + 1)), b, part, M * part) for part in reversed(range(NM))]

    attend(triangle(sp, a))
    for r in reversed(range(2)):
        relay_mate(r)
    relay_level(0, order[:-1])
    relay_level(0, order[-1:], a == 0)
    relay_level(1, order[:1], a == 0)
    for r in range(NR):
        ask(mate, r).wait_recv()
    attend([(chunks_of(low_own), 1, part, None) for part in range(NM)] + triangle(mate, 1 - a))
    relay_level(1, order[1:2], a == 0)

    for k in range(1, Y):
        other = (y + k) % Y
        ahead = other < y
        low = 2 * pair * Y + other
        for r in range(NR):
            kv_wait(low, r)

        late_items = [(chunks_of(low), 1, part, None) for part in range(NM)]

        @pl.when(ahead)
        def _():
            for r in range(NR):
                kv_wait(low + Y, r)
            attend(
                late_items
                + [(chunks_of(low), 0, part, None) for part in range(NM)]
                + [(chunks_of(low + Y), 1, part, None) for part in range(NM)]
            )

        @pl.when(jnp.logical_not(ahead))
        def _():
            attend(late_items)

    relay_level(0, order[-1:], a == 1)
    relay_level(1, order[2:], a == 0)
    for r in range(NM):
        for k in range(1, X):
            mix_wait(source(k), r)
            mix_forward(k, r).start()

    def conv_product():
        loads[6].wait()
        for r in range(NM):
            mix_wait(sib, r)
            for k in range(1, X):
                mix_wait(source_sib(k), r)

        def conv_part(r, carry):
            rows = mix_rows(r)
            part = dot(conv_all[0, rows, :], wc[0:C, :])
            for t in range(1, T):
                part = part + dot(conv_all[t, rows, :], wc[t * C : (t + 1) * C, :])
            total[rows, :] = part
            return carry

        lax.fori_loop(0, NM, conv_part, 0)

    def below(n, carry):
        level = level_at(n)
        later = jnp.logical_or(n > 0, a == 1)

        def item(k, c):
            j = level * Y + (y + k) % Y

            @pl.when(k == 1)
            def _():
                relay_level(n + 1, order[:1], later)

            @pl.when(jnp.logical_and(k == 1, n == 2 * pair - 1))
            def _():
                conv_product()

            @pl.when(k > 0)
            def _():
                for r in order:
                    kv_wait(j, r)

            attend([(chunks_of(j), b, part, None) for b in range(2) for part in range(NM)])
            return c

        lax.fori_loop(0, Y, item, 0)
        relay_level(n + 1, order[1:], later)
        return carry

    lax.fori_loop(0, 2 * pair, below, 0)

    def at_copy(src, piece, h, r, send, target):
        return pltpu.make_async_remote_copy(
            src_ref=src,
            dst_ref=attn_all.at[piece, h, mix_rows(r), :],
            send_sem=send,
            recv_sem=at_recv.at[piece, h, r],
            device_id=target,
        )

    def at_own(k, r):
        target = {"tp": peer(k) if k else sib}
        return at_copy(attn_all.at[tp, a, mix_rows(r), :], tp, a, r, at_send.at[k, r], target)

    def at_off(k, r):
        target = {"sp": mate, "tp": peer(k)}
        return at_copy(away.at[mix_rows(r), :], tp, a, r, at_away.at[k, r], target)

    def at_forward(k, h, r, send):
        piece = source(k)
        return at_copy(attn_all.at[piece, h, mix_rows(r), :], piece, h, r, send, {"tp": sib})

    def at_wait(piece, h, r):
        at_copy(attn_all.at[piece, h, mix_rows(r), :], piece, h, r, at_send.at[0, r], {"tp": sib}).wait_recv()

    def near_forward(k, r):
        return at_forward(k, a, r, at_relay.at[k, r])

    def far_forward(k, r):
        return at_forward(k, 1 - a, r, at_relay_away.at[k, r])

    def finished(b, part):
        first_map = acc[b, part, 0] / row_sum[b, part, 0]
        second_map = acc[b, part, 1] / row_sum[b, part, 1]
        head_mix = first_map - lambdas[a] * second_map
        mean = jnp.mean(head_mix * head_mix, axis=0, keepdims=True)
        normed = head_mix * lax.rsqrt(mean + HEAD_EPS) * gain_t[...] * HEAD_SCALE
        return jnp.transpose(normed).astype(BF16)

    def log_total(b, part, c):
        return row_max[b, part, c] + jnp.log(row_sum[b, part, c])

    for part in range(NM):
        away[part * M : (part + 1) * M, :] = finished(1 - a, part)
        for k in list(range(1, X)) + [0]:
            at_off(k, part).start()
    for part in range(NM):
        attn_all[tp, a, part * M : (part + 1) * M, :] = finished(a, part)
        for k in list(range(1, X)) + [0]:
            at_own(k, part).start()
    for part in range(NM):
        for c in range(2):
            lse_away[c : c + 1, part * M : (part + 1) * M] = log_total(1 - a, part, c)
            lse[a, c : c + 1, part * M : (part + 1) * M] = log_total(a, part, c)
    lse_copy = pltpu.make_async_remote_copy(
        src_ref=lse_away,
        dst_ref=lse_in,
        send_sem=lse_sem.at[0],
        recv_sem=lse_sem.at[1],
        device_id={"sp": mate},
    )
    lse_copy.start()

    loads[7].wait()

    @pl.when(pair == 0)
    def _():
        conv_product()


    for r in range(NM):
        for k in range(1, X):
            at_wait(source(k), a, r)
            near_forward(k, r).start()
    for r in range(NM):
        for k in range(X):
            at_wait(source(k), 1 - a, r)
            far_forward(k, r).start()

    def attn_part(r, carry):
        rows = mix_rows(r)
        for k in range(X):
            at_wait(source_sib(k), a, r)
        for k in range(X):
            at_wait(source_sib(k), 1 - a, r)
        part = total[rows, :]
        for t in range(T):
            both = jnp.concatenate([attn_all[t, h, rows, :] for h in range(H)], axis=1)
            part = part + dot(both, wa[t * C : (t + 1) * C, :])
        result[rows, :] = part.astype(BF16)
        out_copy(r).start()
        return carry

    def out_copy(r):
        return pltpu.make_async_copy(result.at[mix_rows(r), :], out.at[mix_rows(r), :], out_sem.at[r])

    lse_copy.wait_recv()
    lse[1 - a] = lse_in[...]
    lse_done = pltpu.make_async_copy(lse, lse_out, lse_out_sem)
    lse_done.start()
    lax.fori_loop(0, NM, attn_part, 0)
    lse_copy.wait_send()

    for r in range(NR):
        for k in range(X):
            tok_own(k, r).wait_send()
        for k in range(1, X):
            tok_forward(k, r).wait_send()
        send_own(r, drain)
        ask(sp, r).wait_send()
        send_mate(r, drain)

    def drain_level(level, carry):
        for r in range(NR):
            send_below(level, r, drain)
        return carry

    lax.fori_loop(0, 2 * pair, drain_level, 0)

    for r in range(NM):
        for k in range(X):
            mix_own(k, r).wait_send()
            at_own(k, r).wait_send()
            at_off(k, r).wait_send()
            far_forward(k, r).wait_send()
        for k in range(1, X):
            mix_forward(k, r).wait_send()
            near_forward(k, r).wait_send()

    @pl.when(sp + 1 < S)
    def _():
        rim_copy.wait_send()
    lse_done.wait()
    for r in range(NM):
        out_copy(r).wait()


def pair_device(
    dims,
    tokens,
    norm_gain,
    query_weight,
    key_weight,
    value_weight,
    outer_gate_weight,
    inner_gate_weight,
    conv_input_weight,
    conv_taps,
    lambdas,
    head_gain,
    attn_out_weight,
    conv_out_weight,
):
    S, T, Z, Y = dims["S"], dims["T"], dims["Z"], dims["Y"]
    L, Dt = tokens.shape
    H = lambdas.shape[0]
    C = query_weight.shape[1]
    V = C // H
    hd = V // 2
    O = attn_out_weight.shape[1]
    Wd = norm_gain.shape[0]
    R = V
    M = 2 * R
    NR, NM, PAD = L // R, L // M, 16
    X = T // 2
    frequency = ROPE_BASE ** (-np.arange(hd // 2) * 2.0 / hd)
    freq = jnp.asarray(np.tile(frequency, 4)[None, :], F32)
    any_spec = pl.BlockSpec(memory_space=pl.ANY)
    smem = pl.BlockSpec(memory_space=pltpu.SMEM)
    dma = pltpu.SemaphoreType.DMA
    mixed, lse = pl.pallas_call(
        functools.partial(pair_kernel, dict(dims, H=H)),
        out_shape=(
            jax.ShapeDtypeStruct((L, O), BF16),
            jax.ShapeDtypeStruct((H, 2, L), F32),
        ),
        in_specs=[any_spec] * 10 + [smem] + [any_spec] * 3,
        out_specs=(any_spec, any_spec),
        scratch_shapes=[
            pltpu.VMEM((T, L, Dt), BF16),
            pltpu.VMEM((L, Wd), BF16),
            pltpu.VMEM((L, 1), F32),
            pltpu.VMEM((L, V), F32),
            pltpu.VMEM((L, V), F32),
            pltpu.VMEM((V, M), F32),
        ]
        + [pltpu.VMEM((Wd, C), BF16)] * 6
        + [pltpu.VMEM((T * C, O), BF16)] * 2
        + [
            pltpu.VMEM((S + 1, NR, 3, R, V), BF16),
            pltpu.VMEM((2, NM, 2, 1, M), F32),
            pltpu.VMEM((2, NM, 2, 1, M), F32),
            pltpu.VMEM((2, NM, 2, V, M), F32),
            pltpu.VMEM((L, C), BF16),
            pltpu.VMEM((PAD + L, C), F32),
            pltpu.VMEM((PAD, C), BF16),
            pltpu.VMEM((PAD, C), BF16),
            pltpu.VMEM((T, L, C), BF16),
            pltpu.VMEM((T, H, L, V), BF16),
            pltpu.VMEM((L, V), BF16),
            pltpu.VMEM((2, L), F32),
            pltpu.VMEM((2, L), F32),
            pltpu.VMEM((L, O), F32),
            pltpu.VMEM((L, O), BF16),
            pltpu.VMEM((H, 2, L), F32),
            pltpu.VMEM((1, V), F32),
            pltpu.VMEM((1, Wd), F32),
            pltpu.VMEM(conv_taps.shape, F32),
            pltpu.VMEM((1, V), F32),
            dma((12,)),
            dma,
            dma((T, NR)),
            dma((X, NR)),
            dma((X, NR)),
            dma((S, NR)),
            dma((NR,)),
            dma((NR,)),
            dma((NR,)),
            dma((NR,)),
            dma((Z, NR, max(Y - 1, 1))),
            dma((Z, NR)),
            dma((2,)),
            dma((2,)),
            dma((T, NM)),
            dma((X, NM)),
            dma((X, NM)),
            dma((T, H, NM)),
            dma((X, NM)),
            dma((X, NM)),
            dma((X, NM)),
            dma((X, NM)),
            dma((NM,)),
            dma,
        ],
        compiler_params=pltpu.CompilerParams(
            collective_id=0,
            has_side_effects=True,
            vmem_limit_bytes=60 * 1024 * 1024,
        ),
        name="mixer",
    )(
        tokens,
        norm_gain[None, :],
        freq,
        query_weight,
        key_weight,
        value_weight,
        outer_gate_weight,
        inner_gate_weight,
        conv_input_weight,
        conv_taps,
        lambdas,
        head_gain[None, :],
        attn_out_weight,
        conv_out_weight,
    )
    return mixed, lse


def per_device(dims, *arrays):
    tokens, query_weight, lambdas = arrays[0], arrays[2], arrays[9]
    width = query_weight.shape[1] // lambdas.shape[0]
    paired = lambdas.shape[0] == 2 and dims["Z"] % 2 == 0 and dims["T"] % 2 == 0
    paired = paired and width == 128 and tokens.shape[0] % (2 * width) == 0
    return (pair_device if paired else ring_device)(dims, *arrays)


def solution(mesh):
    S, T = mesh.shape["sp"], mesh.shape["tp"]
    Y = max(d for d in range(1, S + 1) if S % d == 0 and d * d <= S)
    dims = {"S": S, "T": T, "Z": S // Y, "Y": Y}
    in_specs = (
        P("sp", "tp"),
        P(),
        P(None, "tp"),
        P(None, "tp"),
        P(None, "tp"),
        P(None, "tp"),
        P(None, "tp"),
        P(None, "tp"),
        P(None, "tp"),
        P("tp"),
        P(),
        P(None, "tp"),
        P(None, "tp"),
    )
    out_specs = (P("sp", "tp"), P("tp", None, "sp"))
    return jax.shard_map(
        functools.partial(per_device, dims),
        mesh=mesh,
        in_specs=in_specs,
        out_specs=out_specs,
        check_vma=False,
    )
```

```python
import functools

import jax
import jax.numpy as jnp
import numpy as np
from jax import lax
from jax.experimental import pallas as pl
from jax.experimental.pallas import tpu as pltpu
from jax.sharding import PartitionSpec as P

NORM_EPS = 1e-06
HEAD_EPS = 1e-05
ROPE_BASE = 500000.0
MASKED = -1e30
HEAD_SCALE = 0.8
F32 = jnp.float32
BF16 = jnp.bfloat16


def dot(a, b):
    return jnp.dot(a, b, preferred_element_type=F32)


def dot_t(a, b):
    return lax.dot_general(a, b, (((1,), (1,)), ((), ())), preferred_element_type=F32)


def ring_kernel(
    dims,
    tokens,
    gain,
    freq,
    wq_h,
    wk_h,
    wv_h,
    wo_h,
    wi_h,
    ws_h,
    taps,
    lambdas,
    head_gain,
    wa_h,
    wc_h,
    out,
    lse,
    tok,
    scaled,
    inv,
    cos_t,
    sin_t,
    wq,
    wk,
    wv,
    wo,
    wi,
    ws,
    wa,
    wc,
    kv,
    qz,
    row_max,
    row_sum,
    acc,
    gate,
    padded,
    tail,
    rim,
    conv_all,
    attn_all,
    total,
    w_sem,
    own_sem,
    tok_recv,
    tok_send,
    tok_relay,
    kv_recv,
    kv_send_z,
    kv_send_y,
    kv_extra,
    rim_sem,
    mix_recv,
    mix_send,
    mix_relay,
):
    S, T, Z, Y, H = dims["S"], dims["T"], dims["Z"], dims["Y"], dims["H"]
    L, Dt = tokens.shape
    Wd = T * Dt
    C = wq_h.shape[1]
    V = C // H
    hd = V // 2
    NR = tok_recv.shape[1]
    R = L // NR
    NM = mix_recv.shape[2]
    M = L // NM
    X = T // 2
    taps_n = taps.shape[0]
    PAD = tail.shape[0]

    sp = lax.axis_index("sp")
    tp = lax.axis_index("tp")
    z = sp // Y
    y = sp % Y
    core = tp % 2
    xi = tp // 2
    sib = xi * 2 + (1 - core)

    def peer(k):
        return ((xi + k) % X) * 2 + core

    def source(k):
        return ((xi - k + X) % X) * 2 + core

    pairs = [(wk_h, wk), (wv_h, wv), (wq_h, wq), (wi_h, wi), (ws_h, ws), (wo_h, wo), (wc_h, wc), (wa_h, wa)]
    own = pltpu.make_async_copy(tokens, tok.at[tp], own_sem)
    own.start()
    loads = [pltpu.make_async_copy(s, d, w_sem.at[i]) for i, (s, d) in enumerate(pairs)]
    for load in loads:
        load.start()

    barrier = pltpu.get_barrier_semaphore()

    def greet(target):
        pl.semaphore_signal(barrier, inc=1, device_id=target)

    for k in range(1, T):
        greet({"tp": (tp + k) % T})
    for k in range(1, Y):
        greet({"sp": z * Y + (y + k) % Y})
    has_up = z + 1 < Z
    has_down = z > 0
    far_up = jnp.logical_and(has_up, y == Y - 1) if Y > 1 else None
    far_down = jnp.logical_and(has_down, y == 0) if Y > 1 else None
    expect = (T - 1) + (Y - 1) + has_up.astype(jnp.int32) + has_down.astype(jnp.int32)

    @pl.when(has_up)
    def _():
        greet({"sp": sp + Y})

    @pl.when(has_down)
    def _():
        greet({"sp": sp - Y})

    if Y > 1:
        expect = expect + far_up.astype(jnp.int32) + far_down.astype(jnp.int32)

        @pl.when(far_up)
        def _():
            greet({"sp": sp + 1})

        @pl.when(far_down)
        def _():
            greet({"sp": sp - 1})

    pl.semaphore_wait(barrier, expect)

    def tok_rows(r):
        return pl.ds(pl.multiple_of(r * R, R), R)

    def tok_copy(src, piece, r, send, target):
        return pltpu.make_async_remote_copy(
            src_ref=src,
            dst_ref=tok.at[piece, tok_rows(r), :],
            send_sem=send,
            recv_sem=tok_recv.at[piece, r],
            device_id={"tp": target},
        )

    def tok_own(k, r):
        target = peer(k) if k else sib
        return tok_copy(tokens.at[tok_rows(r), :], tp, r, tok_send.at[k, r], target)

    def tok_forward(k, r):
        piece = source(k)
        return tok_copy(tok.at[piece, tok_rows(r), :], piece, r, tok_relay.at[k, r], sib)

    def tok_wait(piece, r):
        tok_copy(tok.at[piece, tok_rows(r), :], piece, r, tok_send.at[0, r], sib).wait_recv()

    for r in range(NR):
        for k in list(range(1, X)) + [0]:
            tok_own(k, r).start()

    lane = lax.broadcasted_iota(jnp.int32, (R, V), 1)
    first = (lane % hd) < (hd // 2)

    def table(r, carry):
        base = sp * L + r * R
        pos = (base + lax.broadcasted_iota(jnp.int32, (R, V), 0)).astype(F32)
        angle = pos * freq[...]
        sine = jnp.sin(angle)
        cos_t[tok_rows(r), :] = jnp.cos(angle)
        sin_t[tok_rows(r), :] = jnp.where(first, -sine, sine)
        return carry

    lax.fori_loop(0, NR, table, 0)

    def rotate(block, rows):
        low = (lax.broadcasted_iota(jnp.int32, block.shape, 1) % hd) < (hd // 2)
        other = jnp.where(
            low, pltpu.roll(block, V - hd // 2, 1), pltpu.roll(block, hd // 2, 1)
        )
        return block * cos_t[rows, :] + other * sin_t[rows, :]

    def kv_copy(j, r, send, target):
        block = kv.at[j, tok_rows(r), :]
        return pltpu.make_async_remote_copy(
            src_ref=block,
            dst_ref=block,
            send_sem=send,
            recv_sem=kv_recv.at[j, r],
            device_id={"sp": target},
        )

    def kv_up(dz, r):
        return kv_copy(sp - dz * Y, r, kv_send_z.at[dz, r], sp + Y)

    def kv_side(dz, r, k):
        return kv_copy(sp - dz * Y, r, kv_send_y.at[dz, r, k - 1], z * Y + (y + k) % Y)

    def kv_wait(j, r):
        kv_copy(j, r, kv_send_z.at[0, r], sp).wait_recv()

    EX = NR // 2 if Y == 2 else 0

    def extra(r):
        return kv_copy(0, r, kv_extra.at[r], sp + Y)

    def kv_send(dz, r, act):
        @pl.when(has_up)
        def _():
            act(kv_up(dz, r))

        for k in range(1, Y):
            wanted = jnp.logical_or(dz > 0, y + k < Y)
            if EX:
                other_way = jnp.logical_and(dz == z, jnp.logical_and(dz > 0, r < EX))
                wanted = jnp.logical_and(wanted, jnp.logical_not(jnp.logical_and(y == 0, other_way)))

            @pl.when(wanted)
            def _():
                act(kv_side(dz, r, k))

    def relay(dz, r):
        @pl.when(dz <= z)
        def _():
            kv_wait(sp - dz * Y, r)
            kv_send(dz, r, lambda copy: copy.start())

    def first_relay(r):
        relay(1, r)
        if EX:

            @pl.when(jnp.logical_and(jnp.logical_and(z == 0, y == 1), r < EX))
            def _():
                kv_wait(0, r)

                @pl.when(has_up)
                def _():
                    extra(r).start()

    own.wait()
    loads[0].wait()
    loads[1].wait()

    def key_chunk(r, carry):
        rows = tok_rows(r)
        for k in range(1, X):
            tok_wait(source(k), r)
            tok_forward(k, r).start()
        tok_wait(sib, r)
        for k in range(1, X):
            tok_wait(((xi + k) % X) * 2 + (1 - core), r)
        squares = jnp.zeros((R, 1), F32)
        for t in range(T):
            block = tok[t, rows, :].astype(F32)
            squares = squares + jnp.sum(block * block, axis=1, keepdims=True)
            scaled[rows, t * Dt : (t + 1) * Dt] = (block * gain[:, t * Dt : (t + 1) * Dt]).astype(BF16)
        inverse = lax.rsqrt(squares / Wd + NORM_EPS)
        inv[rows, :] = inverse
        left = scaled[rows, :]
        keys = inverse * dot(left, wk[...])
        for h in range(H):
            kv[sp, rows, h * V : (h + 1) * V] = rotate(keys[:, h * V : (h + 1) * V], rows).astype(BF16)
        kv[sp, rows, C : 2 * C] = (inverse * dot(left, wv[...])).astype(BF16)
        kv_send(0, r, lambda copy: copy.start())

        @pl.when(r > 0)
        def _():
            first_relay(r - 1)

        return carry

    lax.fori_loop(0, NR, key_chunk, 0)

    for load in loads[2:6]:
        load.wait()
    half = lax.broadcasted_iota(jnp.int32, (M, V), 1) < hd
    scale = hd ** (-0.5)

    def mix_rows(r):
        return pl.ds(pl.multiple_of(r * M, M), M)

    def query_chunk(r, carry):
        rows = mix_rows(r)
        inverse = inv[rows, :]
        left = scaled[rows, :]
        queries = inverse * dot(left, wq[...])
        for h in range(H):
            turned = rotate(queries[:, h * V : (h + 1) * V], rows).astype(BF16).astype(F32) * scale
            qz[h, 0, rows, :] = jnp.where(half, turned, 0.0).astype(BF16)
            qz[h, 1, rows, :] = jnp.where(half, 0.0, turned).astype(BF16)
        inner = (inverse * dot(left, wi[...])).astype(BF16)
        signal = (inverse * dot(left, ws[...])).astype(BF16)
        conv_in = (inner.astype(F32) * signal.astype(F32)).astype(BF16)
        padded[pl.ds(pl.multiple_of(PAD + r * M, PAD), M), :] = conv_in.astype(F32)
        gate[rows, :] = (inverse * dot(left, wo[...])).astype(BF16)

        @pl.when(r == 0)
        def _():
            first_relay(NR - 1)

        return carry

    lax.fori_loop(0, NM, query_chunk, 0)
    tail[...] = padded[L : L + PAD, :].astype(BF16)
    rim_copy = pltpu.make_async_remote_copy(
        src_ref=tail,
        dst_ref=rim,
        send_sem=rim_sem.at[0],
        recv_sem=rim_sem.at[1],
        device_id={"sp": (sp + 1) % S},
    )

    @pl.when(sp + 1 < S)
    def _():
        rim_copy.start()

    def attend(j, diagonal):
        def one(i, carry):
            rows = mix_rows(i)
            for h in range(H):
                query = qz[h, :, rows, :].reshape(2 * M, V)
                scores = dot_t(query, kv[j, :, h * V : (h + 1) * V])
                if diagonal:
                    row = lax.broadcasted_iota(jnp.int32, scores.shape, 0)
                    row = jnp.where(row >= M, row - M, row) + i * M
                    col = lax.broadcasted_iota(jnp.int32, scores.shape, 1)
                    scores = jnp.where(row >= col, scores, MASKED)
                    new_max = jnp.max(scores, axis=1, keepdims=True)
                else:
                    old_max = row_max[h, :, rows, :].reshape(2 * M, 1)
                    new_max = jnp.maximum(old_max, jnp.max(scores, axis=1, keepdims=True))
                weights = jnp.exp(scores - new_max)
                sums = jnp.sum(weights, axis=1, keepdims=True)
                mixed = dot(weights.astype(BF16), kv[j, :, C + h * V : C + (h + 1) * V])
                if not diagonal:
                    fade = jnp.exp(old_max - new_max)
                    sums = sums + fade * row_sum[h, :, rows, :].reshape(2 * M, 1)
                    mixed = mixed + fade * acc[h, :, rows, :].reshape(2 * M, V)
                row_max[h, :, rows, :] = new_max.reshape(2, M, 1)
                row_sum[h, :, rows, :] = sums.reshape(2, M, 1)
                acc[h, :, rows, :] = mixed.reshape(2, M, V)
            return carry

        lax.fori_loop(0, NM, one, 0)

    attend(sp, True)

    @pl.when(sp > 0)
    def _():
        rim_copy.wait_recv()
        padded[0:PAD, :] = rim[...].astype(F32)

    @pl.when(sp == 0)
    def _():
        padded[0:PAD, :] = jnp.zeros((PAD, C), F32)

    summed = jnp.zeros((L, C), F32)
    for j in range(taps_n):
        begin = PAD - (taps_n - 1) + j
        summed = summed + taps[j : j + 1, :] * padded[begin : begin + L, :]
    conv_all[tp, :, :] = (gate[...].astype(F32) * summed).astype(BF16)

    def mix_copy(which, buf, piece, r, send, target):
        block = buf.at[piece, mix_rows(r), :]
        return pltpu.make_async_remote_copy(
            src_ref=block,
            dst_ref=block,
            send_sem=send,
            recv_sem=mix_recv.at[which, piece, r],
            device_id={"tp": target},
        )

    def mix_own(which, buf, k, r):
        target = peer(k) if k else sib
        return mix_copy(which, buf, tp, r, mix_send.at[which, k, r], target)

    def mix_forward(which, buf, k, r):
        return mix_copy(which, buf, source(k), r, mix_relay.at[which, k, r], sib)

    def mix_wait(which, buf, piece, r):
        mix_copy(which, buf, piece, r, mix_send.at[which, 0, r], sib).wait_recv()

    for r in range(NM):
        for k in list(range(1, X)) + [0]:
            mix_own(0, conv_all, k, r).start()

    def step(dz, carry):
        def row_block(k, inner):
            def forward(r, c):
                relay(dz + 1, r)
                return c

            lax.fori_loop(k * NR // Y, (k + 1) * NR // Y, forward, 0)
            side = (y + k) % Y
            level = jnp.where(k == 0, z - dz, z - dz + 1)
            j = level * Y + side
            valid = jnp.where(k == 0, dz <= z, jnp.logical_or(level < z, side < y))

            @pl.when(valid)
            def _():
                @pl.when(k > 0)
                def _():
                    for r in range(NR):
                        if r < EX:
                            climbs = jnp.logical_and(level == 0, y == 1)

                            @pl.when(jnp.logical_not(jnp.logical_and(climbs, z == 0)))
                            def _():
                                kv_wait(j, r)

                            @pl.when(jnp.logical_and(climbs, jnp.logical_and(z > 0, has_up)))
                            def _():
                                extra(r).start()

                        else:
                            kv_wait(j, r)

                attend(j, False)

            return inner

        lax.fori_loop(0, Y, row_block, 0)
        return carry

    lax.fori_loop(1, z + 2, step, 0)

    def finish(i, carry):
        rows = mix_rows(i)
        for h in range(H):
            first_map = acc[h, 0, rows, :] / row_sum[h, 0, rows, :]
            second_map = acc[h, 1, rows, :] / row_sum[h, 1, rows, :]
            head_mix = first_map - lambdas[h] * second_map
            mean = jnp.mean(head_mix * head_mix, axis=1, keepdims=True)
            normed = head_mix * lax.rsqrt(mean + HEAD_EPS) * head_gain[...] * HEAD_SCALE
            attn_all[tp, rows, h * V : (h + 1) * V] = normed.astype(BF16)
        for k in list(range(1, X)) + [0]:
            mix_own(1, attn_all, k, i).start()
        return carry

    lax.fori_loop(0, NM, finish, 0)

    loads[6].wait()
    loads[7].wait()

    def gather(which, buf, r):
        for k in range(1, X):
            mix_wait(which, buf, source(k), r)
            mix_forward(which, buf, k, r).start()

    def gather_rest(which, buf, r):
        mix_wait(which, buf, sib, r)
        for k in range(1, X):
            mix_wait(which, buf, ((xi + k) % X) * 2 + (1 - core), r)

    def conv_part(r, carry):
        rows = mix_rows(r)
        gather(0, conv_all, r)
        gather_rest(0, conv_all, r)
        part = dot(conv_all[0, rows, :], wc[0:C, :])
        for t in range(1, T):
            part = part + dot(conv_all[t, rows, :], wc[t * C : (t + 1) * C, :])
        total[rows, :] = part
        return carry

    lax.fori_loop(0, NM, conv_part, 0)

    lanes = lax.broadcasted_iota(jnp.int32, (L, 128), 1)
    columns = jnp.zeros((L, 128), F32)
    for h in range(H):
        for c in range(2):
            value = row_max[h, c, :, :] + jnp.log(row_sum[h, c, :, :])
            columns = jnp.where(lanes == 2 * h + c, value, columns)
    turned_columns = jnp.transpose(columns)
    for h in range(H):
        lse[h] = turned_columns[2 * h : 2 * h + 2, :]

    def attn_part(r, carry):
        rows = mix_rows(r)
        gather(1, attn_all, r)
        gather_rest(1, attn_all, r)
        part = total[rows, :]
        for t in range(T):
            part = part + dot(attn_all[t, rows, :], wa[t * C : (t + 1) * C, :])
        out[rows, :] = part.astype(BF16)
        return carry

    lax.fori_loop(0, NM, attn_part, 0)

    for r in range(NR):
        for k in range(X):
            tok_own(k, r).wait_send()
        for k in range(1, X):
            tok_forward(k, r).wait_send()

    def drain(dz, carry):
        def inner(r, c):
            kv_send(dz, r, lambda copy: copy.wait_send())
            return c

        return lax.fori_loop(0, NR, inner, carry)

    lax.fori_loop(0, z + 1, drain, 0)
    if EX:

        @pl.when(jnp.logical_and(y == 1, has_up))
        def _():
            for r in range(EX):
                extra(r).wait_send()

    for which, buf in ((0, conv_all), (1, attn_all)):
        for r in range(NM):
            for k in range(X):
                mix_own(which, buf, k, r).wait_send()
            for k in range(1, X):
                mix_forward(which, buf, k, r).wait_send()

    @pl.when(sp + 1 < S)
    def _():
        rim_copy.wait_send()


def ring_device(
    dims,
    tokens,
    norm_gain,
    query_weight,
    key_weight,
    value_weight,
    outer_gate_weight,
    inner_gate_weight,
    conv_input_weight,
    conv_taps,
    lambdas,
    head_gain,
    attn_out_weight,
    conv_out_weight,
):
    S, T, Z, Y = dims["S"], dims["T"], dims["Z"], dims["Y"]
    L, Dt = tokens.shape
    H = lambdas.shape[0]
    C = query_weight.shape[1]
    V = C // H
    hd = V // 2
    O = attn_out_weight.shape[1]
    Wd = norm_gain.shape[0]
    NR, NM, PAD = 4, 2, 16
    X = T // 2
    frequency = ROPE_BASE ** (-np.arange(hd // 2) * 2.0 / hd)
    freq = jnp.asarray(np.tile(frequency, 4)[None, :], F32)
    any_spec = pl.BlockSpec(memory_space=pl.ANY)
    vmem = pl.BlockSpec(memory_space=pltpu.VMEM)
    smem = pl.BlockSpec(memory_space=pltpu.SMEM)
    dma = pltpu.SemaphoreType.DMA
    mixed, lse = pl.pallas_call(
        functools.partial(ring_kernel, dict(dims, H=H)),
        out_shape=(
            jax.ShapeDtypeStruct((L, O), BF16),
            jax.ShapeDtypeStruct((H, 2, L), F32),
        ),
        in_specs=[any_spec, vmem, vmem] + [any_spec] * 6 + [vmem, smem, vmem] + [any_spec] * 2,
        out_specs=(vmem, vmem),
        scratch_shapes=[
            pltpu.VMEM((T, L, Dt), BF16),
            pltpu.VMEM((L, Wd), BF16),
            pltpu.VMEM((L, 1), F32),
            pltpu.VMEM((L, V), F32),
            pltpu.VMEM((L, V), F32),
        ]
        + [pltpu.VMEM((Wd, C), BF16)] * 6
        + [pltpu.VMEM((T * C, O), BF16)] * 2
        + [
            pltpu.VMEM((S, L, 2 * C), BF16),
            pltpu.VMEM((H, 2, L, V), BF16),
            pltpu.VMEM((H, 2, L, 1), F32),
            pltpu.VMEM((H, 2, L, 1), F32),
            pltpu.VMEM((H, 2, L, V), F32),
            pltpu.VMEM((L, C), BF16),
            pltpu.VMEM((PAD + L, C), F32),
            pltpu.VMEM((PAD, C), BF16),
            pltpu.VMEM((PAD, C), BF16),
            pltpu.VMEM((T, L, C), BF16),
            pltpu.VMEM((T, L, C), BF16),
            pltpu.VMEM((L, O), F32),
            dma((8,)),
            dma,
            dma((T, NR)),
            dma((X, NR)),
            dma((X, NR)),
            dma((S, NR)),
            dma((Z, NR)),
            dma((Z, NR, max(Y - 1, 1))),
            dma((NR,)),
            dma((2,)),
            dma((2, T, NM)),
            dma((2, X, NM)),
            dma((2, X, NM)),
        ],
        compiler_params=pltpu.CompilerParams(
            collective_id=0, has_side_effects=True, vmem_limit_bytes=60 * 1024 * 1024
        ),
        name="mixer",
    )(
        tokens,
        norm_gain[None, :],
        freq,
        query_weight,
        key_weight,
        value_weight,
        outer_gate_weight,
        inner_gate_weight,
        conv_input_weight,
        conv_taps,
        lambdas,
        head_gain[None, :],
        attn_out_weight,
        conv_out_weight,
    )
    return mixed, lse


def pair_kernel(
    dims,
    tokens,
    gain_h,
    freq_h,
    wq_h,
    wk_h,
    wv_h,
    wo_h,
    wi_h,
    ws_h,
    taps_h,
    lambdas,
    head_gain_h,
    wa_h,
    wc_h,
    out,
    lse,
    tok,
    scaled,
    inv,
    cos_t,
    sin_t,
    gain_t,
    wq,
    wk,
    wv,
    wo,
    wi,
    ws,
    wa,
    wc,
    kvq,
    row_max,
    row_sum,
    acc,
    gate,
    padded,
    tail,
    rim,
    conv_all,
    attn_all,
    away,
    lse_away,
    lse_in,
    total,
    freq,
    gain,
    taps,
    head_gain,
    w_sem,
    own_sem,
    tok_recv,
    tok_send,
    tok_relay,
    kv_recv,
    swap_send,
    ask_recv,
    cross_send,
    side_send,
    up_send,
    rim_sem,
    lse_sem,
    mix_recv,
    mix_send,
    mix_relay,
    at_recv,
    at_send,
    at_away,
    at_relay,
    at_relay_away,
):
    S, T, Z, Y, H = dims["S"], dims["T"], dims["Z"], dims["Y"], dims["H"]
    L, Dt = tokens.shape
    Wd = T * Dt
    C = wq_h.shape[1]
    V = C // H
    hd = V // 2
    NR = tok_recv.shape[1]
    R = L // NR
    NM = at_recv.shape[2]
    M = L // NM
    G = M // R
    X = T // 2
    taps_n = taps.shape[0]
    PAD = tail.shape[0]

    sp = lax.axis_index("sp")
    tp = lax.axis_index("tp")
    z = sp // Y
    y = sp % Y
    pair = z // 2
    a = z % 2
    mate = sp + (1 - 2 * a) * Y
    core = tp % 2
    xi = tp // 2
    sib = xi * 2 + (1 - core)
    has_up = z + 2 - a < Z
    has_down = pair > 0

    def peer(k):
        return ((xi + k) % X) * 2 + core

    def source(k):
        return ((xi - k + X) % X) * 2 + core

    def source_sib(k):
        return ((xi - k + X) % X) * 2 + (1 - core)

    barrier = pltpu.get_barrier_semaphore()

    def greet(target):
        pl.semaphore_signal(barrier, inc=1, device_id=target)

    for k in range(1, T):
        greet({"tp": (tp + k) % T})
    for k in range(X):
        greet({"sp": mate, "tp": peer(k)})
    for k in range(1, Y):
        greet({"sp": z * Y + (y + k) % Y})
    expect = (T - 1) + X + (Y - 1)
    bridge_up = jnp.logical_and(a == 1, has_up)
    bridge_down = jnp.logical_and(a == 0, has_down)
    for near, step in (
        (has_up, 2 * Y),
        (has_down, -2 * Y),
        (bridge_up, Y),
        (bridge_down, -Y),
        (sp + 1 < S, 1),
        (sp > 0, -1),
    ):
        expect = expect + near.astype(jnp.int32)

        @pl.when(near)
        def _():
            greet({"sp": sp + step})

    pairs = [(wk_h, wk), (wv_h, wv), (wq_h, wq), (wi_h, wi), (ws_h, ws), (wo_h, wo), (wc_h, wc), (wa_h, wa)]
    pairs = pairs + [(freq_h, freq), (gain_h, gain), (taps_h, taps), (head_gain_h, head_gain)]
    own = pltpu.make_async_copy(tokens, tok.at[tp], own_sem)
    own.start()
    loads = [pltpu.make_async_copy(s, d, w_sem.at[i]) for i, (s, d) in enumerate(pairs)]
    for load in loads[8:] + loads[:8]:
        load.start()

    pl.semaphore_wait(barrier, expect)

    def tok_rows(r):
        return pl.ds(pl.multiple_of(r * R, R), R)

    def tok_copy(src, piece, r, send, target):
        return pltpu.make_async_remote_copy(
            src_ref=src,
            dst_ref=tok.at[piece, tok_rows(r), :],
            send_sem=send,
            recv_sem=tok_recv.at[piece, r],
            device_id={"tp": target},
        )

    def tok_own(k, r):
        target = peer(k) if k else sib
        return tok_copy(tokens.at[tok_rows(r), :], tp, r, tok_send, target)

    def tok_forward(k, r):
        piece = source(k)
        return tok_copy(tok.at[piece, tok_rows(r), :], piece, r, tok_relay, sib)

    def tok_wait(piece, r):
        tok_copy(tok.at[piece, tok_rows(r), :], piece, r, tok_send, sib).wait_recv()

    for r in reversed(range(NR)):
        for k in list(range(1, X)) + [0]:
            tok_own(k, r).start()

    lane = lax.broadcasted_iota(jnp.int32, (R, V), 1)
    first = (lane % hd) < (hd // 2)

    loads[8].wait()
    loads[11].wait()

    def table(r, carry):
        base = sp * L + r * R
        pos = (base + lax.broadcasted_iota(jnp.int32, (R, V), 0)).astype(F32)
        angle = pos * freq[...]
        sine = jnp.sin(angle)
        cos_t[tok_rows(r), :] = jnp.cos(angle)
        sin_t[tok_rows(r), :] = jnp.where(first, -sine, sine)
        return carry

    lax.fori_loop(0, NR, table, 0)
    gain_t[...] = jnp.transpose(jnp.broadcast_to(head_gain[...], (M, V)))

    row_max[...] = jnp.full(row_max.shape, MASKED, F32)
    row_sum[...] = jnp.zeros(row_sum.shape, F32)
    acc[...] = jnp.zeros(acc.shape, F32)

    def rotate(block, rows):
        other = jnp.where(first, pltpu.roll(block, V - hd // 2, 1), pltpu.roll(block, hd // 2, 1))
        return block * cos_t[rows, :] + other * sin_t[rows, :]

    def kv_copy(src, j, r, send, target):
        return pltpu.make_async_remote_copy(
            src_ref=src,
            dst_ref=kvq.at[j, r, pl.ds(0, 2)],
            send_sem=send,
            recv_sem=kv_recv.at[j, r],
            device_id={"sp": target},
        )

    def sent(ref, sem):
        pltpu.make_async_remote_copy(
            src_ref=ref, dst_ref=ref, send_sem=sem, recv_sem=sem, device_id={"sp": mate}
        ).wait_send()

    def swap(j, r):
        return pltpu.make_async_remote_copy(
            src_ref=kvq.at[S, r, pl.ds(0, 2)],
            dst_ref=kvq.at[j, r, pl.ds(0, 2)],
            send_sem=swap_send,
            recv_sem=kv_recv.at[j, r],
            device_id={"sp": mate},
        )

    def ask(j, r):
        return pltpu.make_async_remote_copy(
            src_ref=kvq.at[S, r, 2],
            dst_ref=kvq.at[j, r, 2],
            send_sem=swap_send,
            recv_sem=ask_recv,
            device_id={"sp": mate},
        )

    def cross(r):
        return kv_copy(kvq.at[S, r, pl.ds(0, 2)], sp, r, cross_send, sp + Y)

    def level_block(level):
        return level * Y + y

    def up(level, r):
        j = level_block(level)
        return kv_copy(kvq.at[j, r, pl.ds(0, 2)], j, r, up_send.at[level], sp + 2 * Y)

    def side(level, r, k):
        j = level_block(level)
        return kv_copy(
            kvq.at[j, r, pl.ds(0, 2)], j, r, side_send.at[level, k - 1], z * Y + (y + k) % Y
        )

    def kv_wait(j, r):
        kv_copy(kvq.at[j, r, pl.ds(0, 2)], j, r, cross_send, mate).wait_recv()

    def beside_wait(level, k, r):
        kv_wait(level * Y + (y + k) % Y, r)

    top = 2 * pair + 1

    def spread(level, r, rises):
        @pl.when(rises)
        def _():
            up(level, r).start()

        for k in range(1, Y):

            @pl.when(jnp.logical_or(level < top, y < (y + k) % Y))
            def _():
                side(level, r, k).start()

    def spread_done(level, rises):
        whole = kvq.at[level_block(level), :, pl.ds(0, 2)]

        @pl.when(rises)
        def _():
            sent(whole, up_send.at[level])

        for k in range(1, Y):

            @pl.when(jnp.logical_or(level < top, y < (y + k) % Y))
            def _():
                sent(whole, side_send.at[level, k - 1])

    def send_own(r):
        swap(sp, r).start()

        @pl.when(bridge_up)
        def _():
            cross(r).start()

        spread(z, r, has_up)

    mate_level = z + 1 - 2 * a

    def relay_mate(r):
        swap(mate, r).wait_recv()
        spread(mate_level, r, bridge_up)

    def relay_below(level, r):
        kv_wait(level_block(level), r)
        spread(level, r, has_up)

    own.wait()
    for load in loads[:5] + loads[9:11]:
        load.wait()
    rim_copy = pltpu.make_async_remote_copy(
        src_ref=tail,
        dst_ref=rim,
        send_sem=rim_sem.at[0],
        recv_sem=rim_sem.at[1],
        device_id={"sp": (sp + 1) % S},
    )
    scale = hd ** (-0.5)

    def chunk(i, carry):
        r = NR - 1 - i
        rows = tok_rows(r)
        for k in range(1, X):
            tok_wait(source(k), r)
            tok_forward(k, r).start()
        tok_wait(sib, r)
        for k in range(1, X):
            tok_wait(source_sib(k), r)
        squares = jnp.zeros((R, 1), F32)
        for t in range(T):
            block = tok[t, rows, :].astype(F32)
            squares = squares + jnp.sum(block * block, axis=1, keepdims=True)
            scaled[rows, t * Dt : (t + 1) * Dt] = (block * gain[:, t * Dt : (t + 1) * Dt]).astype(BF16)
        inverse = lax.rsqrt(squares / Wd + NORM_EPS)
        inv[rows, :] = inverse
        left = scaled[rows, :]
        keys = inverse * dot(left, wk[...])
        values = inverse * dot(left, wv[...])
        for h in range(H):
            mine = a if h else 1 - a
            slot = sp * mine + S * (1 - mine)
            cols = slice(h * V, (h + 1) * V)
            kvq[slot, r, 0] = rotate(keys[:, cols], rows).astype(BF16)
            kvq[slot, r, 1] = jnp.transpose(values[:, cols]).astype(BF16)
        send_own(r)
        queries = inverse * dot(left, wq[...])
        for h in range(H):
            mine = a if h else 1 - a
            slot = sp * mine + S * (1 - mine)
            cols = slice(h * V, (h + 1) * V)
            turned = rotate(queries[:, cols], rows).astype(BF16).astype(F32) * scale
            kvq[slot, r, 2] = jnp.transpose(turned).astype(BF16)

        @pl.when(i == 0)
        def _():
            edge = pl.ds(L - PAD, PAD)
            inner = (inv[edge, :] * dot(scaled[edge, :], wi[...])).astype(BF16)
            signal = (inv[edge, :] * dot(scaled[edge, :], ws[...])).astype(BF16)
            tail[...] = (inner.astype(F32) * signal.astype(F32)).astype(BF16)

            @pl.when(sp + 1 < S)
            def _():
                rim_copy.start()

        @pl.when(i > 1)
        def _():
            relay_mate(r + 2)

        return carry

    lax.fori_loop(0, NR, chunk, 0)
    for r in reversed(range(NR)):
        ask(sp, r).start()

    def level_at(n):
        odd = n % 2
        return 2 * (pair - 1 - n // 2) + a * (1 - odd) + (1 - a) * odd

    def relay_level(n, rows, when=None):
        wanted = n < 2 * pair
        if when is not None:
            wanted = jnp.logical_and(wanted, when)

        @pl.when(wanted)
        def _():
            for r in rows:
                relay_below(level_at(n), r)

    order = list(reversed(range(NR)))

    loads[5].wait()

    def mix_rows(r):
        return pl.ds(pl.multiple_of(r * M, M), M)

    def gate_chunk(r, carry):
        rows = mix_rows(r)
        inverse = inv[rows, :]
        left = scaled[rows, :]
        inner = (inverse * dot(left, wi[...])).astype(BF16)
        signal = (inverse * dot(left, ws[...])).astype(BF16)
        conv_in = (inner.astype(F32) * signal.astype(F32)).astype(BF16)
        padded[pl.ds(pl.multiple_of(PAD + r * M, PAD), M), :] = conv_in.astype(F32)
        gate[rows, :] = (inverse * dot(left, wo[...])).astype(BF16)
        return carry

    lax.fori_loop(0, NM, gate_chunk, 0)

    @pl.when(sp > 0)
    def _():
        rim_copy.wait_recv()
        padded[0:PAD, :] = rim[...].astype(F32)

    @pl.when(sp == 0)
    def _():
        padded[0:PAD, :] = jnp.zeros((PAD, C), F32)

    summed = jnp.zeros((L, C), F32)
    for j in range(taps_n):
        begin = PAD - (taps_n - 1) + j
        summed = summed + taps[j : j + 1, :] * padded[begin : begin + L, :]
    conv_all[tp, :, :] = (gate[...].astype(F32) * summed).astype(BF16)

    def mix_copy(piece, send, target):
        block = conv_all.at[piece]
        return pltpu.make_async_remote_copy(
            src_ref=block,
            dst_ref=block,
            send_sem=send,
            recv_sem=mix_recv.at[piece],
            device_id={"tp": target},
        )

    def mix_own(k):
        return mix_copy(tp, mix_send, peer(k) if k else sib)

    def mix_forward(k):
        return mix_copy(source(k), mix_relay, sib)

    def mix_wait(piece):
        mix_copy(piece, mix_send, sib).wait_recv()

    for k in list(range(1, X)) + [0]:
        mix_own(k).start()

    blank = jnp.zeros((hd, M), BF16)

    def attend(items):
        work = [(item, c) for item in items for c in range(2)]

        def score(item, c):
            chunks, b, part, shift = item
            keys = jnp.concatenate([kvq[j, r, 0] for j, r in chunks], axis=0)
            turned = jnp.concatenate(
                [kvq[level_block(2 * pair + b), G * part + g, 2] for g in range(G)], axis=1
            )
            if c:
                right = jnp.concatenate([blank, turned[hd:]], axis=0)
            else:
                right = jnp.concatenate([turned[:hd], blank], axis=0)
            scores = dot(keys, right)
            if shift is not None:
                key_row = lax.broadcasted_iota(jnp.int32, scores.shape, 0)
                query_lane = lax.broadcasted_iota(jnp.int32, scores.shape, 1)
                scores = jnp.where(key_row <= query_lane + shift, scores, MASKED)
            return scores

        def mix(item, c, fade, weights):
            chunks, b, part, _ = item
            values = jnp.concatenate([kvq[j, r, 1] for j, r in chunks], axis=1)
            acc[b, part, c] = fade * acc[b, part, c] + dot(values, weights)

        ready = [score(*work[0])]
        waiting = []
        for i, (item, c) in enumerate(work):
            for n in range(i + len(ready), min(i + 3, len(work))):
                ready.append(score(*work[n]))
            scores = ready.pop(0)
            _, b, part, _ = item
            old_max = row_max[b, part, c]
            new_max = jnp.maximum(old_max, jnp.max(scores, axis=0, keepdims=True))
            weights = jnp.exp(scores - new_max)
            fade = jnp.exp(old_max - new_max)
            row_max[b, part, c] = new_max
            row_sum[b, part, c] = fade * row_sum[b, part, c] + jnp.sum(weights, axis=0, keepdims=True)
            if waiting:
                mix(*waiting.pop())
            waiting.append((item, c, fade, weights.astype(BF16)))
        mix(*waiting.pop())

    def chunks_of(j, begin=0, end=NR):
        return [(j, r) for r in range(begin, end)]

    low_own = level_block(2 * pair)

    def triangle(j, b):
        return [(chunks_of(j, 0, G * (part + 1)), b, part, M * part) for part in reversed(range(NM))]

    attend(triangle(sp, a))
    for r in reversed(range(2)):
        relay_mate(r)
    relay_level(0, order[:-1])
    relay_level(0, order[-1:], a == 0)
    relay_level(1, order[:1], a == 0)
    asked = kvq.at[mate, :, 2]
    pltpu.make_async_remote_copy(
        src_ref=asked, dst_ref=asked, send_sem=swap_send, recv_sem=ask_recv, device_id={"sp": mate}
    ).wait_recv()
    attend([(chunks_of(low_own), 1, part, None) for part in range(NM)] + triangle(mate, 1 - a))
    relay_level(1, order[1:2], a == 0)

    for k in range(1, Y):
        other = (y + k) % Y
        ahead = other < y
        low = 2 * pair * Y + other
        for r in range(NR):
            kv_wait(low, r)

        late_items = [(chunks_of(low), 1, part, None) for part in range(NM)]

        @pl.when(ahead)
        def _():
            for r in range(NR):
                kv_wait(low + Y, r)
            attend(
                late_items
                + [(chunks_of(low), 0, part, None) for part in range(NM)]
                + [(chunks_of(low + Y), 1, part, None) for part in range(NM)]
            )

        @pl.when(jnp.logical_not(ahead))
        def _():
            attend(late_items)

    relay_level(0, order[-1:], a == 1)
    relay_level(1, order[2:], a == 0)
    for k in range(1, X):
        mix_wait(source(k))
        mix_forward(k).start()

    def conv_product():
        loads[6].wait()
        mix_wait(sib)
        for k in range(1, X):
            mix_wait(source_sib(k))

        def conv_part(r, carry):
            rows = mix_rows(r)
            part = dot(conv_all[0, rows, :], wc[0:C, :])
            for t in range(1, T):
                part = part + dot(conv_all[t, rows, :], wc[t * C : (t + 1) * C, :])
            total[rows, :] = part
            return carry

        lax.fori_loop(0, NM, conv_part, 0)

    def at_copy(src, piece, h, r, send, target):
        return pltpu.make_async_remote_copy(
            src_ref=src,
            dst_ref=attn_all.at[piece, h, mix_rows(r), :],
            send_sem=send,
            recv_sem=at_recv.at[piece, h, r],
            device_id=target,
        )

    def at_own(k, r):
        target = {"tp": peer(k) if k else sib}
        return at_copy(attn_all.at[tp, a, mix_rows(r), :], tp, a, r, at_send, target)

    def at_off(k, r):
        target = {"sp": mate, "tp": peer(k)}
        return at_copy(away.at[mix_rows(r), :], tp, a, r, at_away, target)

    def at_forward(k, h, r, send):
        piece = source(k)
        return at_copy(attn_all.at[piece, h, mix_rows(r), :], piece, h, r, send, {"tp": sib})

    def at_wait(piece, h, r):
        at_copy(attn_all.at[piece, h, mix_rows(r), :], piece, h, r, at_send, {"tp": sib}).wait_recv()

    def near_forward(k, r):
        return at_forward(k, a, r, at_relay)

    def far_forward(k, r):
        return at_forward(k, 1 - a, r, at_relay_away)

    def finished(b, part):
        first_map = acc[b, part, 0] / row_sum[b, part, 0]
        second_map = acc[b, part, 1] / row_sum[b, part, 1]
        head_mix = first_map - lambdas[a] * second_map
        mean = jnp.mean(head_mix * head_mix, axis=0, keepdims=True)
        normed = head_mix * lax.rsqrt(mean + HEAD_EPS) * gain_t[...] * HEAD_SCALE
        return jnp.transpose(normed).astype(BF16)

    def log_total(b, part, c):
        return row_max[b, part, c] + jnp.log(row_sum[b, part, c])

    def send_away():
        for part in range(NM):
            away[part * M : (part + 1) * M, :] = finished(1 - a, part)
            for k in list(range(1, X)) + [0]:
                at_off(k, part).start()

    def below(n, carry):
        level = level_at(n)
        later = jnp.logical_or(n > 0, a == 1)

        def item(k, c):
            j = level * Y + (y + k) % Y
            final = jnp.logical_and(k == Y - 1, n == 2 * pair - 1)

            @pl.when(k == 1)
            def _():
                relay_level(n + 1, order[:2], later)

            @pl.when(final)
            def _():
                conv_product()

            @pl.when(jnp.logical_and(k > 0, jnp.logical_not(final)))
            def _():
                for r in order:
                    beside_wait(level, k, r)
                relay_level(n + 1, order[2:3], later)

            @pl.when(jnp.logical_not(final))
            def _():
                attend([(chunks_of(j), b, part, None) for b in range(2) for part in range(NM)])

            @pl.when(final)
            def _():
                soon = [(j, r) for r in order[:-1]]
                for r in order[:-1]:
                    beside_wait(level, k, r)
                attend([(soon, b, part, None) for b in range(2) for part in range(NM)])
                beside_wait(level, k, order[-1])
                attend([([(j, order[-1])], 1 - a, part, None) for part in range(NM)])
                send_away()
                attend([([(j, order[-1])], a, part, None) for part in range(NM)])

            return c

        lax.fori_loop(0, Y, item, 0)
        relay_level(n + 1, order[3:], later)
        return carry

    lax.fori_loop(0, 2 * pair, below, 0)

    @pl.when(pair == 0)
    def _():
        send_away()

    for part in range(NM):
        attn_all[tp, a, part * M : (part + 1) * M, :] = finished(a, part)
        for k in list(range(1, X)) + [0]:
            at_own(k, part).start()
    for part in range(NM):
        for c in range(2):
            lse_away[c : c + 1, part * M : (part + 1) * M] = log_total(1 - a, part, c)
            lse[a, c : c + 1, part * M : (part + 1) * M] = log_total(a, part, c)
    lse_copy = pltpu.make_async_remote_copy(
        src_ref=lse_away,
        dst_ref=lse_in,
        send_sem=lse_sem.at[0],
        recv_sem=lse_sem.at[1],
        device_id={"sp": mate},
    )
    lse_copy.start()

    loads[7].wait()

    @pl.when(pair == 0)
    def _():
        conv_product()


    for r in range(NM):
        for k in range(1, X):
            at_wait(source(k), a, r)
            near_forward(k, r).start()
    def half_product(r, h):
        rows = mix_rows(r)
        part = total[rows, :]
        for t in range(0, T, 2):
            both = jnp.concatenate([attn_all[t + u, h, rows, :] for u in range(2)], axis=1)
            weight = jnp.concatenate(
                [wa[pl.ds(pl.multiple_of((t + u) * C + h * V, V), V), :] for u in range(2)], axis=0
            )
            part = part + dot(both, weight)
        return part

    def near_part(r, carry):
        for k in range(X):
            at_wait(source_sib(k), a, r)
        total[mix_rows(r), :] = half_product(r, a)
        return carry

    lax.fori_loop(0, NM, near_part, 0)
    for r in range(NM):
        for k in range(X):
            at_wait(source(k), 1 - a, r)
            far_forward(k, r).start()

    def attn_part(r, carry):
        rows = mix_rows(r)
        for k in range(X):
            at_wait(source_sib(k), 1 - a, r)
        out[rows, :] = half_product(r, 1 - a).astype(BF16)
        return carry

    lse_copy.wait_recv()
    lse[1 - a] = lse_in[...]
    lax.fori_loop(0, NM, attn_part, 0)
    lse_copy.wait_send()

    sent(tok.at[pl.ds(0, X)], tok_send)
    sent(kvq.at[S], swap_send)
    sent(conv_all.at[pl.ds(0, X)], mix_send)
    sent(attn_all.at[pl.ds(0, X), 0], at_send)
    sent(attn_all.at[pl.ds(0, X), 0], at_away)
    sent(attn_all.at[pl.ds(0, X), 0], at_relay_away)
    if X > 1:
        sent(tok.at[pl.ds(0, X - 1)], tok_relay)
        sent(conv_all.at[pl.ds(0, X - 1)], mix_relay)
        sent(attn_all.at[pl.ds(0, X - 1), 0], at_relay)

    @pl.when(bridge_up)
    def _():
        sent(kvq.at[S, :, pl.ds(0, 2)], cross_send)

    spread_done(z, has_up)
    spread_done(mate_level, bridge_up)

    def drain_level(level, carry):
        spread_done(level, has_up)
        return carry

    lax.fori_loop(0, 2 * pair, drain_level, 0)

    @pl.when(sp + 1 < S)
    def _():
        rim_copy.wait_send()


def pair_device(
    dims,
    tokens,
    norm_gain,
    query_weight,
    key_weight,
    value_weight,
    outer_gate_weight,
    inner_gate_weight,
    conv_input_weight,
    conv_taps,
    lambdas,
    head_gain,
    attn_out_weight,
    conv_out_weight,
):
    S, T, Z, Y = dims["S"], dims["T"], dims["Z"], dims["Y"]
    L, Dt = tokens.shape
    H = lambdas.shape[0]
    C = query_weight.shape[1]
    V = C // H
    hd = V // 2
    O = attn_out_weight.shape[1]
    Wd = norm_gain.shape[0]
    R = V
    M = 2 * R
    NR, NM, PAD = L // R, L // M, 16
    X = T // 2
    frequency = ROPE_BASE ** (-np.arange(hd // 2) * 2.0 / hd)
    freq = jnp.asarray(np.tile(frequency, 4)[None, :], F32)
    any_spec = pl.BlockSpec(memory_space=pl.ANY)
    vmem = pl.BlockSpec(memory_space=pltpu.VMEM)
    smem = pl.BlockSpec(memory_space=pltpu.SMEM)
    dma = pltpu.SemaphoreType.DMA
    mixed, lse = pl.pallas_call(
        functools.partial(pair_kernel, dict(dims, H=H)),
        out_shape=(
            pltpu.VMEM((L, O), BF16),
            pltpu.VMEM((H, 2, L), F32),
        ),
        in_specs=[any_spec] * 10 + [smem] + [any_spec] * 3,
        out_specs=(vmem, vmem),
        scratch_shapes=[
            pltpu.VMEM((T, L, Dt), BF16),
            pltpu.VMEM((L, Wd), BF16),
            pltpu.VMEM((L, 1), F32),
            pltpu.VMEM((L, V), F32),
            pltpu.VMEM((L, V), F32),
            pltpu.VMEM((V, M), F32),
        ]
        + [pltpu.VMEM((Wd, C), BF16)] * 6
        + [pltpu.VMEM((T * C, O), BF16)] * 2
        + [
            pltpu.VMEM((S + 1, NR, 3, R, V), BF16),
            pltpu.VMEM((2, NM, 2, 1, M), F32),
            pltpu.VMEM((2, NM, 2, 1, M), F32),
            pltpu.VMEM((2, NM, 2, V, M), F32),
            pltpu.VMEM((L, C), BF16),
            pltpu.VMEM((PAD + L, C), F32),
            pltpu.VMEM((PAD, C), BF16),
            pltpu.VMEM((PAD, C), BF16),
            pltpu.VMEM((T, L, C), BF16),
            pltpu.VMEM((T, H, L, V), BF16),
            pltpu.VMEM((L, V), BF16),
            pltpu.VMEM((2, L), F32),
            pltpu.VMEM((2, L), F32),
            pltpu.VMEM((L, O), F32),
            pltpu.VMEM((1, V), F32),
            pltpu.VMEM((1, Wd), F32),
            pltpu.VMEM(conv_taps.shape, F32),
            pltpu.VMEM((1, V), F32),
            dma((12,)),
            dma,
            dma((T, NR)),
            dma,
            dma,
            dma((S, NR)),
            dma,
            dma,
            dma,
            dma((Z, max(Y - 1, 1))),
            dma((Z,)),
            dma((2,)),
            dma((2,)),
            dma((T,)),
            dma,
            dma,
            dma((T, H, NM)),
            dma,
            dma,
            dma,
            dma,
        ],
        compiler_params=pltpu.CompilerParams(
            collective_id=0,
            has_side_effects=True,
            vmem_limit_bytes=60 * 1024 * 1024,
        ),
        name="mixer",
    )(
        tokens,
        norm_gain[None, :],
        freq,
        query_weight,
        key_weight,
        value_weight,
        outer_gate_weight,
        inner_gate_weight,
        conv_input_weight,
        conv_taps,
        lambdas,
        head_gain[None, :],
        attn_out_weight,
        conv_out_weight,
    )
    return mixed, lse


def per_device(dims, *arrays):
    tokens, query_weight, lambdas = arrays[0], arrays[2], arrays[9]
    width = query_weight.shape[1] // lambdas.shape[0]
    paired = lambdas.shape[0] == 2 and dims["Z"] % 2 == 0 and dims["T"] % 2 == 0
    paired = paired and width == 128 and tokens.shape[0] % (2 * width) == 0
    return (pair_device if paired else ring_device)(dims, *arrays)


def solution(mesh):
    S, T = mesh.shape["sp"], mesh.shape["tp"]
    Y = max(d for d in range(1, S + 1) if S % d == 0 and d * d <= S)
    dims = {"S": S, "T": T, "Z": S // Y, "Y": Y}
    in_specs = (
        P("sp", "tp"),
        P(),
        P(None, "tp"),
        P(None, "tp"),
        P(None, "tp"),
        P(None, "tp"),
        P(None, "tp"),
        P(None, "tp"),
        P(None, "tp"),
        P("tp"),
        P(),
        P(None, "tp"),
        P(None, "tp"),
    )
    out_specs = (P("sp", "tp"), P("tp", None, "sp"))
    return jax.shard_map(
        functools.partial(per_device, dims),
        mesh=mesh,
        in_specs=in_specs,
        out_specs=out_specs,
        check_vma=False,
    )
```

```python
import functools

import jax
import jax.numpy as jnp
import numpy as np
from jax import lax
from jax.experimental import pallas as pl
from jax.experimental.pallas import tpu as pltpu
from jax.sharding import PartitionSpec as P

NORM_EPS = 1e-06
HEAD_EPS = 1e-05
ROPE_BASE = 500000.0
MASKED = -1e30
HEAD_SCALE = 0.8
F32 = jnp.float32
BF16 = jnp.bfloat16


def dot(a, b):
    return jnp.dot(a, b, preferred_element_type=F32)


def dot_t(a, b):
    return lax.dot_general(a, b, (((1,), (1,)), ((), ())), preferred_element_type=F32)


def ring_kernel(
    dims,
    tokens,
    gain,
    freq,
    wq_h,
    wk_h,
    wv_h,
    wo_h,
    wi_h,
    ws_h,
    taps,
    lambdas,
    head_gain,
    wa_h,
    wc_h,
    out,
    lse,
    tok,
    scaled,
    inv,
    cos_t,
    sin_t,
    wq,
    wk,
    wv,
    wo,
    wi,
    ws,
    wa,
    wc,
    kv,
    qz,
    row_max,
    row_sum,
    acc,
    gate,
    padded,
    tail,
    rim,
    conv_all,
    attn_all,
    total,
    w_sem,
    own_sem,
    tok_recv,
    tok_send,
    tok_relay,
    kv_recv,
    kv_send_z,
    kv_send_y,
    kv_extra,
    rim_sem,
    mix_recv,
    mix_send,
    mix_relay,
):
    S, T, Z, Y, H = dims["S"], dims["T"], dims["Z"], dims["Y"], dims["H"]
    L, Dt = tokens.shape
    Wd = T * Dt
    C = wq_h.shape[1]
    V = C // H
    hd = V // 2
    NR = tok_recv.shape[1]
    R = L // NR
    NM = mix_recv.shape[2]
    M = L // NM
    X = T // 2
    taps_n = taps.shape[0]
    PAD = tail.shape[0]

    sp = lax.axis_index("sp")
    tp = lax.axis_index("tp")
    z = sp // Y
    y = sp % Y
    core = tp % 2
    xi = tp // 2
    sib = xi * 2 + (1 - core)

    def peer(k):
        return ((xi + k) % X) * 2 + core

    def source(k):
        return ((xi - k + X) % X) * 2 + core

    pairs = [(wk_h, wk), (wv_h, wv), (wq_h, wq), (wi_h, wi), (ws_h, ws), (wo_h, wo), (wc_h, wc), (wa_h, wa)]
    own = pltpu.make_async_copy(tokens, tok.at[tp], own_sem)
    own.start()
    loads = [pltpu.make_async_copy(s, d, w_sem.at[i]) for i, (s, d) in enumerate(pairs)]
    for load in loads:
        load.start()

    barrier = pltpu.get_barrier_semaphore()

    def greet(target):
        pl.semaphore_signal(barrier, inc=1, device_id=target)

    for k in range(1, T):
        greet({"tp": (tp + k) % T})
    for k in range(1, Y):
        greet({"sp": z * Y + (y + k) % Y})
    has_up = z + 1 < Z
    has_down = z > 0
    far_up = jnp.logical_and(has_up, y == Y - 1) if Y > 1 else None
    far_down = jnp.logical_and(has_down, y == 0) if Y > 1 else None
    expect = (T - 1) + (Y - 1) + has_up.astype(jnp.int32) + has_down.astype(jnp.int32)

    @pl.when(has_up)
    def _():
        greet({"sp": sp + Y})

    @pl.when(has_down)
    def _():
        greet({"sp": sp - Y})

    if Y > 1:
        expect = expect + far_up.astype(jnp.int32) + far_down.astype(jnp.int32)

        @pl.when(far_up)
        def _():
            greet({"sp": sp + 1})

        @pl.when(far_down)
        def _():
            greet({"sp": sp - 1})

    pl.semaphore_wait(barrier, expect)

    def tok_rows(r):
        return pl.ds(pl.multiple_of(r * R, R), R)

    def tok_copy(src, piece, r, send, target):
        return pltpu.make_async_remote_copy(
            src_ref=src,
            dst_ref=tok.at[piece, tok_rows(r), :],
            send_sem=send,
            recv_sem=tok_recv.at[piece, r],
            device_id={"tp": target},
        )

    def tok_own(k, r):
        target = peer(k) if k else sib
        return tok_copy(tokens.at[tok_rows(r), :], tp, r, tok_send.at[k, r], target)

    def tok_forward(k, r):
        piece = source(k)
        return tok_copy(tok.at[piece, tok_rows(r), :], piece, r, tok_relay.at[k, r], sib)

    def tok_wait(piece, r):
        tok_copy(tok.at[piece, tok_rows(r), :], piece, r, tok_send.at[0, r], sib).wait_recv()

    for r in range(NR):
        for k in list(range(1, X)) + [0]:
            tok_own(k, r).start()

    lane = lax.broadcasted_iota(jnp.int32, (R, V), 1)
    first = (lane % hd) < (hd // 2)

    def table(r, carry):
        base = sp * L + r * R
        pos = (base + lax.broadcasted_iota(jnp.int32, (R, V), 0)).astype(F32)
        angle = pos * freq[...]
        sine = jnp.sin(angle)
        cos_t[tok_rows(r), :] = jnp.cos(angle)
        sin_t[tok_rows(r), :] = jnp.where(first, -sine, sine)
        return carry

    lax.fori_loop(0, NR, table, 0)

    def rotate(block, rows):
        low = (lax.broadcasted_iota(jnp.int32, block.shape, 1) % hd) < (hd // 2)
        other = jnp.where(
            low, pltpu.roll(block, V - hd // 2, 1), pltpu.roll(block, hd // 2, 1)
        )
        return block * cos_t[rows, :] + other * sin_t[rows, :]

    def kv_copy(j, r, send, target):
        block = kv.at[j, tok_rows(r), :]
        return pltpu.make_async_remote_copy(
            src_ref=block,
            dst_ref=block,
            send_sem=send,
            recv_sem=kv_recv.at[j, r],
            device_id={"sp": target},
        )

    def kv_up(dz, r):
        return kv_copy(sp - dz * Y, r, kv_send_z.at[dz, r], sp + Y)

    def kv_side(dz, r, k):
        return kv_copy(sp - dz * Y, r, kv_send_y.at[dz, r, k - 1], z * Y + (y + k) % Y)

    def kv_wait(j, r):
        kv_copy(j, r, kv_send_z.at[0, r], sp).wait_recv()

    EX = NR // 2 if Y == 2 else 0

    def extra(r):
        return kv_copy(0, r, kv_extra.at[r], sp + Y)

    def kv_send(dz, r, act):
        @pl.when(has_up)
        def _():
            act(kv_up(dz, r))

        for k in range(1, Y):
            wanted = jnp.logical_or(dz > 0, y + k < Y)
            if EX:
                other_way = jnp.logical_and(dz == z, jnp.logical_and(dz > 0, r < EX))
                wanted = jnp.logical_and(wanted, jnp.logical_not(jnp.logical_and(y == 0, other_way)))

            @pl.when(wanted)
            def _():
                act(kv_side(dz, r, k))

    def relay(dz, r):
        @pl.when(dz <= z)
        def _():
            kv_wait(sp - dz * Y, r)
            kv_send(dz, r, lambda copy: copy.start())

    def first_relay(r):
        relay(1, r)
        if EX:

            @pl.when(jnp.logical_and(jnp.logical_and(z == 0, y == 1), r < EX))
            def _():
                kv_wait(0, r)

                @pl.when(has_up)
                def _():
                    extra(r).start()

    own.wait()
    loads[0].wait()
    loads[1].wait()

    def key_chunk(r, carry):
        rows = tok_rows(r)
        for k in range(1, X):
            tok_wait(source(k), r)
            tok_forward(k, r).start()
        tok_wait(sib, r)
        for k in range(1, X):
            tok_wait(((xi + k) % X) * 2 + (1 - core), r)
        squares = jnp.zeros((R, 1), F32)
        for t in range(T):
            block = tok[t, rows, :].astype(F32)
            squares = squares + jnp.sum(block * block, axis=1, keepdims=True)
            scaled[rows, t * Dt : (t + 1) * Dt] = (block * gain[:, t * Dt : (t + 1) * Dt]).astype(BF16)
        inverse = lax.rsqrt(squares / Wd + NORM_EPS)
        inv[rows, :] = inverse
        left = scaled[rows, :]
        keys = inverse * dot(left, wk[...])
        for h in range(H):
            kv[sp, rows, h * V : (h + 1) * V] = rotate(keys[:, h * V : (h + 1) * V], rows).astype(BF16)
        kv[sp, rows, C : 2 * C] = (inverse * dot(left, wv[...])).astype(BF16)
        kv_send(0, r, lambda copy: copy.start())

        @pl.when(r > 0)
        def _():
            first_relay(r - 1)

        return carry

    lax.fori_loop(0, NR, key_chunk, 0)

    for load in loads[2:6]:
        load.wait()
    half = lax.broadcasted_iota(jnp.int32, (M, V), 1) < hd
    scale = hd ** (-0.5)

    def mix_rows(r):
        return pl.ds(pl.multiple_of(r * M, M), M)

    def query_chunk(r, carry):
        rows = mix_rows(r)
        inverse = inv[rows, :]
        left = scaled[rows, :]
        queries = inverse * dot(left, wq[...])
        for h in range(H):
            turned = rotate(queries[:, h * V : (h + 1) * V], rows).astype(BF16).astype(F32) * scale
            qz[h, 0, rows, :] = jnp.where(half, turned, 0.0).astype(BF16)
            qz[h, 1, rows, :] = jnp.where(half, 0.0, turned).astype(BF16)
        inner = (inverse * dot(left, wi[...])).astype(BF16)
        signal = (inverse * dot(left, ws[...])).astype(BF16)
        conv_in = (inner.astype(F32) * signal.astype(F32)).astype(BF16)
        padded[pl.ds(pl.multiple_of(PAD + r * M, PAD), M), :] = conv_in.astype(F32)
        gate[rows, :] = (inverse * dot(left, wo[...])).astype(BF16)

        @pl.when(r == 0)
        def _():
            first_relay(NR - 1)

        return carry

    lax.fori_loop(0, NM, query_chunk, 0)
    tail[...] = padded[L : L + PAD, :].astype(BF16)
    rim_copy = pltpu.make_async_remote_copy(
        src_ref=tail,
        dst_ref=rim,
        send_sem=rim_sem.at[0],
        recv_sem=rim_sem.at[1],
        device_id={"sp": (sp + 1) % S},
    )

    @pl.when(sp + 1 < S)
    def _():
        rim_copy.start()

    def attend(j, diagonal):
        def one(i, carry):
            rows = mix_rows(i)
            for h in range(H):
                query = qz[h, :, rows, :].reshape(2 * M, V)
                scores = dot_t(query, kv[j, :, h * V : (h + 1) * V])
                if diagonal:
                    row = lax.broadcasted_iota(jnp.int32, scores.shape, 0)
                    row = jnp.where(row >= M, row - M, row) + i * M
                    col = lax.broadcasted_iota(jnp.int32, scores.shape, 1)
                    scores = jnp.where(row >= col, scores, MASKED)
                    new_max = jnp.max(scores, axis=1, keepdims=True)
                else:
                    old_max = row_max[h, :, rows, :].reshape(2 * M, 1)
                    new_max = jnp.maximum(old_max, jnp.max(scores, axis=1, keepdims=True))
                weights = jnp.exp(scores - new_max)
                sums = jnp.sum(weights, axis=1, keepdims=True)
                mixed = dot(weights.astype(BF16), kv[j, :, C + h * V : C + (h + 1) * V])
                if not diagonal:
                    fade = jnp.exp(old_max - new_max)
                    sums = sums + fade * row_sum[h, :, rows, :].reshape(2 * M, 1)
                    mixed = mixed + fade * acc[h, :, rows, :].reshape(2 * M, V)
                row_max[h, :, rows, :] = new_max.reshape(2, M, 1)
                row_sum[h, :, rows, :] = sums.reshape(2, M, 1)
                acc[h, :, rows, :] = mixed.reshape(2, M, V)
            return carry

        lax.fori_loop(0, NM, one, 0)

    attend(sp, True)

    @pl.when(sp > 0)
    def _():
        rim_copy.wait_recv()
        padded[0:PAD, :] = rim[...].astype(F32)

    @pl.when(sp == 0)
    def _():
        padded[0:PAD, :] = jnp.zeros((PAD, C), F32)

    summed = jnp.zeros((L, C), F32)
    for j in range(taps_n):
        begin = PAD - (taps_n - 1) + j
        summed = summed + taps[j : j + 1, :] * padded[begin : begin + L, :]
    conv_all[tp, :, :] = (gate[...].astype(F32) * summed).astype(BF16)

    def mix_copy(which, buf, piece, r, send, target):
        block = buf.at[piece, mix_rows(r), :]
        return pltpu.make_async_remote_copy(
            src_ref=block,
            dst_ref=block,
            send_sem=send,
            recv_sem=mix_recv.at[which, piece, r],
            device_id={"tp": target},
        )

    def mix_own(which, buf, k, r):
        target = peer(k) if k else sib
        return mix_copy(which, buf, tp, r, mix_send.at[which, k, r], target)

    def mix_forward(which, buf, k, r):
        return mix_copy(which, buf, source(k), r, mix_relay.at[which, k, r], sib)

    def mix_wait(which, buf, piece, r):
        mix_copy(which, buf, piece, r, mix_send.at[which, 0, r], sib).wait_recv()

    for r in range(NM):
        for k in list(range(1, X)) + [0]:
            mix_own(0, conv_all, k, r).start()

    def step(dz, carry):
        def row_block(k, inner):
            def forward(r, c):
                relay(dz + 1, r)
                return c

            lax.fori_loop(k * NR // Y, (k + 1) * NR // Y, forward, 0)
            side = (y + k) % Y
            level = jnp.where(k == 0, z - dz, z - dz + 1)
            j = level * Y + side
            valid = jnp.where(k == 0, dz <= z, jnp.logical_or(level < z, side < y))

            @pl.when(valid)
            def _():
                @pl.when(k > 0)
                def _():
                    for r in range(NR):
                        if r < EX:
                            climbs = jnp.logical_and(level == 0, y == 1)

                            @pl.when(jnp.logical_not(jnp.logical_and(climbs, z == 0)))
                            def _():
                                kv_wait(j, r)

                            @pl.when(jnp.logical_and(climbs, jnp.logical_and(z > 0, has_up)))
                            def _():
                                extra(r).start()

                        else:
                            kv_wait(j, r)

                attend(j, False)

            return inner

        lax.fori_loop(0, Y, row_block, 0)
        return carry

    lax.fori_loop(1, z + 2, step, 0)

    def finish(i, carry):
        rows = mix_rows(i)
        for h in range(H):
            first_map = acc[h, 0, rows, :] / row_sum[h, 0, rows, :]
            second_map = acc[h, 1, rows, :] / row_sum[h, 1, rows, :]
            head_mix = first_map - lambdas[h] * second_map
            mean = jnp.mean(head_mix * head_mix, axis=1, keepdims=True)
            normed = head_mix * lax.rsqrt(mean + HEAD_EPS) * head_gain[...] * HEAD_SCALE
            attn_all[tp, rows, h * V : (h + 1) * V] = normed.astype(BF16)
        for k in list(range(1, X)) + [0]:
            mix_own(1, attn_all, k, i).start()
        return carry

    lax.fori_loop(0, NM, finish, 0)

    loads[6].wait()
    loads[7].wait()

    def gather(which, buf, r):
        for k in range(1, X):
            mix_wait(which, buf, source(k), r)
            mix_forward(which, buf, k, r).start()

    def gather_rest(which, buf, r):
        mix_wait(which, buf, sib, r)
        for k in range(1, X):
            mix_wait(which, buf, ((xi + k) % X) * 2 + (1 - core), r)

    def conv_part(r, carry):
        rows = mix_rows(r)
        gather(0, conv_all, r)
        gather_rest(0, conv_all, r)
        part = dot(conv_all[0, rows, :], wc[0:C, :])
        for t in range(1, T):
            part = part + dot(conv_all[t, rows, :], wc[t * C : (t + 1) * C, :])
        total[rows, :] = part
        return carry

    lax.fori_loop(0, NM, conv_part, 0)

    lanes = lax.broadcasted_iota(jnp.int32, (L, 128), 1)
    columns = jnp.zeros((L, 128), F32)
    for h in range(H):
        for c in range(2):
            value = row_max[h, c, :, :] + jnp.log(row_sum[h, c, :, :])
            columns = jnp.where(lanes == 2 * h + c, value, columns)
    turned_columns = jnp.transpose(columns)
    for h in range(H):
        lse[h] = turned_columns[2 * h : 2 * h + 2, :]

    def attn_part(r, carry):
        rows = mix_rows(r)
        gather(1, attn_all, r)
        gather_rest(1, attn_all, r)
        part = total[rows, :]
        for t in range(T):
            part = part + dot(attn_all[t, rows, :], wa[t * C : (t + 1) * C, :])
        out[rows, :] = part.astype(BF16)
        return carry

    lax.fori_loop(0, NM, attn_part, 0)

    for r in range(NR):
        for k in range(X):
            tok_own(k, r).wait_send()
        for k in range(1, X):
            tok_forward(k, r).wait_send()

    def drain(dz, carry):
        def inner(r, c):
            kv_send(dz, r, lambda copy: copy.wait_send())
            return c

        return lax.fori_loop(0, NR, inner, carry)

    lax.fori_loop(0, z + 1, drain, 0)
    if EX:

        @pl.when(jnp.logical_and(y == 1, has_up))
        def _():
            for r in range(EX):
                extra(r).wait_send()

    for which, buf in ((0, conv_all), (1, attn_all)):
        for r in range(NM):
            for k in range(X):
                mix_own(which, buf, k, r).wait_send()
            for k in range(1, X):
                mix_forward(which, buf, k, r).wait_send()

    @pl.when(sp + 1 < S)
    def _():
        rim_copy.wait_send()


def ring_device(
    dims,
    tokens,
    norm_gain,
    query_weight,
    key_weight,
    value_weight,
    outer_gate_weight,
    inner_gate_weight,
    conv_input_weight,
    conv_taps,
    lambdas,
    head_gain,
    attn_out_weight,
    conv_out_weight,
):
    S, T, Z, Y = dims["S"], dims["T"], dims["Z"], dims["Y"]
    L, Dt = tokens.shape
    H = lambdas.shape[0]
    C = query_weight.shape[1]
    V = C // H
    hd = V // 2
    O = attn_out_weight.shape[1]
    Wd = norm_gain.shape[0]
    NR, NM, PAD = 4, 2, 16
    X = T // 2
    frequency = ROPE_BASE ** (-np.arange(hd // 2) * 2.0 / hd)
    freq = jnp.asarray(np.tile(frequency, 4)[None, :], F32)
    any_spec = pl.BlockSpec(memory_space=pl.ANY)
    vmem = pl.BlockSpec(memory_space=pltpu.VMEM)
    smem = pl.BlockSpec(memory_space=pltpu.SMEM)
    dma = pltpu.SemaphoreType.DMA
    mixed, lse = pl.pallas_call(
        functools.partial(ring_kernel, dict(dims, H=H)),
        out_shape=(
            jax.ShapeDtypeStruct((L, O), BF16),
            jax.ShapeDtypeStruct((H, 2, L), F32),
        ),
        in_specs=[any_spec, vmem, vmem] + [any_spec] * 6 + [vmem, smem, vmem] + [any_spec] * 2,
        out_specs=(vmem, vmem),
        scratch_shapes=[
            pltpu.VMEM((T, L, Dt), BF16),
            pltpu.VMEM((L, Wd), BF16),
            pltpu.VMEM((L, 1), F32),
            pltpu.VMEM((L, V), F32),
            pltpu.VMEM((L, V), F32),
        ]
        + [pltpu.VMEM((Wd, C), BF16)] * 6
        + [pltpu.VMEM((T * C, O), BF16)] * 2
        + [
            pltpu.VMEM((S, L, 2 * C), BF16),
            pltpu.VMEM((H, 2, L, V), BF16),
            pltpu.VMEM((H, 2, L, 1), F32),
            pltpu.VMEM((H, 2, L, 1), F32),
            pltpu.VMEM((H, 2, L, V), F32),
            pltpu.VMEM((L, C), BF16),
            pltpu.VMEM((PAD + L, C), F32),
            pltpu.VMEM((PAD, C), BF16),
            pltpu.VMEM((PAD, C), BF16),
            pltpu.VMEM((T, L, C), BF16),
            pltpu.VMEM((T, L, C), BF16),
            pltpu.VMEM((L, O), F32),
            dma((8,)),
            dma,
            dma((T, NR)),
            dma((X, NR)),
            dma((X, NR)),
            dma((S, NR)),
            dma((Z, NR)),
            dma((Z, NR, max(Y - 1, 1))),
            dma((NR,)),
            dma((2,)),
            dma((2, T, NM)),
            dma((2, X, NM)),
            dma((2, X, NM)),
        ],
        compiler_params=pltpu.CompilerParams(
            collective_id=0, has_side_effects=True, vmem_limit_bytes=60 * 1024 * 1024
        ),
        name="mixer",
    )(
        tokens,
        norm_gain[None, :],
        freq,
        query_weight,
        key_weight,
        value_weight,
        outer_gate_weight,
        inner_gate_weight,
        conv_input_weight,
        conv_taps,
        lambdas,
        head_gain[None, :],
        attn_out_weight,
        conv_out_weight,
    )
    return mixed, lse


def pair_kernel(
    dims,
    tokens,
    gain_h,
    freq_h,
    wq_h,
    wk_h,
    wv_h,
    wo_h,
    wi_h,
    ws_h,
    taps_h,
    lambdas,
    head_gain_h,
    wa_h,
    wc_h,
    out,
    lse,
    tok,
    scaled,
    inv,
    cos_t,
    sin_t,
    gain_t,
    wq,
    wk,
    wv,
    wo,
    wi,
    ws,
    wa,
    wc,
    kvq,
    turned,
    row_max,
    row_sum,
    acc,
    gate,
    padded,
    tail,
    rim,
    conv_all,
    attn_all,
    away,
    lse_away,
    lse_in,
    total,
    freq,
    gain,
    taps,
    head_gain,
    w_sem,
    own_sem,
    tok_recv,
    tok_send,
    tok_relay,
    kv_recv,
    side_recv,
    swap_send,
    ask_recv,
    cross_send,
    side_send,
    up_send,
    rim_sem,
    lse_sem,
    mix_recv,
    mix_send,
    mix_relay,
    at_recv,
    at_send,
    at_away,
    at_relay,
    at_relay_away,
):
    S, T, Z, Y, H = dims["S"], dims["T"], dims["Z"], dims["Y"], dims["H"]
    L, Dt = tokens.shape
    Wd = T * Dt
    C = wq_h.shape[1]
    V = C // H
    hd = V // 2
    NR = tok_recv.shape[1]
    R = L // NR
    NM = at_recv.shape[2]
    M = L // NM
    G = M // R
    LATE = 2
    LAG = 3
    X = T // 2
    taps_n = taps.shape[0]
    PAD = tail.shape[0]

    sp = lax.axis_index("sp")
    tp = lax.axis_index("tp")
    z = sp // Y
    y = sp % Y
    pair = z // 2
    a = z % 2
    mate = sp + (1 - 2 * a) * Y
    core = tp % 2
    xi = tp // 2
    sib = xi * 2 + (1 - core)
    has_up = z + 2 - a < Z
    has_down = pair > 0

    def peer(k):
        return ((xi + k) % X) * 2 + core

    def source(k):
        return ((xi - k + X) % X) * 2 + core

    def source_sib(k):
        return ((xi - k + X) % X) * 2 + (1 - core)

    own = pltpu.make_async_copy(tokens, tok.at[tp], own_sem)
    own.start()
    barrier = pltpu.get_barrier_semaphore()

    def greet(target):
        pl.semaphore_signal(barrier, inc=1, device_id=target)

    for k in range(1, T):
        greet({"tp": (tp + k) % T})
    for k in range(X):
        greet({"sp": mate, "tp": peer(k)})
    for k in range(1, Y):
        greet({"sp": z * Y + (y + k) % Y})
    expect = (T - 1) + X + (Y - 1)
    bridge_up = jnp.logical_and(a == 1, has_up)
    prompt = jnp.logical_not(bridge_up)
    bridge_down = jnp.logical_and(a == 0, has_down)
    for near, step in (
        (has_up, 2 * Y),
        (has_down, -2 * Y),
        (bridge_up, Y),
        (bridge_down, -Y),
        (sp + 1 < S, 1),
        (sp > 0, -1),
    ):
        expect = expect + near.astype(jnp.int32)

        @pl.when(near)
        def _():
            greet({"sp": sp + step})

    pairs = [(wk_h, wk), (wv_h, wv), (wq_h, wq), (wi_h, wi), (ws_h, ws), (wo_h, wo), (wc_h, wc), (wa_h, wa)]
    pairs = pairs + [(freq_h, freq), (gain_h, gain), (taps_h, taps), (head_gain_h, head_gain)]
    loads = [pltpu.make_async_copy(s, d, w_sem.at[i]) for i, (s, d) in enumerate(pairs)]

    pl.semaphore_wait(barrier, expect)

    def tok_rows(r):
        return pl.ds(pl.multiple_of(r * R, R), R)

    def tok_copy(src, piece, r, send, target):
        return pltpu.make_async_remote_copy(
            src_ref=src,
            dst_ref=tok.at[piece, tok_rows(r), :],
            send_sem=send,
            recv_sem=tok_recv.at[piece, r],
            device_id={"tp": target},
        )

    def tok_own(k, r):
        target = peer(k) if k else sib
        return tok_copy(tok.at[tp, tok_rows(r), :], tp, r, tok_send, target)

    def tok_forward(k, r):
        piece = source(k)
        return tok_copy(tok.at[piece, tok_rows(r), :], piece, r, tok_relay, sib)

    def tok_wait(piece, r):
        tok_copy(tok.at[piece, tok_rows(r), :], piece, r, tok_send, sib).wait_recv()

    own.wait()
    for r in reversed(range(NR)):
        for k in list(range(1, X)) + [0]:
            tok_own(k, r).start()
    for load in loads[8:] + loads[:8]:
        load.start()

    lane = lax.broadcasted_iota(jnp.int32, (R, V), 1)
    first = (lane % hd) < (hd // 2)

    loads[8].wait()
    loads[11].wait()

    def table(r, carry):
        base = sp * L + r * R
        pos = (base + lax.broadcasted_iota(jnp.int32, (R, V), 0)).astype(F32)
        angle = pos * freq[...]
        sine = jnp.sin(angle)
        cos_t[tok_rows(r), :] = jnp.cos(angle)
        sin_t[tok_rows(r), :] = jnp.where(first, -sine, sine)
        return carry

    lax.fori_loop(0, NR, table, 0)
    gain_t[...] = jnp.transpose(jnp.broadcast_to(head_gain[...], (M, V)))

    row_max[...] = jnp.full(row_max.shape, MASKED, F32)
    row_sum[...] = jnp.zeros(row_sum.shape, F32)
    acc[...] = jnp.zeros(acc.shape, F32)

    def rotate(block, rows):
        other = jnp.where(first, pltpu.roll(block, V - hd // 2, 1), pltpu.roll(block, hd // 2, 1))
        return block * cos_t[rows, :] + other * sin_t[rows, :]

    def level_block(level):
        return level * Y + y

    def kv_copy(level, r, send, target, src=None, recv=None):
        block = kvq.at[level_block(level), r, pl.ds(0, 2)]
        return pltpu.make_async_remote_copy(
            src_ref=block if src is None else src,
            dst_ref=block,
            send_sem=send,
            recv_sem=kv_recv.at[level, r] if recv is None else recv,
            device_id={"sp": target},
        )

    def sent(ref, sem):
        pltpu.make_async_remote_copy(
            src_ref=ref, dst_ref=ref, send_sem=sem, recv_sem=sem, device_id={"sp": mate}
        ).wait_send()

    mate_level = z + 1 - 2 * a
    top = 2 * pair + 1

    def swap(r):
        return kv_copy(z, r, swap_send, mate, kvq.at[S, r, pl.ds(0, 2)])

    def ask(j, r):
        return pltpu.make_async_remote_copy(
            src_ref=kvq.at[S, r, 2],
            dst_ref=kvq.at[j, r, 2],
            send_sem=swap_send,
            recv_sem=ask_recv,
            device_id={"sp": mate},
        )

    def cross(r):
        return kv_copy(z, r, cross_send, sp + Y, kvq.at[S, r, pl.ds(0, 2)])

    def up(level, r):
        return kv_copy(level, r, up_send.at[level], sp + 2 * Y)

    def side(level, r, k):
        late = 1 - jnp.minimum(r // LATE, 1)
        return kv_copy(
            level,
            r,
            side_send.at[level, k - 1],
            z * Y + (y + k) % Y,
            recv=side_recv.at[level, k - 1, late],
        )

    def kv_wait(level, r):
        kv_copy(level, r, cross_send, mate).wait_recv()

    def beside_wait(level, k, late):
        rows = pl.ds(0, LATE) if late else pl.ds(LATE, NR - LATE)
        block = kvq.at[level * Y + (y + k) % Y, rows, pl.ds(0, 2)]
        pltpu.make_async_remote_copy(
            src_ref=block,
            dst_ref=block,
            send_sem=cross_send,
            recv_sem=side_recv.at[level, Y - k - 1, int(late)],
            device_id={"sp": mate},
        ).wait_recv()

    def spread(level, r, rises):
        @pl.when(rises)
        def _():
            up(level, r).start()

        for k in range(1, Y):

            @pl.when(jnp.logical_or(level < top, y < (y + k) % Y))
            def _():
                side(level, r, k).start()

    def spread_done(level, rises):
        whole = kvq.at[level_block(level), :, pl.ds(0, 2)]

        @pl.when(rises)
        def _():
            sent(whole, up_send.at[level])

        for k in range(1, Y):

            @pl.when(jnp.logical_or(level < top, y < (y + k) % Y))
            def _():
                sent(whole, side_send.at[level, k - 1])

    def send_own(r):
        swap(r).start()

        @pl.when(bridge_up)
        def _():
            cross(r).start()

        spread(z, r, has_up)


    def relay_mate(r):
        kv_wait(mate_level, r)
        spread(mate_level, r, bridge_up)

    def relay_below(level, r):
        kv_wait(level, r)
        spread(level, r, has_up)

    for load in loads[:5] + loads[9:11]:
        load.wait()
    rim_copy = pltpu.make_async_remote_copy(
        src_ref=tail,
        dst_ref=rim,
        send_sem=rim_sem.at[0],
        recv_sem=rim_sem.at[1],
        device_id={"sp": (sp + 1) % S},
    )
    scale = hd ** (-0.5)

    def tok_next(r):
        for k in range(1, X):
            tok_wait(source(k), r)
            tok_forward(k, r).start()

    tok_next(NR - 1)

    def chunk(i, carry):
        r = NR - 1 - i
        rows = tok_rows(r)
        tok_wait(sib, r)
        for k in range(1, X):
            tok_wait(source_sib(k), r)

        @pl.when(i < NR - 1)
        def _():
            tok_next(r - 1)

        squares = jnp.zeros((R, 1), F32)
        for t in range(T):
            block = tok[t, rows, :].astype(F32)
            squares = squares + jnp.sum(block * block, axis=1, keepdims=True)
            scaled[rows, t * Dt : (t + 1) * Dt] = (block * gain[:, t * Dt : (t + 1) * Dt]).astype(BF16)
        inverse = lax.rsqrt(squares / Wd + NORM_EPS)
        inv[rows, :] = inverse
        left = scaled[rows, :]
        keys = inverse * dot(left, wk[...])
        values = inverse * dot(left, wv[...])
        for h in range(H):
            mine = a if h else 1 - a
            slot = sp * mine + S * (1 - mine)
            cols = slice(h * V, (h + 1) * V)
            kvq[slot, r, 0] = rotate(keys[:, cols], rows).astype(BF16)
            kvq[slot, r, 1] = values[:, cols].astype(BF16)
        send_own(r)
        queries = inverse * dot(left, wq[...])
        for h in range(H):
            mine = a if h else 1 - a
            slot = sp * mine + S * (1 - mine)
            cols = slice(h * V, (h + 1) * V)
            kvq[slot, r, 2] = (rotate(queries[:, cols], rows).astype(BF16).astype(F32) * scale).astype(BF16)

        @pl.when(i == 0)
        def _():
            edge = pl.ds(L - PAD, PAD)
            inner = (inv[edge, :] * dot(scaled[edge, :], wi[...])).astype(BF16)
            signal = (inv[edge, :] * dot(scaled[edge, :], ws[...])).astype(BF16)
            tail[...] = (inner.astype(F32) * signal.astype(F32)).astype(BF16)

            @pl.when(sp + 1 < S)
            def _():
                rim_copy.start()

        @pl.when(jnp.logical_and(prompt, i >= LAG))
        def _():
            relay_mate(r + LAG)

        return carry

    lax.fori_loop(0, NR, chunk, 0)
    for r in reversed(range(NR)):
        ask(sp, r).start()

    def level_at(n):
        odd = n % 2
        return 2 * (pair - 1 - n // 2) + a * (1 - odd) + (1 - a) * odd

    def relay_level(n, rows, when=None):
        wanted = n < 2 * pair
        if when is not None:
            wanted = jnp.logical_and(wanted, when)

        @pl.when(wanted)
        def _():
            for r in rows:
                relay_below(level_at(n), r)

    order = list(reversed(range(NR)))

    loads[5].wait()

    def mix_rows(r):
        return pl.ds(pl.multiple_of(r * M, M), M)

    def gate_chunk(r, carry):
        rows = mix_rows(r)
        inverse = inv[rows, :]
        left = scaled[rows, :]
        inner = (inverse * dot(left, wi[...])).astype(BF16)
        signal = (inverse * dot(left, ws[...])).astype(BF16)
        conv_in = (inner.astype(F32) * signal.astype(F32)).astype(BF16)
        padded[pl.ds(pl.multiple_of(PAD + r * M, PAD), M), :] = conv_in.astype(F32)
        gate[rows, :] = (inverse * dot(left, wo[...])).astype(BF16)
        return carry

    lax.fori_loop(0, NM, gate_chunk, 0)

    @pl.when(sp > 0)
    def _():
        rim_copy.wait_recv()
        padded[0:PAD, :] = rim[...].astype(F32)

    @pl.when(sp == 0)
    def _():
        padded[0:PAD, :] = jnp.zeros((PAD, C), F32)

    summed = jnp.zeros((L, C), F32)
    for j in range(taps_n):
        begin = PAD - (taps_n - 1) + j
        summed = summed + taps[j : j + 1, :] * padded[begin : begin + L, :]
    conv_all[tp, :, :] = (gate[...].astype(F32) * summed).astype(BF16)

    def mix_copy(piece, send, target):
        block = conv_all.at[piece]
        return pltpu.make_async_remote_copy(
            src_ref=block,
            dst_ref=block,
            send_sem=send,
            recv_sem=mix_recv.at[piece],
            device_id={"tp": target},
        )

    def mix_own(k):
        return mix_copy(tp, mix_send, peer(k) if k else sib)

    def mix_forward(k):
        return mix_copy(source(k), mix_relay, sib)

    def mix_wait(piece):
        mix_copy(piece, mix_send, sib).wait_recv()

    for k in list(range(1, X)) + [0]:
        mix_own(k).start()

    blank = jnp.zeros((hd, M), BF16)

    def flip(blocks):
        return jnp.transpose(jnp.concatenate(blocks, axis=0))

    def turn_queries(b):
        j = level_block(2 * pair + b)
        for part in range(NM):
            turned[b, part] = flip([kvq[j, G * part + g, 2] for g in range(G)])

    def attend(items):
        work = [(item, c) for item in items for c in range(2)]
        flipped = {}

        def score(item, c):
            chunks, b, part, shift = item
            keys = jnp.concatenate([kvq[j, r, 0] for j, r in chunks], axis=0)
            if c:
                right = jnp.concatenate([blank, turned[b, part, hd:, :]], axis=0)
            else:
                right = jnp.concatenate([turned[b, part, :hd, :], blank], axis=0)
            scores = dot(keys, right)
            if shift is not None:
                key_row = lax.broadcasted_iota(jnp.int32, scores.shape, 0)
                query_lane = lax.broadcasted_iota(jnp.int32, scores.shape, 1)
                scores = jnp.where(key_row <= query_lane + shift, scores, MASKED)
            return scores

        def mix(item, c, fade, weights):
            chunks, b, part, _ = item
            if id(chunks) not in flipped:
                flipped[id(chunks)] = flip([kvq[j, r, 1] for j, r in chunks])
            values = flipped[id(chunks)]
            acc[b, part, c] = fade * acc[b, part, c] + dot(values, weights)

        ready = [score(*work[0])]
        waiting = []
        for i, (item, c) in enumerate(work):
            for n in range(i + len(ready), min(i + 3, len(work))):
                ready.append(score(*work[n]))
            scores = ready.pop(0)
            _, b, part, _ = item
            old_max = row_max[b, part, c]
            new_max = jnp.maximum(old_max, jnp.max(scores, axis=0, keepdims=True))
            weights = jnp.exp(scores - new_max)
            fade = jnp.exp(old_max - new_max)
            row_max[b, part, c] = new_max
            row_sum[b, part, c] = fade * row_sum[b, part, c] + jnp.sum(weights, axis=0, keepdims=True)
            if waiting:
                mix(*waiting.pop())
            waiting.append((item, c, fade, weights.astype(BF16)))
        mix(*waiting.pop())

    def chunks_of(j, begin=0, end=NR):
        return [(j, r) for r in range(begin, end)]

    low_own = level_block(2 * pair)

    def triangle(j, b):
        return [(chunks_of(j, 0, G * (part + 1)), b, part, M * part) for part in reversed(range(NM))]

    turn_queries(a)
    attend(triangle(sp, a))
    def relay_rest(i, carry):
        relay_mate(NR - 1 - i)
        return carry

    lax.fori_loop(jnp.where(prompt, NR - LAG, 0), NR, relay_rest, 0)
    relay_level(0, order[:3])
    relay_level(0, order[3:], a == 0)
    relay_level(1, order[:2], a == 0)
    asked = kvq.at[mate, :, 2]
    pltpu.make_async_remote_copy(
        src_ref=asked, dst_ref=asked, send_sem=swap_send, recv_sem=ask_recv, device_id={"sp": mate}
    ).wait_recv()
    turn_queries(1 - a)
    whole_own = chunks_of(low_own)
    attend([(whole_own, 1, part, None) for part in range(NM)] + triangle(mate, 1 - a))
    relay_level(0, order[3:5], a == 1)
    relay_level(1, order[2:4], a == 0)

    for k in range(1, Y):
        other = (y + k) % Y
        ahead = other < y
        low = 2 * pair * Y + other
    for k in range(1, Y):
        other = (y + k) % Y
        ahead = other < y
        low = chunks_of(2 * pair * Y + other)
        high = chunks_of(top * Y + other)
        for late in (False, True):
            beside_wait(2 * pair, k, late)
        late_items = [(low, 1, part, None) for part in range(NM)]

        @pl.when(ahead)
        def _():
            for late in (False, True):
                beside_wait(top, k, late)
            attend(
                late_items
                + [(low, 0, part, None) for part in range(NM)]
                + [(high, 1, part, None) for part in range(NM)]
            )

        @pl.when(jnp.logical_not(ahead))
        def _():
            attend(late_items)

    relay_level(0, order[5:], a == 1)
    relay_level(1, order[4:], a == 0)
    for k in range(1, X):
        mix_wait(source(k))
        mix_forward(k).start()

    def conv_product():
        loads[6].wait()
        mix_wait(sib)
        for k in range(1, X):
            mix_wait(source_sib(k))

        def conv_part(r, carry):
            rows = mix_rows(r)
            part = dot(conv_all[0, rows, :], wc[0:C, :])
            for t in range(1, T):
                part = part + dot(conv_all[t, rows, :], wc[t * C : (t + 1) * C, :])
            total[rows, :] = part
            return carry

        lax.fori_loop(0, NM, conv_part, 0)

    def at_copy(src, piece, h, r, send, target):
        return pltpu.make_async_remote_copy(
            src_ref=src,
            dst_ref=attn_all.at[piece, h, mix_rows(r), :],
            send_sem=send,
            recv_sem=at_recv.at[piece, h, r],
            device_id=target,
        )

    def at_own(k, r):
        target = {"tp": peer(k) if k else sib}
        return at_copy(attn_all.at[tp, a, mix_rows(r), :], tp, a, r, at_send, target)

    def at_off(k, r):
        target = {"sp": mate, "tp": peer(k)}
        return at_copy(away.at[mix_rows(r), :], tp, a, r, at_away, target)

    def at_forward(k, h, r, send):
        piece = source(k)
        return at_copy(attn_all.at[piece, h, mix_rows(r), :], piece, h, r, send, {"tp": sib})

    def at_wait(piece, h, r):
        at_copy(attn_all.at[piece, h, mix_rows(r), :], piece, h, r, at_send, {"tp": sib}).wait_recv()

    def near_forward(k, r):
        return at_forward(k, a, r, at_relay)

    def far_forward(k, r):
        return at_forward(k, 1 - a, r, at_relay_away)

    def finished(b, part):
        first_map = acc[b, part, 0] / row_sum[b, part, 0]
        second_map = acc[b, part, 1] / row_sum[b, part, 1]
        head_mix = first_map - lambdas[a] * second_map
        mean = jnp.mean(head_mix * head_mix, axis=0, keepdims=True)
        normed = head_mix * lax.rsqrt(mean + HEAD_EPS) * gain_t[...] * HEAD_SCALE
        return jnp.transpose(normed).astype(BF16)

    def log_total(b, part, c):
        return row_max[b, part, c] + jnp.log(row_sum[b, part, c])

    def send_away():
        for part in range(NM):
            away[part * M : (part + 1) * M, :] = finished(1 - a, part)
            for k in list(range(1, X)) + [0]:
                at_off(k, part).start()

    def below(n, carry):
        level = level_at(n)
        later = jnp.logical_or(n > 0, a == 1)

        def item(k, c):
            j = level * Y + (y + k) % Y
            final = jnp.logical_and(k == Y - 1, n == 2 * pair - 1)

            @pl.when(k == 1)
            def _():
                relay_level(n + 1, order[:2], later)

                @pl.when(n == 2 * pair - 2)
                def _():
                    conv_product()

                relay_level(n + 1, order[2:4], later)

            @pl.when(jnp.logical_and(k > 0, jnp.logical_not(final)))
            def _():
                for late in (False, True):
                    beside_wait(level, k, late)

            @pl.when(jnp.logical_not(final))
            def _():
                chunks = chunks_of(j)
                attend([(chunks, b, part, None) for b in range(2) for part in range(NM)])

            @pl.when(final)
            def _():
                soon, last = chunks_of(j, LATE), chunks_of(j, 0, LATE)
                beside_wait(level, k, False)
                attend([(soon, b, part, None) for b in range(2) for part in range(NM)])
                beside_wait(level, k, True)
                attend([(last, 1 - a, part, None) for part in range(NM)])
                send_away()
                attend([(last, a, part, None) for part in range(NM)])

            return c

        lax.fori_loop(0, Y, item, 0)
        relay_level(n + 1, order[4:], later)
        return carry

    lax.fori_loop(0, 2 * pair, below, 0)

    @pl.when(pair == 0)
    def _():
        send_away()

    for part in range(NM):
        attn_all[tp, a, part * M : (part + 1) * M, :] = finished(a, part)
        for k in list(range(1, X)) + [0]:
            at_own(k, part).start()
    for part in range(NM):
        for c in range(2):
            lse_away[c : c + 1, part * M : (part + 1) * M] = log_total(1 - a, part, c)
            lse[a, c : c + 1, part * M : (part + 1) * M] = log_total(a, part, c)
    lse_copy = pltpu.make_async_remote_copy(
        src_ref=lse_away,
        dst_ref=lse_in,
        send_sem=lse_sem.at[0],
        recv_sem=lse_sem.at[1],
        device_id={"sp": mate},
    )
    lse_copy.start()

    loads[7].wait()

    @pl.when(pair == 0)
    def _():
        conv_product()


    for r in range(NM):
        for k in range(1, X):
            at_wait(source(k), a, r)
            near_forward(k, r).start()
    def half_product(r, h):
        rows = mix_rows(r)
        part = total[rows, :]
        for t in range(0, T, 2):
            both = jnp.concatenate([attn_all[t + u, h, rows, :] for u in range(2)], axis=1)
            weight = jnp.concatenate(
                [wa[pl.ds(pl.multiple_of((t + u) * C + h * V, V), V), :] for u in range(2)], axis=0
            )
            part = part + dot(both, weight)
        return part

    def near_part(r, carry):
        for k in range(X):
            at_wait(source_sib(k), a, r)
        total[mix_rows(r), :] = half_product(r, a)
        return carry

    lax.fori_loop(0, NM, near_part, 0)
    for r in range(NM):
        for k in range(X):
            at_wait(source(k), 1 - a, r)
            far_forward(k, r).start()

    def attn_part(r, carry):
        rows = mix_rows(r)
        for k in range(X):
            at_wait(source_sib(k), 1 - a, r)
        out[rows, :] = half_product(r, 1 - a).astype(BF16)
        return carry

    lse_copy.wait_recv()
    lse[1 - a] = lse_in[...]
    lax.fori_loop(0, NM, attn_part, 0)
    lse_copy.wait_send()

    sent(tok.at[pl.ds(0, X)], tok_send)
    sent(kvq.at[S], swap_send)
    sent(conv_all.at[pl.ds(0, X)], mix_send)
    sent(attn_all.at[pl.ds(0, X), 0], at_send)
    sent(attn_all.at[pl.ds(0, X), 0], at_away)
    sent(attn_all.at[pl.ds(0, X), 0], at_relay_away)
    if X > 1:
        sent(tok.at[pl.ds(0, X - 1)], tok_relay)
        sent(conv_all.at[pl.ds(0, X - 1)], mix_relay)
        sent(attn_all.at[pl.ds(0, X - 1), 0], at_relay)

    @pl.when(bridge_up)
    def _():
        sent(kvq.at[S, :, pl.ds(0, 2)], cross_send)

    spread_done(z, has_up)
    spread_done(mate_level, bridge_up)

    def drain_level(level, carry):
        spread_done(level, has_up)
        return carry

    lax.fori_loop(0, 2 * pair, drain_level, 0)

    @pl.when(sp + 1 < S)
    def _():
        rim_copy.wait_send()


def pair_device(
    dims,
    tokens,
    norm_gain,
    query_weight,
    key_weight,
    value_weight,
    outer_gate_weight,
    inner_gate_weight,
    conv_input_weight,
    conv_taps,
    lambdas,
    head_gain,
    attn_out_weight,
    conv_out_weight,
):
    S, T, Z, Y = dims["S"], dims["T"], dims["Z"], dims["Y"]
    L, Dt = tokens.shape
    H = lambdas.shape[0]
    C = query_weight.shape[1]
    V = C // H
    hd = V // 2
    O = attn_out_weight.shape[1]
    Wd = norm_gain.shape[0]
    R = V // 2
    M = 2 * V
    NR, NM, PAD = L // R, L // M, 16
    X = T // 2
    frequency = ROPE_BASE ** (-np.arange(hd // 2) * 2.0 / hd)
    freq = jnp.asarray(np.tile(frequency, 4)[None, :], F32)
    any_spec = pl.BlockSpec(memory_space=pl.ANY)
    vmem = pl.BlockSpec(memory_space=pltpu.VMEM)
    smem = pl.BlockSpec(memory_space=pltpu.SMEM)
    dma = pltpu.SemaphoreType.DMA
    mixed, lse = pl.pallas_call(
        functools.partial(pair_kernel, dict(dims, H=H)),
        out_shape=(
            pltpu.VMEM((L, O), BF16),
            pltpu.VMEM((H, 2, L), F32),
        ),
        in_specs=[any_spec] * 10 + [smem] + [any_spec] * 3,
        out_specs=(vmem, vmem),
        scratch_shapes=[
            pltpu.VMEM((T, L, Dt), BF16),
            pltpu.VMEM((L, Wd), BF16),
            pltpu.VMEM((L, 1), F32),
            pltpu.VMEM((L, V), F32),
            pltpu.VMEM((L, V), F32),
            pltpu.VMEM((V, M), F32),
        ]
        + [pltpu.VMEM((Wd, C), BF16)] * 6
        + [pltpu.VMEM((T * C, O), BF16)] * 2
        + [
            pltpu.VMEM((S + 1, NR, 3, R, V), BF16),
            pltpu.VMEM((2, NM, V, M), BF16),
            pltpu.VMEM((2, NM, 2, 1, M), F32),
            pltpu.VMEM((2, NM, 2, 1, M), F32),
            pltpu.VMEM((2, NM, 2, V, M), F32),
            pltpu.VMEM((L, C), BF16),
            pltpu.VMEM((PAD + L, C), F32),
            pltpu.VMEM((PAD, C), BF16),
            pltpu.VMEM((PAD, C), BF16),
            pltpu.VMEM((T, L, C), BF16),
            pltpu.VMEM((T, H, L, V), BF16),
            pltpu.VMEM((L, V), BF16),
            pltpu.VMEM((2, L), F32),
            pltpu.VMEM((2, L), F32),
            pltpu.VMEM((L, O), F32),
            pltpu.VMEM((1, V), F32),
            pltpu.VMEM((1, Wd), F32),
            pltpu.VMEM(conv_taps.shape, F32),
            pltpu.VMEM((1, V), F32),
            dma((12,)),
            dma,
            dma((T, NR)),
            dma,
            dma,
            dma((Z, NR)),
            dma((Z, max(Y - 1, 1), 2)),
            dma,
            dma,
            dma,
            dma((Z, max(Y - 1, 1))),
            dma((Z,)),
            dma((2,)),
            dma((2,)),
            dma((T,)),
            dma,
            dma,
            dma((T, H, NM)),
            dma,
            dma,
            dma,
            dma,
        ],
        compiler_params=pltpu.CompilerParams(
            collective_id=0,
            has_side_effects=True,
            vmem_limit_bytes=60 * 1024 * 1024,
        ),
        name="mixer",
    )(
        tokens,
        norm_gain[None, :],
        freq,
        query_weight,
        key_weight,
        value_weight,
        outer_gate_weight,
        inner_gate_weight,
        conv_input_weight,
        conv_taps,
        lambdas,
        head_gain[None, :],
        attn_out_weight,
        conv_out_weight,
    )
    return mixed, lse


def per_device(dims, *arrays):
    tokens, query_weight, lambdas = arrays[0], arrays[2], arrays[9]
    width = query_weight.shape[1] // lambdas.shape[0]
    paired = lambdas.shape[0] == 2 and dims["Z"] % 2 == 0 and dims["T"] % 2 == 0
    paired = paired and width == 128 and tokens.shape[0] % (2 * width) == 0
    return (pair_device if paired else ring_device)(dims, *arrays)


def solution(mesh):
    S, T = mesh.shape["sp"], mesh.shape["tp"]
    Y = max(d for d in range(1, S + 1) if S % d == 0 and d * d <= S)
    dims = {"S": S, "T": T, "Z": S // Y, "Y": Y}
    in_specs = (
        P("sp", "tp"),
        P(),
        P(None, "tp"),
        P(None, "tp"),
        P(None, "tp"),
        P(None, "tp"),
        P(None, "tp"),
        P(None, "tp"),
        P(None, "tp"),
        P("tp"),
        P(),
        P(None, "tp"),
        P(None, "tp"),
    )
    out_specs = (P("sp", "tp"), P("tp", None, "sp"))
    return jax.shard_map(
        functools.partial(per_device, dims),
        mesh=mesh,
        in_specs=in_specs,
        out_specs=out_specs,
        check_vma=False,
    )
```

```python
import functools

import jax
import jax.numpy as jnp
import numpy as np
from jax import lax
from jax.experimental import pallas as pl
from jax.experimental.pallas import tpu as pltpu
from jax.sharding import PartitionSpec as P

NORM_EPS = 1e-06
HEAD_EPS = 1e-05
ROPE_BASE = 500000.0
MASKED = -1e30
HEAD_SCALE = 0.8
F32 = jnp.float32
BF16 = jnp.bfloat16


def dot(a, b):
    return jnp.dot(a, b, preferred_element_type=F32)


def dot_t(a, b):
    return lax.dot_general(a, b, (((1,), (1,)), ((), ())), preferred_element_type=F32)


def ring_kernel(
    dims,
    tokens,
    gain,
    freq,
    wq_h,
    wk_h,
    wv_h,
    wo_h,
    wi_h,
    ws_h,
    taps,
    lambdas,
    head_gain,
    wa_h,
    wc_h,
    out,
    lse,
    tok,
    scaled,
    inv,
    cos_t,
    sin_t,
    wq,
    wk,
    wv,
    wo,
    wi,
    ws,
    wa,
    wc,
    kv,
    qz,
    row_max,
    row_sum,
    acc,
    gate,
    padded,
    tail,
    rim,
    conv_all,
    attn_all,
    total,
    w_sem,
    own_sem,
    tok_recv,
    tok_send,
    tok_relay,
    kv_recv,
    kv_send_z,
    kv_send_y,
    kv_extra,
    rim_sem,
    mix_recv,
    mix_send,
    mix_relay,
):
    S, T, Z, Y, H = dims["S"], dims["T"], dims["Z"], dims["Y"], dims["H"]
    L, Dt = tokens.shape
    Wd = T * Dt
    C = wq_h.shape[1]
    V = C // H
    hd = V // 2
    NR = tok_recv.shape[1]
    R = L // NR
    NM = mix_recv.shape[2]
    M = L // NM
    X = T // 2
    taps_n = taps.shape[0]
    PAD = tail.shape[0]

    sp = lax.axis_index("sp")
    tp = lax.axis_index("tp")
    z = sp // Y
    y = sp % Y
    core = tp % 2
    xi = tp // 2
    sib = xi * 2 + (1 - core)

    def peer(k):
        return ((xi + k) % X) * 2 + core

    def source(k):
        return ((xi - k + X) % X) * 2 + core

    pairs = [(wk_h, wk), (wv_h, wv), (wq_h, wq), (wi_h, wi), (ws_h, ws), (wo_h, wo), (wc_h, wc), (wa_h, wa)]
    own = pltpu.make_async_copy(tokens, tok.at[tp], own_sem)
    own.start()
    loads = [pltpu.make_async_copy(s, d, w_sem.at[i]) for i, (s, d) in enumerate(pairs)]
    for load in loads:
        load.start()

    barrier = pltpu.get_barrier_semaphore()

    def greet(target):
        pl.semaphore_signal(barrier, inc=1, device_id=target)

    for k in range(1, T):
        greet({"tp": (tp + k) % T})
    for k in range(1, Y):
        greet({"sp": z * Y + (y + k) % Y})
    has_up = z + 1 < Z
    has_down = z > 0
    far_up = jnp.logical_and(has_up, y == Y - 1) if Y > 1 else None
    far_down = jnp.logical_and(has_down, y == 0) if Y > 1 else None
    expect = (T - 1) + (Y - 1) + has_up.astype(jnp.int32) + has_down.astype(jnp.int32)

    @pl.when(has_up)
    def _():
        greet({"sp": sp + Y})

    @pl.when(has_down)
    def _():
        greet({"sp": sp - Y})

    if Y > 1:
        expect = expect + far_up.astype(jnp.int32) + far_down.astype(jnp.int32)

        @pl.when(far_up)
        def _():
            greet({"sp": sp + 1})

        @pl.when(far_down)
        def _():
            greet({"sp": sp - 1})

    pl.semaphore_wait(barrier, expect)

    def tok_rows(r):
        return pl.ds(pl.multiple_of(r * R, R), R)

    def tok_copy(src, piece, r, send, target):
        return pltpu.make_async_remote_copy(
            src_ref=src,
            dst_ref=tok.at[piece, tok_rows(r), :],
            send_sem=send,
            recv_sem=tok_recv.at[piece, r],
            device_id={"tp": target},
        )

    def tok_own(k, r):
        target = peer(k) if k else sib
        return tok_copy(tokens.at[tok_rows(r), :], tp, r, tok_send.at[k, r], target)

    def tok_forward(k, r):
        piece = source(k)
        return tok_copy(tok.at[piece, tok_rows(r), :], piece, r, tok_relay.at[k, r], sib)

    def tok_wait(piece, r):
        tok_copy(tok.at[piece, tok_rows(r), :], piece, r, tok_send.at[0, r], sib).wait_recv()

    for r in range(NR):
        for k in list(range(1, X)) + [0]:
            tok_own(k, r).start()

    lane = lax.broadcasted_iota(jnp.int32, (R, V), 1)
    first = (lane % hd) < (hd // 2)

    def table(r, carry):
        base = sp * L + r * R
        pos = (base + lax.broadcasted_iota(jnp.int32, (R, V), 0)).astype(F32)
        angle = pos * freq[...]
        sine = jnp.sin(angle)
        cos_t[tok_rows(r), :] = jnp.cos(angle)
        sin_t[tok_rows(r), :] = jnp.where(first, -sine, sine)
        return carry

    lax.fori_loop(0, NR, table, 0)

    def rotate(block, rows):
        low = (lax.broadcasted_iota(jnp.int32, block.shape, 1) % hd) < (hd // 2)
        other = jnp.where(
            low, pltpu.roll(block, V - hd // 2, 1), pltpu.roll(block, hd // 2, 1)
        )
        return block * cos_t[rows, :] + other * sin_t[rows, :]

    def kv_copy(j, r, send, target):
        block = kv.at[j, tok_rows(r), :]
        return pltpu.make_async_remote_copy(
            src_ref=block,
            dst_ref=block,
            send_sem=send,
            recv_sem=kv_recv.at[j, r],
            device_id={"sp": target},
        )

    def kv_up(dz, r):
        return kv_copy(sp - dz * Y, r, kv_send_z.at[dz, r], sp + Y)

    def kv_side(dz, r, k):
        return kv_copy(sp - dz * Y, r, kv_send_y.at[dz, r, k - 1], z * Y + (y + k) % Y)

    def kv_wait(j, r):
        kv_copy(j, r, kv_send_z.at[0, r], sp).wait_recv()

    EX = NR // 2 if Y == 2 else 0

    def extra(r):
        return kv_copy(0, r, kv_extra.at[r], sp + Y)

    def kv_send(dz, r, act):
        @pl.when(has_up)
        def _():
            act(kv_up(dz, r))

        for k in range(1, Y):
            wanted = jnp.logical_or(dz > 0, y + k < Y)
            if EX:
                other_way = jnp.logical_and(dz == z, jnp.logical_and(dz > 0, r < EX))
                wanted = jnp.logical_and(wanted, jnp.logical_not(jnp.logical_and(y == 0, other_way)))

            @pl.when(wanted)
            def _():
                act(kv_side(dz, r, k))

    def relay(dz, r):
        @pl.when(dz <= z)
        def _():
            kv_wait(sp - dz * Y, r)
            kv_send(dz, r, lambda copy: copy.start())

    def first_relay(r):
        relay(1, r)
        if EX:

            @pl.when(jnp.logical_and(jnp.logical_and(z == 0, y == 1), r < EX))
            def _():
                kv_wait(0, r)

                @pl.when(has_up)
                def _():
                    extra(r).start()

    own.wait()
    loads[0].wait()
    loads[1].wait()

    def key_chunk(r, carry):
        rows = tok_rows(r)
        for k in range(1, X):
            tok_wait(source(k), r)
            tok_forward(k, r).start()
        tok_wait(sib, r)
        for k in range(1, X):
            tok_wait(((xi + k) % X) * 2 + (1 - core), r)
        squares = jnp.zeros((R, 1), F32)
        for t in range(T):
            block = tok[t, rows, :].astype(F32)
            squares = squares + jnp.sum(block * block, axis=1, keepdims=True)
            scaled[rows, t * Dt : (t + 1) * Dt] = (block * gain[:, t * Dt : (t + 1) * Dt]).astype(BF16)
        inverse = lax.rsqrt(squares / Wd + NORM_EPS)
        inv[rows, :] = inverse
        left = scaled[rows, :]
        keys = inverse * dot(left, wk[...])
        for h in range(H):
            kv[sp, rows, h * V : (h + 1) * V] = rotate(keys[:, h * V : (h + 1) * V], rows).astype(BF16)
        kv[sp, rows, C : 2 * C] = (inverse * dot(left, wv[...])).astype(BF16)
        kv_send(0, r, lambda copy: copy.start())

        @pl.when(r > 0)
        def _():
            first_relay(r - 1)

        return carry

    lax.fori_loop(0, NR, key_chunk, 0)

    for load in loads[2:6]:
        load.wait()
    half = lax.broadcasted_iota(jnp.int32, (M, V), 1) < hd
    scale = hd ** (-0.5)

    def mix_rows(r):
        return pl.ds(pl.multiple_of(r * M, M), M)

    def query_chunk(r, carry):
        rows = mix_rows(r)
        inverse = inv[rows, :]
        left = scaled[rows, :]
        queries = inverse * dot(left, wq[...])
        for h in range(H):
            turned = rotate(queries[:, h * V : (h + 1) * V], rows).astype(BF16).astype(F32) * scale
            qz[h, 0, rows, :] = jnp.where(half, turned, 0.0).astype(BF16)
            qz[h, 1, rows, :] = jnp.where(half, 0.0, turned).astype(BF16)
        inner = (inverse * dot(left, wi[...])).astype(BF16)
        signal = (inverse * dot(left, ws[...])).astype(BF16)
        conv_in = (inner.astype(F32) * signal.astype(F32)).astype(BF16)
        padded[pl.ds(pl.multiple_of(PAD + r * M, PAD), M), :] = conv_in.astype(F32)
        gate[rows, :] = (inverse * dot(left, wo[...])).astype(BF16)

        @pl.when(r == 0)
        def _():
            first_relay(NR - 1)

        return carry

    lax.fori_loop(0, NM, query_chunk, 0)
    tail[...] = padded[L : L + PAD, :].astype(BF16)
    rim_copy = pltpu.make_async_remote_copy(
        src_ref=tail,
        dst_ref=rim,
        send_sem=rim_sem.at[0],
        recv_sem=rim_sem.at[1],
        device_id={"sp": (sp + 1) % S},
    )

    @pl.when(sp + 1 < S)
    def _():
        rim_copy.start()

    def attend(j, diagonal):
        def one(i, carry):
            rows = mix_rows(i)
            for h in range(H):
                query = qz[h, :, rows, :].reshape(2 * M, V)
                scores = dot_t(query, kv[j, :, h * V : (h + 1) * V])
                if diagonal:
                    row = lax.broadcasted_iota(jnp.int32, scores.shape, 0)
                    row = jnp.where(row >= M, row - M, row) + i * M
                    col = lax.broadcasted_iota(jnp.int32, scores.shape, 1)
                    scores = jnp.where(row >= col, scores, MASKED)
                    new_max = jnp.max(scores, axis=1, keepdims=True)
                else:
                    old_max = row_max[h, :, rows, :].reshape(2 * M, 1)
                    new_max = jnp.maximum(old_max, jnp.max(scores, axis=1, keepdims=True))
                weights = jnp.exp(scores - new_max)
                sums = jnp.sum(weights, axis=1, keepdims=True)
                mixed = dot(weights.astype(BF16), kv[j, :, C + h * V : C + (h + 1) * V])
                if not diagonal:
                    fade = jnp.exp(old_max - new_max)
                    sums = sums + fade * row_sum[h, :, rows, :].reshape(2 * M, 1)
                    mixed = mixed + fade * acc[h, :, rows, :].reshape(2 * M, V)
                row_max[h, :, rows, :] = new_max.reshape(2, M, 1)
                row_sum[h, :, rows, :] = sums.reshape(2, M, 1)
                acc[h, :, rows, :] = mixed.reshape(2, M, V)
            return carry

        lax.fori_loop(0, NM, one, 0)

    attend(sp, True)

    @pl.when(sp > 0)
    def _():
        rim_copy.wait_recv()
        padded[0:PAD, :] = rim[...].astype(F32)

    @pl.when(sp == 0)
    def _():
        padded[0:PAD, :] = jnp.zeros((PAD, C), F32)

    summed = jnp.zeros((L, C), F32)
    for j in range(taps_n):
        begin = PAD - (taps_n - 1) + j
        summed = summed + taps[j : j + 1, :] * padded[begin : begin + L, :]
    conv_all[tp, :, :] = (gate[...].astype(F32) * summed).astype(BF16)

    def mix_copy(which, buf, piece, r, send, target):
        block = buf.at[piece, mix_rows(r), :]
        return pltpu.make_async_remote_copy(
            src_ref=block,
            dst_ref=block,
            send_sem=send,
            recv_sem=mix_recv.at[which, piece, r],
            device_id={"tp": target},
        )

    def mix_own(which, buf, k, r):
        target = peer(k) if k else sib
        return mix_copy(which, buf, tp, r, mix_send.at[which, k, r], target)

    def mix_forward(which, buf, k, r):
        return mix_copy(which, buf, source(k), r, mix_relay.at[which, k, r], sib)

    def mix_wait(which, buf, piece, r):
        mix_copy(which, buf, piece, r, mix_send.at[which, 0, r], sib).wait_recv()

    for r in range(NM):
        for k in list(range(1, X)) + [0]:
            mix_own(0, conv_all, k, r).start()

    def step(dz, carry):
        def row_block(k, inner):
            def forward(r, c):
                relay(dz + 1, r)
                return c

            lax.fori_loop(k * NR // Y, (k + 1) * NR // Y, forward, 0)
            side = (y + k) % Y
            level = jnp.where(k == 0, z - dz, z - dz + 1)
            j = level * Y + side
            valid = jnp.where(k == 0, dz <= z, jnp.logical_or(level < z, side < y))

            @pl.when(valid)
            def _():
                @pl.when(k > 0)
                def _():
                    for r in range(NR):
                        if r < EX:
                            climbs = jnp.logical_and(level == 0, y == 1)

                            @pl.when(jnp.logical_not(jnp.logical_and(climbs, z == 0)))
                            def _():
                                kv_wait(j, r)

                            @pl.when(jnp.logical_and(climbs, jnp.logical_and(z > 0, has_up)))
                            def _():
                                extra(r).start()

                        else:
                            kv_wait(j, r)

                attend(j, False)

            return inner

        lax.fori_loop(0, Y, row_block, 0)
        return carry

    lax.fori_loop(1, z + 2, step, 0)

    def finish(i, carry):
        rows = mix_rows(i)
        for h in range(H):
            first_map = acc[h, 0, rows, :] / row_sum[h, 0, rows, :]
            second_map = acc[h, 1, rows, :] / row_sum[h, 1, rows, :]
            head_mix = first_map - lambdas[h] * second_map
            mean = jnp.mean(head_mix * head_mix, axis=1, keepdims=True)
            normed = head_mix * lax.rsqrt(mean + HEAD_EPS) * head_gain[...] * HEAD_SCALE
            attn_all[tp, rows, h * V : (h + 1) * V] = normed.astype(BF16)
        for k in list(range(1, X)) + [0]:
            mix_own(1, attn_all, k, i).start()
        return carry

    lax.fori_loop(0, NM, finish, 0)

    loads[6].wait()
    loads[7].wait()

    def gather(which, buf, r):
        for k in range(1, X):
            mix_wait(which, buf, source(k), r)
            mix_forward(which, buf, k, r).start()

    def gather_rest(which, buf, r):
        mix_wait(which, buf, sib, r)
        for k in range(1, X):
            mix_wait(which, buf, ((xi + k) % X) * 2 + (1 - core), r)

    def conv_part(r, carry):
        rows = mix_rows(r)
        gather(0, conv_all, r)
        gather_rest(0, conv_all, r)
        part = dot(conv_all[0, rows, :], wc[0:C, :])
        for t in range(1, T):
            part = part + dot(conv_all[t, rows, :], wc[t * C : (t + 1) * C, :])
        total[rows, :] = part
        return carry

    lax.fori_loop(0, NM, conv_part, 0)

    lanes = lax.broadcasted_iota(jnp.int32, (L, 128), 1)
    columns = jnp.zeros((L, 128), F32)
    for h in range(H):
        for c in range(2):
            value = row_max[h, c, :, :] + jnp.log(row_sum[h, c, :, :])
            columns = jnp.where(lanes == 2 * h + c, value, columns)
    turned_columns = jnp.transpose(columns)
    for h in range(H):
        lse[h] = turned_columns[2 * h : 2 * h + 2, :]

    def attn_part(r, carry):
        rows = mix_rows(r)
        gather(1, attn_all, r)
        gather_rest(1, attn_all, r)
        part = total[rows, :]
        for t in range(T):
            part = part + dot(attn_all[t, rows, :], wa[t * C : (t + 1) * C, :])
        out[rows, :] = part.astype(BF16)
        return carry

    lax.fori_loop(0, NM, attn_part, 0)

    for r in range(NR):
        for k in range(X):
            tok_own(k, r).wait_send()
        for k in range(1, X):
            tok_forward(k, r).wait_send()

    def drain(dz, carry):
        def inner(r, c):
            kv_send(dz, r, lambda copy: copy.wait_send())
            return c

        return lax.fori_loop(0, NR, inner, carry)

    lax.fori_loop(0, z + 1, drain, 0)
    if EX:

        @pl.when(jnp.logical_and(y == 1, has_up))
        def _():
            for r in range(EX):
                extra(r).wait_send()

    for which, buf in ((0, conv_all), (1, attn_all)):
        for r in range(NM):
            for k in range(X):
                mix_own(which, buf, k, r).wait_send()
            for k in range(1, X):
                mix_forward(which, buf, k, r).wait_send()

    @pl.when(sp + 1 < S)
    def _():
        rim_copy.wait_send()


def ring_device(
    dims,
    tokens,
    norm_gain,
    query_weight,
    key_weight,
    value_weight,
    outer_gate_weight,
    inner_gate_weight,
    conv_input_weight,
    conv_taps,
    lambdas,
    head_gain,
    attn_out_weight,
    conv_out_weight,
):
    S, T, Z, Y = dims["S"], dims["T"], dims["Z"], dims["Y"]
    L, Dt = tokens.shape
    H = lambdas.shape[0]
    C = query_weight.shape[1]
    V = C // H
    hd = V // 2
    O = attn_out_weight.shape[1]
    Wd = norm_gain.shape[0]
    NR, NM, PAD = 4, 2, 16
    X = T // 2
    frequency = ROPE_BASE ** (-np.arange(hd // 2) * 2.0 / hd)
    freq = jnp.asarray(np.tile(frequency, 4)[None, :], F32)
    any_spec = pl.BlockSpec(memory_space=pl.ANY)
    vmem = pl.BlockSpec(memory_space=pltpu.VMEM)
    smem = pl.BlockSpec(memory_space=pltpu.SMEM)
    dma = pltpu.SemaphoreType.DMA
    mixed, lse = pl.pallas_call(
        functools.partial(ring_kernel, dict(dims, H=H)),
        out_shape=(
            jax.ShapeDtypeStruct((L, O), BF16),
            jax.ShapeDtypeStruct((H, 2, L), F32),
        ),
        in_specs=[any_spec, vmem, vmem] + [any_spec] * 6 + [vmem, smem, vmem] + [any_spec] * 2,
        out_specs=(vmem, vmem),
        scratch_shapes=[
            pltpu.VMEM((T, L, Dt), BF16),
            pltpu.VMEM((L, Wd), BF16),
            pltpu.VMEM((L, 1), F32),
            pltpu.VMEM((L, V), F32),
            pltpu.VMEM((L, V), F32),
        ]
        + [pltpu.VMEM((Wd, C), BF16)] * 6
        + [pltpu.VMEM((T * C, O), BF16)] * 2
        + [
            pltpu.VMEM((S, L, 2 * C), BF16),
            pltpu.VMEM((H, 2, L, V), BF16),
            pltpu.VMEM((H, 2, L, 1), F32),
            pltpu.VMEM((H, 2, L, 1), F32),
            pltpu.VMEM((H, 2, L, V), F32),
            pltpu.VMEM((L, C), BF16),
            pltpu.VMEM((PAD + L, C), F32),
            pltpu.VMEM((PAD, C), BF16),
            pltpu.VMEM((PAD, C), BF16),
            pltpu.VMEM((T, L, C), BF16),
            pltpu.VMEM((T, L, C), BF16),
            pltpu.VMEM((L, O), F32),
            dma((8,)),
            dma,
            dma((T, NR)),
            dma((X, NR)),
            dma((X, NR)),
            dma((S, NR)),
            dma((Z, NR)),
            dma((Z, NR, max(Y - 1, 1))),
            dma((NR,)),
            dma((2,)),
            dma((2, T, NM)),
            dma((2, X, NM)),
            dma((2, X, NM)),
        ],
        compiler_params=pltpu.CompilerParams(
            collective_id=0, has_side_effects=True, vmem_limit_bytes=60 * 1024 * 1024
        ),
        name="mixer",
    )(
        tokens,
        norm_gain[None, :],
        freq,
        query_weight,
        key_weight,
        value_weight,
        outer_gate_weight,
        inner_gate_weight,
        conv_input_weight,
        conv_taps,
        lambdas,
        head_gain[None, :],
        attn_out_weight,
        conv_out_weight,
    )
    return mixed, lse


def pair_kernel(
    dims,
    tokens,
    gain_h,
    freq_h,
    wq_h,
    wk_h,
    wv_h,
    wo_h,
    wi_h,
    ws_h,
    taps_h,
    lambdas,
    head_gain_h,
    wa_h,
    wc_h,
    out,
    lse,
    tok,
    scaled,
    inv,
    cos_t,
    sin_t,
    gain_t,
    wq,
    wk,
    wv,
    wo,
    wi,
    ws,
    wa,
    wc,
    kvq,
    turned,
    row_max,
    row_sum,
    acc,
    gate,
    padded,
    tail,
    rim,
    conv_all,
    attn_all,
    away,
    lse_away,
    lse_in,
    total,
    freq,
    gain,
    taps,
    head_gain,
    w_sem,
    own_sem,
    tok_recv,
    tok_send,
    tok_relay,
    kv_recv,
    side_recv,
    swap_send,
    ask_recv,
    cross_send,
    side_send,
    up_send,
    rim_sem,
    lse_sem,
    mix_recv,
    mix_send,
    mix_relay,
    at_recv,
    at_send,
    at_away,
    at_relay,
    at_relay_away,
):
    S, T, Z, Y, H = dims["S"], dims["T"], dims["Z"], dims["Y"], dims["H"]
    L, Dt = tokens.shape
    Wd = T * Dt
    C = wq_h.shape[1]
    V = C // H
    hd = V // 2
    NR = tok_recv.shape[1]
    R = L // NR
    NM = at_recv.shape[2]
    M = L // NM
    G = M // R
    LATE = 2
    LAG = 3
    X = T // 2
    taps_n = taps.shape[0]
    PAD = tail.shape[0]

    sp = lax.axis_index("sp")
    tp = lax.axis_index("tp")
    z = sp // Y
    y = sp % Y
    pair = z // 2
    a = z % 2
    mate = sp + (1 - 2 * a) * Y
    core = tp % 2
    xi = tp // 2
    sib = xi * 2 + (1 - core)
    has_up = z + 2 - a < Z
    has_down = pair > 0

    def peer(k):
        return ((xi + k) % X) * 2 + core

    def source(k):
        return ((xi - k + X) % X) * 2 + core

    def source_sib(k):
        return ((xi - k + X) % X) * 2 + (1 - core)

    own = pltpu.make_async_copy(tokens, tok.at[tp], own_sem)
    own.start()
    barrier = pltpu.get_barrier_semaphore()

    def greet(target):
        pl.semaphore_signal(barrier, inc=1, device_id=target)

    for k in range(1, T):
        greet({"tp": (tp + k) % T})
    for k in range(X):
        greet({"sp": mate, "tp": peer(k)})
    for k in range(1, Y):
        greet({"sp": z * Y + (y + k) % Y})
    expect = (T - 1) + X + (Y - 1)
    bridge_up = jnp.logical_and(a == 1, has_up)
    prompt = jnp.logical_not(bridge_up)
    bridge_down = jnp.logical_and(a == 0, has_down)
    for near, step in (
        (has_up, 2 * Y),
        (has_down, -2 * Y),
        (bridge_up, Y),
        (bridge_down, -Y),
        (sp + 1 < S, 1),
        (sp > 0, -1),
    ):
        expect = expect + near.astype(jnp.int32)

        @pl.when(near)
        def _():
            greet({"sp": sp + step})

    pairs = [(wk_h, wk), (wv_h, wv), (wq_h, wq), (wi_h, wi), (ws_h, ws), (wo_h, wo), (wc_h, wc), (wa_h, wa)]
    pairs = pairs + [(freq_h, freq), (gain_h, gain), (taps_h, taps), (head_gain_h, head_gain)]
    loads = [pltpu.make_async_copy(s, d, w_sem.at[i]) for i, (s, d) in enumerate(pairs)]

    pl.semaphore_wait(barrier, expect)

    def tok_rows(r):
        return pl.ds(pl.multiple_of(r * R, R), R)

    def tok_copy(src, piece, r, send, target):
        return pltpu.make_async_remote_copy(
            src_ref=src,
            dst_ref=tok.at[piece, tok_rows(r), :],
            send_sem=send,
            recv_sem=tok_recv.at[piece, r],
            device_id={"tp": target},
        )

    def tok_own(k, r):
        target = peer(k) if k else sib
        return tok_copy(tok.at[tp, tok_rows(r), :], tp, r, tok_send, target)

    def tok_forward(k, r):
        piece = source(k)
        return tok_copy(tok.at[piece, tok_rows(r), :], piece, r, tok_relay, sib)

    def tok_wait(piece, r):
        tok_copy(tok.at[piece, tok_rows(r), :], piece, r, tok_send, sib).wait_recv()

    own.wait()
    for r in reversed(range(NR)):
        for k in list(range(1, X)) + [0]:
            tok_own(k, r).start()
    for load in loads[8:] + loads[:8]:
        load.start()

    lane = lax.broadcasted_iota(jnp.int32, (R, V), 1)
    first = (lane % hd) < (hd // 2)

    loads[8].wait()
    loads[11].wait()

    def table(r, carry):
        base = sp * L + r * R
        pos = (base + lax.broadcasted_iota(jnp.int32, (R, V), 0)).astype(F32)
        angle = pos * freq[...]
        sine = jnp.sin(angle)
        cos_t[tok_rows(r), :] = jnp.cos(angle)
        sin_t[tok_rows(r), :] = jnp.where(first, -sine, sine)
        return carry

    lax.fori_loop(0, NR, table, 0)
    gain_t[...] = jnp.transpose(jnp.broadcast_to(head_gain[...], (M, V)))

    row_max[...] = jnp.full(row_max.shape, MASKED, F32)
    row_sum[...] = jnp.zeros(row_sum.shape, F32)
    acc[...] = jnp.zeros(acc.shape, F32)

    def rotate(block, rows):
        other = jnp.where(first, pltpu.roll(block, V - hd // 2, 1), pltpu.roll(block, hd // 2, 1))
        return block * cos_t[rows, :] + other * sin_t[rows, :]

    def level_block(level):
        return level * Y + y

    def kv_copy(level, r, send, target, src=None, recv=None):
        block = kvq.at[level_block(level), r, pl.ds(0, 2)]
        return pltpu.make_async_remote_copy(
            src_ref=block if src is None else src,
            dst_ref=block,
            send_sem=send,
            recv_sem=kv_recv.at[level, r] if recv is None else recv,
            device_id={"sp": target},
        )

    def sent(ref, sem):
        pltpu.make_async_remote_copy(
            src_ref=ref, dst_ref=ref, send_sem=sem, recv_sem=sem, device_id={"sp": mate}
        ).wait_send()

    mate_level = z + 1 - 2 * a
    top = 2 * pair + 1

    def swap(r):
        return kv_copy(z, r, swap_send, mate, kvq.at[S, r, pl.ds(0, 2)])

    def ask(j, r):
        return pltpu.make_async_remote_copy(
            src_ref=kvq.at[S, r, 2],
            dst_ref=kvq.at[j, r, 2],
            send_sem=swap_send,
            recv_sem=ask_recv,
            device_id={"sp": mate},
        )

    def cross(r):
        return kv_copy(z, r, cross_send, sp + Y, kvq.at[S, r, pl.ds(0, 2)])

    def up(level, r):
        return kv_copy(level, r, up_send.at[level], sp + 2 * Y)

    def side(level, r, k):
        late = 1 - jnp.minimum(r // LATE, 1)
        return kv_copy(
            level,
            r,
            side_send.at[level, k - 1],
            z * Y + (y + k) % Y,
            recv=side_recv.at[level, k - 1, late],
        )

    def kv_wait(level, r):
        kv_copy(level, r, cross_send, mate).wait_recv()

    def beside_wait(level, k, late):
        rows = pl.ds(0, LATE) if late else pl.ds(LATE, NR - LATE)
        block = kvq.at[level * Y + (y + k) % Y, rows, pl.ds(0, 2)]
        pltpu.make_async_remote_copy(
            src_ref=block,
            dst_ref=block,
            send_sem=cross_send,
            recv_sem=side_recv.at[level, Y - k - 1, int(late)],
            device_id={"sp": mate},
        ).wait_recv()

    def spread(level, r, rises):
        @pl.when(rises)
        def _():
            up(level, r).start()

        for k in range(1, Y):

            @pl.when(jnp.logical_or(level < top, y < (y + k) % Y))
            def _():
                side(level, r, k).start()

    def spread_done(level, rises):
        whole = kvq.at[level_block(level), :, pl.ds(0, 2)]

        @pl.when(rises)
        def _():
            sent(whole, up_send.at[level])

        for k in range(1, Y):

            @pl.when(jnp.logical_or(level < top, y < (y + k) % Y))
            def _():
                sent(whole, side_send.at[level, k - 1])

    def send_own(r):
        swap(r).start()

        @pl.when(bridge_up)
        def _():
            cross(r).start()

        spread(z, r, has_up)


    def relay_mate(r):
        kv_wait(mate_level, r)
        spread(mate_level, r, bridge_up)

    def relay_below(level, r):
        kv_wait(level, r)
        spread(level, r, has_up)

    for load in loads[:5] + loads[9:11]:
        load.wait()
    rim_copy = pltpu.make_async_remote_copy(
        src_ref=tail,
        dst_ref=rim,
        send_sem=rim_sem.at[0],
        recv_sem=rim_sem.at[1],
        device_id={"sp": (sp + 1) % S},
    )
    scale = hd ** (-0.5)

    def tok_next(r):
        for k in range(1, X):
            tok_wait(source(k), r)
            tok_forward(k, r).start()

    tok_next(NR - 1)

    def chunk(i, carry):
        r = NR - 1 - i
        rows = tok_rows(r)
        tok_wait(sib, r)
        for k in range(1, X):
            tok_wait(source_sib(k), r)

        @pl.when(i < NR - 1)
        def _():
            tok_next(r - 1)

        squares = jnp.zeros((R, 1), F32)
        for t in range(T):
            block = tok[t, rows, :].astype(F32)
            squares = squares + jnp.sum(block * block, axis=1, keepdims=True)
            scaled[rows, t * Dt : (t + 1) * Dt] = (block * gain[:, t * Dt : (t + 1) * Dt]).astype(BF16)
        inverse = lax.rsqrt(squares / Wd + NORM_EPS)
        inv[rows, :] = inverse
        left = scaled[rows, :]
        keys = inverse * dot(left, wk[...])
        values = inverse * dot(left, wv[...])
        for h in range(H):
            mine = a if h else 1 - a
            slot = sp * mine + S * (1 - mine)
            cols = slice(h * V, (h + 1) * V)
            kvq[slot, r, 0] = rotate(keys[:, cols], rows).astype(BF16)
            kvq[slot, r, 1] = values[:, cols].astype(BF16)
        send_own(r)
        queries = inverse * dot(left, wq[...])
        for h in range(H):
            mine = a if h else 1 - a
            slot = sp * mine + S * (1 - mine)
            cols = slice(h * V, (h + 1) * V)
            kvq[slot, r, 2] = (rotate(queries[:, cols], rows).astype(BF16).astype(F32) * scale).astype(BF16)

        @pl.when(i == 0)
        def _():
            edge = pl.ds(L - PAD, PAD)
            inner = (inv[edge, :] * dot(scaled[edge, :], wi[...])).astype(BF16)
            signal = (inv[edge, :] * dot(scaled[edge, :], ws[...])).astype(BF16)
            tail[...] = (inner.astype(F32) * signal.astype(F32)).astype(BF16)

            @pl.when(sp + 1 < S)
            def _():
                rim_copy.start()

        @pl.when(jnp.logical_and(prompt, i >= LAG))
        def _():
            relay_mate(r + LAG)

        return carry

    lax.fori_loop(0, NR, chunk, 0)
    for r in reversed(range(NR)):
        ask(sp, r).start()

    def level_at(n):
        odd = n % 2
        return 2 * (pair - 1 - n // 2) + a * (1 - odd) + (1 - a) * odd

    def relay_level(n, rows, when=None):
        wanted = n < 2 * pair
        if when is not None:
            wanted = jnp.logical_and(wanted, when)

        @pl.when(wanted)
        def _():
            for r in rows:
                relay_below(level_at(n), r)

    order = list(reversed(range(NR)))

    def relay_rest(i, carry):
        relay_mate(NR - 1 - i)
        return carry

    @pl.when(a == 0)
    def _():
        lax.fori_loop(NR - LAG, NR, relay_rest, 0)

    relay_level(0, order[:4], a == 0)
    relay_level(0, order[:2], a == 1)

    loads[5].wait()

    def mix_rows(r):
        return pl.ds(pl.multiple_of(r * M, M), M)

    def gate_chunk(r, carry):
        rows = mix_rows(r)
        inverse = inv[rows, :]
        left = scaled[rows, :]
        inner = (inverse * dot(left, wi[...])).astype(BF16)
        signal = (inverse * dot(left, ws[...])).astype(BF16)
        conv_in = (inner.astype(F32) * signal.astype(F32)).astype(BF16)
        padded[pl.ds(pl.multiple_of(PAD + r * M, PAD), M), :] = conv_in.astype(F32)
        gate[rows, :] = (inverse * dot(left, wo[...])).astype(BF16)
        return carry

    lax.fori_loop(0, NM, gate_chunk, 0)

    @pl.when(sp > 0)
    def _():
        rim_copy.wait_recv()
        padded[0:PAD, :] = rim[...].astype(F32)

    @pl.when(sp == 0)
    def _():
        padded[0:PAD, :] = jnp.zeros((PAD, C), F32)

    summed = jnp.zeros((L, C), F32)
    for j in range(taps_n):
        begin = PAD - (taps_n - 1) + j
        summed = summed + taps[j : j + 1, :] * padded[begin : begin + L, :]
    conv_all[tp, :, :] = (gate[...].astype(F32) * summed).astype(BF16)

    def mix_copy(piece, send, target):
        block = conv_all.at[piece]
        return pltpu.make_async_remote_copy(
            src_ref=block,
            dst_ref=block,
            send_sem=send,
            recv_sem=mix_recv.at[piece],
            device_id={"tp": target},
        )

    def mix_own(k):
        return mix_copy(tp, mix_send, peer(k) if k else sib)

    def mix_forward(k):
        return mix_copy(source(k), mix_relay, sib)

    def mix_wait(piece):
        mix_copy(piece, mix_send, sib).wait_recv()

    for k in list(range(1, X)) + [0]:
        mix_own(k).start()

    blank = jnp.zeros((hd, M), BF16)

    def flip(blocks):
        return jnp.transpose(jnp.concatenate(blocks, axis=0))

    def turn_queries(b):
        j = level_block(2 * pair + b)
        for part in range(NM):
            turned[b, part] = flip([kvq[j, G * part + g, 2] for g in range(G)])

    def attend(items):
        work = [(item, c) for item in items for c in range(2)]
        flipped = {}

        def score(item, c):
            chunks, b, part, shift = item
            keys = jnp.concatenate([kvq[j, r, 0] for j, r in chunks], axis=0)
            if c:
                right = jnp.concatenate([blank, turned[b, part, hd:, :]], axis=0)
            else:
                right = jnp.concatenate([turned[b, part, :hd, :], blank], axis=0)
            scores = dot(keys, right)
            if shift is not None:
                key_row = lax.broadcasted_iota(jnp.int32, scores.shape, 0)
                query_lane = lax.broadcasted_iota(jnp.int32, scores.shape, 1)
                scores = jnp.where(key_row <= query_lane + shift, scores, MASKED)
            return scores

        def mix(item, c, fade, weights):
            chunks, b, part, _ = item
            if id(chunks) not in flipped:
                flipped[id(chunks)] = flip([kvq[j, r, 1] for j, r in chunks])
            values = flipped[id(chunks)]
            acc[b, part, c] = fade * acc[b, part, c] + dot(values, weights)

        ready = [score(*work[0])]
        waiting = []
        for i, (item, c) in enumerate(work):
            for n in range(i + len(ready), min(i + 3, len(work))):
                ready.append(score(*work[n]))
            scores = ready.pop(0)
            _, b, part, _ = item
            old_max = row_max[b, part, c]
            new_max = jnp.maximum(old_max, jnp.max(scores, axis=0, keepdims=True))
            weights = jnp.exp(scores - new_max)
            fade = jnp.exp(old_max - new_max)
            row_max[b, part, c] = new_max
            row_sum[b, part, c] = fade * row_sum[b, part, c] + jnp.sum(weights, axis=0, keepdims=True)
            if waiting:
                mix(*waiting.pop())
            waiting.append((item, c, fade, weights.astype(BF16)))
        mix(*waiting.pop())

    def chunks_of(j, begin=0, end=NR):
        return [(j, r) for r in range(begin, end)]

    low_own = level_block(2 * pair)

    def triangle(j, b):
        return [(chunks_of(j, 0, G * (part + 1)), b, part, M * part) for part in reversed(range(NM))]

    turn_queries(a)
    attend(triangle(sp, a))
    @pl.when(a == 1)
    def _():
        lax.fori_loop(jnp.where(prompt, NR - LAG, 0), NR, relay_rest, 0)

    relay_level(0, order[2:3], a == 1)
    relay_level(0, order[4:], a == 0)
    relay_level(1, order[:2], a == 0)
    asked = kvq.at[mate, :, 2]
    pltpu.make_async_remote_copy(
        src_ref=asked, dst_ref=asked, send_sem=swap_send, recv_sem=ask_recv, device_id={"sp": mate}
    ).wait_recv()
    turn_queries(1 - a)
    whole_own = chunks_of(low_own)
    attend([(whole_own, 1, part, None) for part in range(NM)] + triangle(mate, 1 - a))
    relay_level(0, order[3:5], a == 1)
    relay_level(1, order[2:4], a == 0)

    for k in range(1, Y):
        other = (y + k) % Y
        ahead = other < y
        low = 2 * pair * Y + other
    for k in range(1, Y):
        other = (y + k) % Y
        ahead = other < y
        low = chunks_of(2 * pair * Y + other)
        high = chunks_of(top * Y + other)
        for late in (False, True):
            beside_wait(2 * pair, k, late)
        late_items = [(low, 1, part, None) for part in range(NM)]

        @pl.when(ahead)
        def _():
            for late in (False, True):
                beside_wait(top, k, late)
            attend(
                late_items
                + [(low, 0, part, None) for part in range(NM)]
                + [(high, 1, part, None) for part in range(NM)]
            )

        @pl.when(jnp.logical_not(ahead))
        def _():
            attend(late_items)

    relay_level(0, order[5:], a == 1)
    relay_level(1, order[4:], a == 0)
    def conv_pass():
        for k in range(1, X):
            mix_wait(source(k))
            mix_forward(k).start()

    def conv_product():
        loads[6].wait()
        mix_wait(sib)
        for k in range(1, X):
            mix_wait(source_sib(k))

        def conv_part(r, carry):
            rows = mix_rows(r)
            part = dot(conv_all[0, rows, :], wc[0:C, :])
            for t in range(1, T):
                part = part + dot(conv_all[t, rows, :], wc[t * C : (t + 1) * C, :])
            total[rows, :] = part
            return carry

        lax.fori_loop(0, NM, conv_part, 0)

    def at_copy(src, piece, h, r, send, target):
        return pltpu.make_async_remote_copy(
            src_ref=src,
            dst_ref=attn_all.at[piece, h, mix_rows(r), :],
            send_sem=send,
            recv_sem=at_recv.at[piece, h, r],
            device_id=target,
        )

    def at_own(k, r):
        target = {"tp": peer(k) if k else sib}
        return at_copy(attn_all.at[tp, a, mix_rows(r), :], tp, a, r, at_send, target)

    def at_off(k, r):
        target = {"sp": mate, "tp": peer(k)}
        return at_copy(away.at[mix_rows(r), :], tp, a, r, at_away, target)

    def at_forward(k, h, r, send):
        piece = source(k)
        return at_copy(attn_all.at[piece, h, mix_rows(r), :], piece, h, r, send, {"tp": sib})

    def at_wait(piece, h, r):
        at_copy(attn_all.at[piece, h, mix_rows(r), :], piece, h, r, at_send, {"tp": sib}).wait_recv()

    def near_forward(k, r):
        return at_forward(k, a, r, at_relay)

    def far_forward(k, r):
        return at_forward(k, 1 - a, r, at_relay_away)

    def finished(b, part):
        first_map = acc[b, part, 0] / row_sum[b, part, 0]
        second_map = acc[b, part, 1] / row_sum[b, part, 1]
        head_mix = first_map - lambdas[a] * second_map
        mean = jnp.mean(head_mix * head_mix, axis=0, keepdims=True)
        normed = head_mix * lax.rsqrt(mean + HEAD_EPS) * gain_t[...] * HEAD_SCALE
        return jnp.transpose(normed).astype(BF16)

    def log_total(b, part, c):
        return row_max[b, part, c] + jnp.log(row_sum[b, part, c])

    def send_away():
        for part in range(NM):
            away[part * M : (part + 1) * M, :] = finished(1 - a, part)
            for k in list(range(1, X)) + [0]:
                at_off(k, part).start()

    def below(n, carry):
        level = level_at(n)
        later = jnp.logical_or(n > 0, a == 1)

        def item(k, c):
            j = level * Y + (y + k) % Y
            final = jnp.logical_and(k == Y - 1, n == 2 * pair - 1)

            @pl.when(k == 1)
            def _():
                relay_level(n + 1, order[:2], later)

                @pl.when(n == 2 * pair - 2)
                def _():
                    conv_pass()

                relay_level(n + 1, order[2:4], later)

            @pl.when(jnp.logical_and(k > 0, jnp.logical_not(final)))
            def _():
                for late in (False, True):
                    beside_wait(level, k, late)
                relay_level(n + 1, order[4:6], later)

            @pl.when(jnp.logical_not(final))
            def _():
                chunks = chunks_of(j)
                attend([(chunks, b, part, None) for b in range(2) for part in range(NM)])

            @pl.when(final)
            def _():
                soon, last = chunks_of(j, LATE), chunks_of(j, 0, LATE)
                conv_product()
                beside_wait(level, k, False)
                attend([(soon, b, part, None) for b in range(2) for part in range(NM)])
                beside_wait(level, k, True)
                attend([(last, 1 - a, part, None) for part in range(NM)])
                send_away()
                attend([(last, a, part, None) for part in range(NM)])

            return c

        lax.fori_loop(0, Y, item, 0)
        relay_level(n + 1, order[6:], later)
        return carry

    lax.fori_loop(0, 2 * pair, below, 0)

    @pl.when(pair == 0)
    def _():
        send_away()

    for part in range(NM):
        attn_all[tp, a, part * M : (part + 1) * M, :] = finished(a, part)
        for k in list(range(1, X)) + [0]:
            at_own(k, part).start()
    for part in range(NM):
        for c in range(2):
            lse_away[c : c + 1, part * M : (part + 1) * M] = log_total(1 - a, part, c)
            lse[a, c : c + 1, part * M : (part + 1) * M] = log_total(a, part, c)
    lse_copy = pltpu.make_async_remote_copy(
        src_ref=lse_away,
        dst_ref=lse_in,
        send_sem=lse_sem.at[0],
        recv_sem=lse_sem.at[1],
        device_id={"sp": mate},
    )
    lse_copy.start()

    loads[7].wait()

    @pl.when(pair == 0)
    def _():
        conv_pass()
        conv_product()


    def pass_near():
        for r in range(NM):
            for k in range(1, X):
                at_wait(source(k), a, r)
                near_forward(k, r).start()

    def pass_far():
        for r in range(NM):
            for k in range(X):
                at_wait(source(k), 1 - a, r)
                far_forward(k, r).start()

    @pl.when(a == 1)
    def _():
        pass_far()

    pass_near()

    @pl.when(a == 0)
    def _():
        pass_far()

    def half_product(r, h):
        rows = mix_rows(r)
        part = total[rows, :]
        for t in range(0, T, 2):
            both = jnp.concatenate([attn_all[t + u, h, rows, :] for u in range(2)], axis=1)
            weight = jnp.concatenate(
                [wa[pl.ds(pl.multiple_of((t + u) * C + h * V, V), V), :] for u in range(2)], axis=0
            )
            part = part + dot(both, weight)
        return part

    def near_part(r, carry):
        for k in range(X):
            at_wait(source_sib(k), a, r)
        total[mix_rows(r), :] = half_product(r, a)
        return carry

    lax.fori_loop(0, NM, near_part, 0)
    def attn_part(r, carry):
        rows = mix_rows(r)
        for k in range(X):
            at_wait(source_sib(k), 1 - a, r)
        out[rows, :] = half_product(r, 1 - a).astype(BF16)
        return carry

    lse_copy.wait_recv()
    lse[1 - a] = lse_in[...]
    lax.fori_loop(0, NM, attn_part, 0)
    lse_copy.wait_send()

    sent(tok.at[pl.ds(0, X)], tok_send)
    sent(kvq.at[S], swap_send)
    sent(conv_all.at[pl.ds(0, X)], mix_send)
    sent(attn_all.at[pl.ds(0, X), 0], at_send)
    sent(attn_all.at[pl.ds(0, X), 0], at_away)
    sent(attn_all.at[pl.ds(0, X), 0], at_relay_away)
    if X > 1:
        sent(tok.at[pl.ds(0, X - 1)], tok_relay)
        sent(conv_all.at[pl.ds(0, X - 1)], mix_relay)
        sent(attn_all.at[pl.ds(0, X - 1), 0], at_relay)

    @pl.when(bridge_up)
    def _():
        sent(kvq.at[S, :, pl.ds(0, 2)], cross_send)

    spread_done(z, has_up)
    spread_done(mate_level, bridge_up)

    def drain_level(level, carry):
        spread_done(level, has_up)
        return carry

    lax.fori_loop(0, 2 * pair, drain_level, 0)

    @pl.when(sp + 1 < S)
    def _():
        rim_copy.wait_send()


def pair_device(
    dims,
    tokens,
    norm_gain,
    query_weight,
    key_weight,
    value_weight,
    outer_gate_weight,
    inner_gate_weight,
    conv_input_weight,
    conv_taps,
    lambdas,
    head_gain,
    attn_out_weight,
    conv_out_weight,
):
    S, T, Z, Y = dims["S"], dims["T"], dims["Z"], dims["Y"]
    L, Dt = tokens.shape
    H = lambdas.shape[0]
    C = query_weight.shape[1]
    V = C // H
    hd = V // 2
    O = attn_out_weight.shape[1]
    Wd = norm_gain.shape[0]
    R = V // 2
    M = 2 * V
    NR, NM, PAD = L // R, L // M, 16
    X = T // 2
    frequency = ROPE_BASE ** (-np.arange(hd // 2) * 2.0 / hd)
    freq = jnp.asarray(np.tile(frequency, 4)[None, :], F32)
    any_spec = pl.BlockSpec(memory_space=pl.ANY)
    vmem = pl.BlockSpec(memory_space=pltpu.VMEM)
    smem = pl.BlockSpec(memory_space=pltpu.SMEM)
    dma = pltpu.SemaphoreType.DMA
    mixed, lse = pl.pallas_call(
        functools.partial(pair_kernel, dict(dims, H=H)),
        out_shape=(
            pltpu.VMEM((L, O), BF16),
            pltpu.VMEM((H, 2, L), F32),
        ),
        in_specs=[any_spec] * 10 + [smem] + [any_spec] * 3,
        out_specs=(vmem, vmem),
        scratch_shapes=[
            pltpu.VMEM((T, L, Dt), BF16),
            pltpu.VMEM((L, Wd), BF16),
            pltpu.VMEM((L, 1), F32),
            pltpu.VMEM((L, V), F32),
            pltpu.VMEM((L, V), F32),
            pltpu.VMEM((V, M), F32),
        ]
        + [pltpu.VMEM((Wd, C), BF16)] * 6
        + [pltpu.VMEM((T * C, O), BF16)] * 2
        + [
            pltpu.VMEM((S + 1, NR, 3, R, V), BF16),
            pltpu.VMEM((2, NM, V, M), BF16),
            pltpu.VMEM((2, NM, 2, 1, M), F32),
            pltpu.VMEM((2, NM, 2, 1, M), F32),
            pltpu.VMEM((2, NM, 2, V, M), F32),
            pltpu.VMEM((L, C), BF16),
            pltpu.VMEM((PAD + L, C), F32),
            pltpu.VMEM((PAD, C), BF16),
            pltpu.VMEM((PAD, C), BF16),
            pltpu.VMEM((T, L, C), BF16),
            pltpu.VMEM((T, H, L, V), BF16),
            pltpu.VMEM((L, V), BF16),
            pltpu.VMEM((2, L), F32),
            pltpu.VMEM((2, L), F32),
            pltpu.VMEM((L, O), F32),
            pltpu.VMEM((1, V), F32),
            pltpu.VMEM((1, Wd), F32),
            pltpu.VMEM(conv_taps.shape, F32),
            pltpu.VMEM((1, V), F32),
            dma((12,)),
            dma,
            dma((T, NR)),
            dma,
            dma,
            dma((Z, NR)),
            dma((Z, max(Y - 1, 1), 2)),
            dma,
            dma,
            dma,
            dma((Z, max(Y - 1, 1))),
            dma((Z,)),
            dma((2,)),
            dma((2,)),
            dma((T,)),
            dma,
            dma,
            dma((T, H, NM)),
            dma,
            dma,
            dma,
            dma,
        ],
        compiler_params=pltpu.CompilerParams(
            collective_id=0,
            has_side_effects=True,
            vmem_limit_bytes=60 * 1024 * 1024,
        ),
        name="mixer",
    )(
        tokens,
        norm_gain[None, :],
        freq,
        query_weight,
        key_weight,
        value_weight,
        outer_gate_weight,
        inner_gate_weight,
        conv_input_weight,
        conv_taps,
        lambdas,
        head_gain[None, :],
        attn_out_weight,
        conv_out_weight,
    )
    return mixed, lse


def per_device(dims, *arrays):
    tokens, query_weight, lambdas = arrays[0], arrays[2], arrays[9]
    width = query_weight.shape[1] // lambdas.shape[0]
    paired = lambdas.shape[0] == 2 and dims["Z"] % 2 == 0 and dims["T"] % 2 == 0
    paired = paired and width == 128 and tokens.shape[0] % (2 * width) == 0
    return (pair_device if paired else ring_device)(dims, *arrays)


def solution(mesh):
    S, T = mesh.shape["sp"], mesh.shape["tp"]
    Y = max(d for d in range(1, S + 1) if S % d == 0 and d * d <= S)
    dims = {"S": S, "T": T, "Z": S // Y, "Y": Y}
    in_specs = (
        P("sp", "tp"),
        P(),
        P(None, "tp"),
        P(None, "tp"),
        P(None, "tp"),
        P(None, "tp"),
        P(None, "tp"),
        P(None, "tp"),
        P(None, "tp"),
        P("tp"),
        P(),
        P(None, "tp"),
        P(None, "tp"),
    )
    out_specs = (P("sp", "tp"), P("tp", None, "sp"))
    return jax.shard_map(
        functools.partial(per_device, dims),
        mesh=mesh,
        in_specs=in_specs,
        out_specs=out_specs,
        check_vma=False,
    )
```
